256 devices in a mesh: sp: 64 (over z, y, core), tp: 4 (over x).
Axes of the slice: x: 4, y: 4, z: 8, core: 2. Of those that a mesh axis runs over, the one named last changes fastest.
Arguments:
- queries: bfloat16 [8192, 2048], P('sp', 'tp'), may hold values from -6 to 6
- forget_logits: bfloat16 [2, 8192, 2048], P(None, 'sp', 'tp'), may hold values from -7.5 to 7.5
- value_matrix: bfloat16 [8192, 2048], P('sp', 'tp'), may hold values from -6 to 6
- output_gate_logits: bfloat16 [8192, 2048], P('sp', 'tp'), may hold values from -6 to 6
- forget_slack: float32 [2048], P('tp'), may hold values from 6.1035156e-05 to 0.07
- spike_log_forget: float32 [8192, 16], P('sp', 'tp'), may hold values from -2.8 to 0, as said below
- head_norm_gain: bfloat16 [128], replicated, may hold values from 0.099609375 to 1.8984375
- output_weight: bfloat16 [2048, 2048], P('tp'), may hold values from -0.125 to 0.125
- residual: bfloat16 [8192, 2048], P('sp'), may hold values from -6 to 6
- mixer_norm_gain: bfloat16 [2048], replicated, may hold values from 0.099609375 to 1.8984375
- mixer_gate_weight: bfloat16 [2048, 5632], P('sp', 'tp'), may hold values from -0.125 to 0.125
- mixer_up_weight: bfloat16 [2048, 5632], P('sp', 'tp'), may hold values from -0.125 to 0.125
- mixer_down_weight: bfloat16 [5632, 2048], P('tp', 'sp'), may hold values from -0.078125 to 0.078125
Outputs:
- layer_out: bfloat16 [8192, 2048], P(('sp', 'tp'))
The draws below stay inside these ranges and needn't reach their ends.
Inputs may be any that keep to these rules, and one draw needn't show every extreme that they name: `spike_log_forget`: zero at all but a few tokens.
All inputs are finite; a program needn't handle non-finite values.
Results may differ from the reference program's by a relative error of at most 0.015.
Values may be sent and summed in bfloat16 or wider, within the bound.
No kernel may reach another device: no remote copies, remote signals or barrier semaphores. Data moves between devices by JAX's collectives and lax.ppermute only.
A program may use at most 128 MiB of HBM per device.

```python
import jax
import jax.numpy as jnp
from jax import lax

D = 2048
FF = 5632
HEADS = 16
HEAD = 128
BLOCK = 128
TOK_DEV = 128
TOKENS = 8192
N_TP = 4


def quick_heads(key, quick_count):
    pick_key = jax.random.fold_in(jax.random.fold_in(key, 23), 0)
    ordering = jax.random.permutation(pick_key, HEADS)
    return ordering < quick_count


def draw_forget_logits(key, part):
    noise_key, steady_key, slow_key, channel_key = jax.random.split(jax.random.fold_in(key, 11), 4)
    channels = HEADS * HEAD
    blocks_count = TOKENS // TOK_DEV
    quick_count = HEADS // 2
    slow_share = 0.5
    quick = quick_heads(key, quick_count)
    slow_block = jax.random.uniform(slow_key, (2, blocks_count, HEADS), jnp.float32) < slow_share
    quick_shift = jnp.where(slow_block, 6.0, -3.0)
    steady_shift = jax.random.uniform(steady_key, (2, blocks_count, HEADS), jnp.float32, -6.0, 1.5)
    head_shift = jnp.where(quick[None, None, :], quick_shift, steady_shift)
    channel_shift = jax.random.uniform(channel_key, (2, blocks_count, HEADS, HEAD), jnp.float32, -1.0, 1.0)
    shifted = (head_shift[:, :, :, None] + channel_shift).reshape(2, blocks_count, 1, channels)
    noise = jnp.clip(jax.random.normal(noise_key, (2, blocks_count, TOK_DEV, channels), jnp.float32), -6.0, 6.0)
    total = jnp.clip(shifted + noise, -7.5, 7.5)
    return total.reshape(2, TOKENS, channels).astype(jnp.bfloat16)


def draw_forget_slack(key, part):
    fast_key = jax.random.fold_in(jax.random.fold_in(key, 23), 1)
    slow_key = jax.random.fold_in(jax.random.fold_in(key, 23), 2)
    quick_count = HEADS // 2
    quick = quick_heads(key, quick_count)[:, None]
    quick_rate = jnp.exp(jax.random.uniform(fast_key, (HEADS, HEAD), jnp.float32, jnp.log(0.02), jnp.log(0.07)))
    steady_rate = jnp.exp(jax.random.uniform(slow_key, (HEADS, HEAD), jnp.float32, jnp.log(0.5), jnp.log(2.0))) / TOKENS
    return jnp.where(quick, quick_rate, steady_rate).reshape(HEADS * HEAD)


def draw_spike_log_forget(key, part):
    place_key, depth_key = jax.random.split(jax.random.fold_in(key, 37))
    spots = jax.random.randint(place_key, (4,), 0, TOKENS)
    upper = jnp.log(0.8)
    depths = jax.random.uniform(depth_key, (4, HEADS), jnp.float32, jnp.log(0.5), upper)
    hits = (jnp.arange(TOKENS)[:, None] == spots[None, :]).astype(jnp.float32)
    return jnp.dot(hits, depths)


def block_levels(stream_key, dims, pieces, least, top_value):
    def one(axis_at, parts):
        heights = jax.random.uniform(jax.random.fold_in(jax.random.fold_in(stream_key, 6), axis_at), (parts,), jnp.float32, least / len(pieces), top_value / len(pieces))
        return jnp.repeat(jnp.exp(heights), dims[axis_at] // parts).reshape((-1,) + (1,) * (len(dims) - axis_at - 1))

    gain = one(*pieces[0])
    for cut in pieces[1:]:
        gain = gain * one(*cut)
    return gain


def scatter_about(own_key, dims, spread, most, pieces=(), held_as=jnp.bfloat16):
    values = spread * jax.random.normal(own_key, dims, jnp.float32)
    if pieces:
        values = values * block_levels(own_key, dims, pieces, -0.22, 0.18)
    return jnp.clip(values, -most, most).astype(held_as)


def setup_inputs(seed: int = 0) -> dict:
    seeds = jax.random.split(jax.random.key(seed), 14)
    queries = scatter_about(seeds[0], (TOKENS, HEADS * HEAD), 1.0, 6.0, ((0, 64), (1, 4)))
    forget_logits = draw_forget_logits(jax.random.fold_in(seeds[13], 71), 0)
    value_matrix = scatter_about(seeds[2], (TOKENS, HEADS * HEAD), 1.0, 6.0, ((0, 64), (1, 4)))
    output_gate_logits = scatter_about(seeds[3], (TOKENS, HEADS * HEAD), 1.0, 6.0, ((0, 64), (1, 4)))
    forget_slack = draw_forget_slack(jax.random.fold_in(seeds[13], 71), 0)
    spike_log_forget = draw_spike_log_forget(jax.random.fold_in(seeds[13], 71), 0)
    head_norm_gain = jnp.clip(1.0 + 0.18 * jax.random.normal(seeds[6], (HEAD,), jnp.float32), 0.099609375, 1.8984375).astype(jnp.bfloat16)
    output_weight = scatter_about(seeds[7], (HEADS * HEAD, D), (HEADS * HEAD) ** -0.5, 0.125, ((0, 4),))
    residual = scatter_about(seeds[8], (TOKENS, D), 1.0, 6.0, ((0, 64),))
    mixer_norm_gain = jnp.clip(1.0 + 0.18 * jax.random.normal(seeds[9], (D,), jnp.float32), 0.099609375, 1.8984375).astype(jnp.bfloat16)
    mixer_gate_weight = scatter_about(seeds[10], (D, FF), D ** -0.5, 0.125, ((0, 64), (1, 4)))
    mixer_up_weight = scatter_about(seeds[11], (D, FF), D ** -0.5, 0.125, ((0, 64), (1, 4)))
    mixer_down_weight = scatter_about(seeds[12], (FF, D), FF ** -0.5, 0.078125, ((0, 4), (1, 64)))
    return dict(queries=queries, forget_logits=forget_logits, value_matrix=value_matrix, output_gate_logits=output_gate_logits, forget_slack=forget_slack, spike_log_forget=spike_log_forget, head_norm_gain=head_norm_gain, output_weight=output_weight, residual=residual, mixer_norm_gain=mixer_norm_gain, mixer_gate_weight=mixer_gate_weight, mixer_up_weight=mixer_up_weight, mixer_down_weight=mixer_down_weight)


NORM_EPS = 1e-06
BEST_PRECISION = lax.Precision.HIGHEST

def rms_scale(entries, gain_vec):
    return entries * lax.rsqrt(lax.optimization_barrier(jnp.mean(entries * entries, axis=-1, keepdims=True)) + NORM_EPS) * gain_vec.astype(jnp.float32)

def full_sweep(query_f, key_f, decay_f, value_f):
    total_rows, heads_all, head_width = query_f.shape
    blocks_count = total_rows // BLOCK
    tri_mask = jnp.tril(jnp.ones((BLOCK, BLOCK), bool))

    def to_blocks(tensor):
        return tensor.reshape(blocks_count, BLOCK, heads_all, head_width)

    def advance(state_now, segment):
        query_seg, key_seg, decay_seg, value_seg = segment
        running = jnp.cumsum(decay_seg, axis=0)
        query_scaled = query_seg * jnp.exp(running)
        key_scaled = key_seg * jnp.exp(-running)
        scores = jnp.einsum('thd,shd->hts', query_scaled, key_scaled, precision=BEST_PRECISION)
        scores = jnp.where(tri_mask[None], scores, 0.0)
        result = jnp.einsum('hts,shv->thv', scores, value_seg, precision=BEST_PRECISION)
        result = result + jnp.einsum('thd,hdv->thv', query_scaled, state_now, precision=BEST_PRECISION)
        final_log = running[-1]
        state_next = jnp.exp(final_log)[:, :, None] * state_now + jnp.einsum('shd,shv->hdv', key_seg * jnp.exp(final_log[None] - running), value_seg, precision=BEST_PRECISION)
        return (state_next, result)
    initial = jnp.zeros((heads_all, head_width, head_width), jnp.float32)
    _, results = lax.scan(advance, initial, (to_blocks(query_f), to_blocks(key_f), to_blocks(decay_f), to_blocks(value_f)))
    return results.reshape(total_rows, heads_all, head_width)

def reference(queries, forget_logits, value_matrix, output_gate_logits, forget_slack, spike_log_forget, head_norm_gain, output_weight, residual, mixer_norm_gain, mixer_gate_weight, mixer_up_weight, mixer_down_weight):
    total_rows = queries.shape[0]
    query_f = (jax.nn.silu(queries.astype(jnp.float32)) * HEAD ** (-0.5)).reshape(total_rows, HEADS, HEAD)
    value_f = value_matrix.astype(jnp.float32).reshape(total_rows, HEADS, HEAD)
    gate_random_key = (forget_slack * jax.nn.sigmoid(-forget_logits.astype(jnp.float32))).reshape(2, total_rows, HEADS, HEAD)
    decay_logarithm = jnp.log1p(-gate_random_key) + spike_log_forget[None, :, :, None]
    forward_out = full_sweep(query_f, gate_random_key[0], decay_logarithm[0], value_f)
    backward_out = jnp.flip(full_sweep(jnp.flip(query_f, 0), jnp.flip(gate_random_key[1], 0), jnp.flip(decay_logarithm[1], 0), jnp.flip(value_f, 0)), 0)
    mixture = forward_out + backward_out
    mixed = (rms_scale(mixture, head_norm_gain).reshape(total_rows, HEADS * HEAD) * jax.nn.silu(output_gate_logits.astype(jnp.float32))).astype(jnp.bfloat16)
    group_cols = HEADS * HEAD // N_TP
    summed = residual.astype(jnp.float32)
    for group_index in range(N_TP):
        low_col = group_index * group_cols
        partial_out = jnp.dot(mixed[:, low_col:low_col + group_cols], output_weight[low_col:low_col + group_cols], preferred_element_type=jnp.float32).astype(jnp.bfloat16)
        summed = summed + lax.optimization_barrier(partial_out).astype(jnp.float32)
    hidden_state = summed.astype(jnp.bfloat16)
    unit_cols = FF // N_TP

    def channel_mix(hidden_seg):
        normed = rms_scale(hidden_seg.astype(jnp.float32), mixer_norm_gain).astype(jnp.bfloat16)
        gate_act = jnp.dot(normed, mixer_gate_weight, preferred_element_type=jnp.float32)
        up_act = jnp.dot(normed, mixer_up_weight, preferred_element_type=jnp.float32)
        inner = (jax.nn.silu(gate_act) * up_act).astype(jnp.bfloat16)
        summed_seg = hidden_seg.astype(jnp.float32)
        for group_index in range(N_TP):
            low_unit = group_index * unit_cols
            lowered = jnp.dot(inner[:, low_unit:low_unit + unit_cols], mixer_down_weight[low_unit:low_unit + unit_cols], preferred_element_type=jnp.float32).astype(jnp.bfloat16)
            summed_seg = summed_seg + lax.optimization_barrier(lowered).astype(jnp.float32)
        return summed_seg.astype(jnp.bfloat16)
    hidden_blocks = hidden_state.reshape(total_rows // TOK_DEV, TOK_DEV, D)
    return lax.map(channel_mix, hidden_blocks).reshape(total_rows, D)
```

```python
import jax
import jax.numpy as jnp
from jax import lax
from jax.experimental import pallas as pl
from jax.experimental.pallas import tpu as pltpu
from jax.sharding import Mesh
from jax.sharding import PartitionSpec as P

SP = ("sp_0", "sp_1", "sp_2")
SP_TP = ("sp_0", "sp_1", "sp_2", "tp")
NORM_EPS = 1e-06
F32 = jnp.float32
BF16 = jnp.bfloat16
HEAD = 128


def nt_dot(a, b):
    return lax.dot_general(a, b, (((1,), (1,)), ((), ())), preferred_element_type=F32)


def tn_dot(a, b):
    return lax.dot_general(a, b, (((0,), (0,)), ((), ())), preferred_element_type=F32)


def in_three(a):
    high = a.astype(BF16)
    rest = a - high.astype(F32)
    middle = rest.astype(BF16)
    return high, middle, (rest - middle.astype(F32)).astype(BF16)


def local_body(q_ref, f_ref, v_ref, slack_ref, spike_ref, send_ref, near_ref, reach_ref):
    rows = q_ref.shape[0]
    heads = spike_ref.shape[1]
    chunk = send_ref.shape[1] - 8
    pieces = HEAD // chunk
    at_row = lax.broadcasted_iota(jnp.int32, (rows, rows), 0)
    at_col = lax.broadcasted_iota(jnp.int32, (rows, rows), 1)
    for h in range(heads):
        cols = slice(h * HEAD, (h + 1) * HEAD)
        q = q_ref[:, cols].astype(F32)
        q = q * jax.nn.sigmoid(q) * HEAD ** (-0.5)
        v = v_ref[:, cols]
        scores = jnp.zeros((rows, rows), F32)
        for w in range(2):
            keep = at_row >= at_col if w == 0 else at_row <= at_col
            key = slack_ref[:, cols] * jax.nn.sigmoid(-f_ref[w, :, cols].astype(F32))
            decay = jnp.log1p(-key) + spike_ref[:, h : h + 1]
            ones = keep.astype(BF16)
            high, middle, low = in_three(decay)
            running = (
                jnp.dot(ones, low, preferred_element_type=F32)
                + jnp.dot(ones, middle, preferred_element_type=F32)
                + jnp.dot(ones, high, preferred_element_type=F32)
            )
            final = running[rows - 1 : rows] if w == 0 else running[0:1]
            q_scaled = (q * jnp.exp(running)).astype(BF16)
            k_scaled = (key * jnp.exp(-running)).astype(BF16)
            scores = scores + jnp.where(keep, nt_dot(q_scaled, k_scaled), 0.0)
            k_end = (key * jnp.exp(final - running)).astype(BF16)
            state = tn_dot(v, k_end).astype(BF16)
            reach_ref[w, :, cols] = q_scaled
            at = (w * heads + h) * pieces
            send_ref[at : at + pieces, 0:chunk, :] = state.reshape(pieces, chunk, HEAD)
            total = jnp.concatenate([t.astype(F32) for t in in_three(jnp.exp(final))], axis=0)
            total = jnp.concatenate([total, jnp.zeros((5, HEAD), F32)], axis=0).astype(BF16)
            send_ref[at : at + pieces, chunk : chunk + 8, :] = jnp.broadcast_to(
                total[None], (pieces, 8, HEAD)
            )
        near_ref[:, cols] = jnp.dot(scores.astype(BF16), v, preferred_element_type=F32)


def scan_body(back_ref, got_ref, give_ref):
    blocks, wide, _ = got_ref.shape
    chunk = wide - 8
    back = back_ref[0]
    state = jnp.zeros((chunk, HEAD), F32)
    for b in range(blocks):
        at = jnp.where(back == 1, blocks - 1 - b, b)
        give_ref[at] = state.astype(BF16)
        piece = got_ref[at].astype(F32)
        total = piece[chunk : chunk + 1] + piece[chunk + 1 : chunk + 2] + piece[chunk + 2 : chunk + 3]
        state = total * state + piece[0:chunk]


def project_body(
    own_ref, near_ref, reach_ref, enter_ref, gate_ref, gain_ref, weight_ref, o0, o1, o2, o3, mixed_ref
):
    heads = near_ref.shape[1] // HEAD
    gain = gain_ref[...].astype(F32)
    for h in range(heads):
        cols = slice(h * HEAD, (h + 1) * HEAD)
        mix = near_ref[:, cols]
        mix = mix + nt_dot(reach_ref[0, :, cols], enter_ref[h])
        mix = mix + nt_dot(reach_ref[1, :, cols], enter_ref[heads + h])
        scale = lax.rsqrt(jnp.mean(mix * mix, axis=-1, keepdims=True) + NORM_EPS)
        g = gate_ref[:, cols].astype(F32)
        mixed_ref[:, cols] = (mix * scale * gain * (g * jax.nn.sigmoid(g))).astype(BF16)
    outs = (o0, o1, o2, o3)
    part = o0.shape[0]
    own = own_ref[0]
    for d in range(len(outs)):
        at = pl.multiple_of(lax.rem(own + d, len(outs)) * part, part)
        outs[d][...] = jnp.dot(
            mixed_ref[pl.ds(at, part), :], weight_ref[...], preferred_element_type=F32
        ).astype(BF16)


VMEM = pl.BlockSpec(memory_space=pltpu.VMEM)
SMEM = pl.BlockSpec(memory_space=pltpu.SMEM)


def shift(array, axis, by):
    size = lax.axis_size(axis)
    return lax.ppermute(array, axis, [(k, (k + by) % size) for k in range(size)])


def local(
    queries,
    forget_logits,
    value_matrix,
    output_gate_logits,
    forget_slack,
    spike_log_forget,
    head_norm_gain,
    output_weight,
    residual,
    mixer_norm_gain,
    mixer_gate_weight,
    mixer_up_weight,
    mixer_down_weight,
):
    rows, width = queries.shape
    heads = spike_log_forget.shape[1]
    model = output_weight.shape[1]
    hidden = mixer_gate_weight.shape[1]
    blocks = lax.axis_size(SP)
    n_tp = lax.axis_size("tp")
    sp_at = lax.axis_index(SP)
    tp_at = lax.axis_index("tp")
    chunk = 2 * heads * HEAD // blocks

    packed = jnp.concatenate([mixer_gate_weight, mixer_up_weight, mixer_down_weight.T], axis=1)
    whole = lax.all_gather(packed, SP, axis=0, tiled=True)

    send, near, reach = pl.pallas_call(
        local_body,
        out_shape=(
            jax.ShapeDtypeStruct((blocks, chunk + 8, HEAD), BF16),
            jax.ShapeDtypeStruct((rows, width), F32),
            jax.ShapeDtypeStruct((2, rows, width), BF16),
        ),
        in_specs=[VMEM] * 5,
        out_specs=(VMEM,) * 3,
        name="local_sweep",
    )(queries, forget_logits, value_matrix, forget_slack[None], spike_log_forget)
    got = lax.all_to_all(send, SP, 0, 0, tiled=True)
    give = pl.pallas_call(
        scan_body,
        out_shape=jax.ShapeDtypeStruct((blocks, chunk, HEAD), BF16),
        in_specs=[SMEM, VMEM],
        out_specs=VMEM,
        name="block_scan",
    )((sp_at >= blocks // 2).astype(jnp.int32)[None], got)
    enter = lax.all_to_all(give, SP, 0, 0, tiled=True).reshape(2 * heads, HEAD, HEAD)

    part = rows // n_tp
    parts = pl.pallas_call(
        project_body,
        out_shape=(jax.ShapeDtypeStruct((part, model), BF16),) * n_tp,
        in_specs=[SMEM] + [VMEM] * 6,
        out_specs=(VMEM,) * n_tp,
        scratch_shapes=[pltpu.VMEM((rows, width), BF16)],
        name="norm_project",
    )(tp_at[None], near, reach, enter, output_gate_logits, head_norm_gain[None], output_weight)

    arrived = [parts[0]] + [shift(parts[d], "tp", d) for d in range(1, n_tp)]
    own_resid = lax.dynamic_slice_in_dim(residual, tp_at * part, part, 0)
    hidden_f = own_resid.astype(F32)
    for a in arrived:
        hidden_f = hidden_f + a.astype(F32)
    hidden_state = hidden_f.astype(BF16)
    held = hidden_state.astype(F32)
    normed = (
        held
        * lax.rsqrt(jnp.mean(held * held, axis=-1, keepdims=True) + NORM_EPS)
        * mixer_norm_gain.astype(F32)
    ).astype(BF16)
    everyone = jnp.concatenate([normed] + [shift(normed, "tp", d) for d in range(1, n_tp)], axis=0)
    gate_act = jnp.dot(everyone, whole[:, :hidden], preferred_element_type=F32)
    up_act = jnp.dot(everyone, whole[:, hidden : 2 * hidden], preferred_element_type=F32)
    inner = (jax.nn.silu(gate_act) * up_act).astype(BF16)
    lowered = nt_dot(inner, whole[:, 2 * hidden :]).astype(BF16)
    out = hidden_state.astype(F32) + lowered[:part].astype(F32)
    for d in range(1, n_tp):
        out = out + shift(lowered[d * part : (d + 1) * part], "tp", n_tp - d).astype(F32)
    return out.astype(BF16)


def solution(mesh):
    torus = Mesh(mesh.devices.reshape(8, 4, 2, mesh.shape["tp"]), ("sp_0", "sp_1", "sp_2", "tp"))
    return jax.shard_map(
        local,
        mesh=torus,
        in_specs=(
            P(SP, "tp"),
            P(None, SP, "tp"),
            P(SP, "tp"),
            P(SP, "tp"),
            P("tp"),
            P(SP, "tp"),
            P(),
            P("tp", None),
            P(SP, None),
            P(),
            P(SP, "tp"),
            P(SP, "tp"),
            P("tp", SP),
        ),
        out_specs=P(SP_TP, None),
        check_vma=False,
    )
```

```python
import jax
import jax.numpy as jnp
from jax import lax
from jax.experimental import pallas as pl
from jax.experimental.pallas import tpu as pltpu
from jax.sharding import Mesh
from jax.sharding import PartitionSpec as P

SP = ("sp_0", "y_hi", "y_lo", "sp_2")
SP_TP = SP + ("tp",)
WEIGHTS = ("sp_0", "y_hi", "sp_2")
NORM_EPS = 1e-06
F32 = jnp.float32
BF16 = jnp.bfloat16
HEAD = 128


def nt_dot(a, b):
    return lax.dot_general(a, b, (((1,), (1,)), ((), ())), preferred_element_type=F32)


def tn_dot(a, b):
    return lax.dot_general(a, b, (((0,), (0,)), ((), ())), preferred_element_type=F32)


def in_three(a):
    high = a.astype(BF16)
    rest = a - high.astype(F32)
    middle = rest.astype(BF16)
    return high, middle, (rest - middle.astype(F32)).astype(BF16)


def local_body(q_ref, f_ref, v_ref, slack_ref, spike_ref, send_ref, near_ref, reach_ref):
    rows = q_ref.shape[0]
    heads = spike_ref.shape[0]
    chunk = send_ref.shape[1] - 8
    pieces = HEAD // chunk
    at_row = lax.broadcasted_iota(jnp.int32, (rows, rows), 0)
    at_col = lax.broadcasted_iota(jnp.int32, (rows, rows), 1)
    spikes = []
    for w in range(2):
        keep = at_row >= at_col if w == 0 else at_row <= at_col
        ones = keep.astype(BF16)
        high, middle, low = in_three(spike_ref[...])
        spikes.append(nt_dot(ones, low) + nt_dot(ones, middle) + nt_dot(ones, high))
    for h in range(heads):
        cols = slice(h * HEAD, (h + 1) * HEAD)
        q = q_ref[:, cols].astype(F32)
        q = q * jax.nn.sigmoid(q) * HEAD ** (-0.5)
        v = v_ref[:, cols]
        scores = jnp.zeros((rows, rows), F32)
        for w in range(2):
            keep = at_row >= at_col if w == 0 else at_row <= at_col
            key = slack_ref[:, cols] * jax.nn.sigmoid(-f_ref[w, :, cols].astype(F32))
            decay = jnp.log1p(-key)
            ones = keep.astype(BF16)
            high, middle, low = in_three(decay)
            running = (
                jnp.dot(ones, low, preferred_element_type=F32)
                + jnp.dot(ones, middle, preferred_element_type=F32)
                + jnp.dot(ones, high, preferred_element_type=F32)
                + spikes[w][:, h : h + 1]
            )
            final = running[rows - 1 : rows] if w == 0 else running[0:1]
            q_scaled = (q * jnp.exp(running)).astype(BF16)
            k_scaled = (key * jnp.exp(-running)).astype(BF16)
            scores = scores + jnp.where(keep, nt_dot(q_scaled, k_scaled), 0.0)
            k_end = (key * jnp.exp(final - running)).astype(BF16)
            state = tn_dot(v, k_end).astype(BF16)
            reach_ref[w, :, cols] = q_scaled
            at = (w * heads + h) * pieces
            send_ref[at : at + pieces, 0:chunk, :] = state.reshape(pieces, chunk, HEAD)
            total = jnp.concatenate([t.astype(F32) for t in in_three(jnp.exp(final))], axis=0)
            total = jnp.concatenate([total, jnp.zeros((5, HEAD), F32)], axis=0).astype(BF16)
            send_ref[at : at + pieces, chunk : chunk + 8, :] = jnp.broadcast_to(
                total[None], (pieces, 8, HEAD)
            )
        near_ref[:, cols] = jnp.dot(scores.astype(BF16), v, preferred_element_type=F32)


def scan_body(back_ref, got_ref, give_ref):
    blocks, wide, _ = got_ref.shape
    chunk = wide - 8
    back = back_ref[0]
    state = jnp.zeros((chunk, HEAD), F32)
    for b in range(blocks):
        at = jnp.where(back == 1, blocks - 1 - b, b)
        give_ref[at] = state.astype(BF16)
        piece = got_ref[at].astype(F32)
        total = piece[chunk : chunk + 1] + piece[chunk + 1 : chunk + 2] + piece[chunk + 2 : chunk + 3]
        state = total * state + piece[0:chunk]


def project_body(
    own_ref, near_ref, reach_ref, enter_ref, gate_ref, gain_ref, weight_ref, o0, o1, o2, o3, mixed_ref
):
    heads = near_ref.shape[1] // HEAD
    gain = gain_ref[...].astype(F32)
    for h in range(heads):
        cols = slice(h * HEAD, (h + 1) * HEAD)
        mix = near_ref[:, cols]
        mix = mix + nt_dot(reach_ref[0, :, cols], enter_ref[h])
        mix = mix + nt_dot(reach_ref[1, :, cols], enter_ref[heads + h])
        scale = lax.rsqrt(jnp.mean(mix * mix, axis=-1, keepdims=True) + NORM_EPS)
        g = gate_ref[:, cols].astype(F32)
        mixed_ref[:, cols] = (mix * scale * gain * (g * jax.nn.sigmoid(g))).astype(BF16)
    outs = (o0, o1, o2, o3)
    part = o0.shape[0]
    own = own_ref[0]
    for d in range(len(outs)):
        at = pl.multiple_of(lax.rem(own + d, len(outs)) * part, part)
        outs[d][...] = jnp.dot(
            mixed_ref[pl.ds(at, part), :], weight_ref[...], preferred_element_type=F32
        ).astype(BF16)


VMEM = pl.BlockSpec(memory_space=pltpu.VMEM)
SMEM = pl.BlockSpec(memory_space=pltpu.SMEM)


def shift(array, axis, by):
    size = lax.axis_size(axis)
    return lax.ppermute(array, axis, [(k, (k + by) % size) for k in range(size)])


def local(
    queries,
    forget_logits,
    value_matrix,
    output_gate_logits,
    forget_slack,
    spike_log_forget,
    head_norm_gain,
    output_weight,
    residual,
    mixer_norm_gain,
    mixer_gate_weight,
    mixer_up_weight,
    mixer_down_weight,
):
    rows, width = queries.shape
    heads = spike_log_forget.shape[1]
    model = output_weight.shape[1]
    hidden = mixer_gate_weight.shape[1]
    blocks = lax.axis_size(SP)
    n_tp = lax.axis_size("tp")
    sp_at = lax.axis_index(SP)
    tp_at = lax.axis_index("tp")
    chunk = 2 * heads * HEAD // blocks
    half = (hidden // 2 + HEAD - 1) // HEAD * HEAD

    low, high = [], []
    for weight in (mixer_gate_weight, mixer_up_weight, mixer_down_weight.T):
        low.append(weight[:, :half])
        high.append(jnp.pad(weight[:, half:], ((0, 0), (0, 2 * half - hidden))))
    low, high = jnp.concatenate(low, axis=1), jnp.concatenate(high, axis=1)
    y_at = lax.axis_index("y_lo")
    core_at = lax.axis_index("sp_2")
    pairs = [(a, b) for a in range(2) for b in range(2)]
    same = lax.ppermute(
        jnp.where(core_at == 0, low, high), ("y_lo", "sp_2"), [(2 * a + b, 2 * b + a) for a, b in pairs]
    )
    other = lax.ppermute(
        jnp.where(core_at == 0, high, low),
        ("y_lo", "sp_2"),
        [(2 * a + b, 2 * (1 - b) + a) for a, b in pairs],
    )
    packed = jnp.concatenate(
        [jnp.where(y_at == 0, same, other), jnp.where(y_at == 0, other, same)], axis=0
    )
    whole = lax.all_gather(packed, WEIGHTS, axis=0, tiled=True)

    send, near, reach = pl.pallas_call(
        local_body,
        out_shape=(
            jax.ShapeDtypeStruct((blocks, chunk + 8, HEAD), BF16),
            jax.ShapeDtypeStruct((rows, width), F32),
            jax.ShapeDtypeStruct((2, rows, width), BF16),
        ),
        in_specs=[VMEM] * 5,
        out_specs=(VMEM,) * 3,
        name="local_sweep",
    )(queries, forget_logits, value_matrix, forget_slack[None], spike_log_forget.T)
    got = lax.all_to_all(send, SP, 0, 0, tiled=True)
    give = pl.pallas_call(
        scan_body,
        out_shape=jax.ShapeDtypeStruct((blocks, chunk, HEAD), BF16),
        in_specs=[SMEM, VMEM],
        out_specs=VMEM,
        name="block_scan",
    )((sp_at >= blocks // 2).astype(jnp.int32)[None], got)
    enter = lax.all_to_all(give, SP, 0, 0, tiled=True).reshape(2 * heads, HEAD, HEAD)

    part = rows // n_tp
    parts = pl.pallas_call(
        project_body,
        out_shape=(jax.ShapeDtypeStruct((part, model), BF16),) * n_tp,
        in_specs=[SMEM] + [VMEM] * 6,
        out_specs=(VMEM,) * n_tp,
        scratch_shapes=[pltpu.VMEM((rows, width), BF16)],
        name="norm_project",
    )(tp_at[None], near, reach, enter, output_gate_logits, head_norm_gain[None], output_weight)

    arrived = [parts[0]] + [shift(parts[d], "tp", d) for d in range(1, n_tp)]
    own_resid = lax.dynamic_slice_in_dim(residual, tp_at * part, part, 0)
    hidden_f = own_resid.astype(F32)
    for a in arrived:
        hidden_f = hidden_f + a.astype(F32)
    hidden_state = hidden_f.astype(BF16)
    held = hidden_state.astype(F32)
    normed = (
        held
        * lax.rsqrt(jnp.mean(held * held, axis=-1, keepdims=True) + NORM_EPS)
        * mixer_norm_gain.astype(F32)
    ).astype(BF16)
    both = jnp.concatenate([normed, shift(normed, "y_lo", 1)], axis=0)
    everyone = jnp.concatenate([both] + [shift(both, "tp", d) for d in range(1, n_tp)], axis=0)
    gate_act = jnp.dot(everyone, whole[:, :half], preferred_element_type=F32)
    up_act = jnp.dot(everyone, whole[:, half : 2 * half], preferred_element_type=F32)
    inner = (jax.nn.silu(gate_act) * up_act).astype(BF16)
    lowered = nt_dot(inner, whole[:, 2 * half :]).astype(BF16)
    span = 2 * part
    summed = lowered[:span].astype(F32)
    for d in range(1, n_tp):
        summed = summed + shift(lowered[d * span : (d + 1) * span], "tp", n_tp - d).astype(F32)
    theirs = shift(summed[part:].astype(BF16), "y_lo", 1)
    return (hidden_state.astype(F32) + summed[:part] + theirs.astype(F32)).astype(BF16)


def solution(mesh):
    torus = Mesh(mesh.devices.reshape(8, 2, 2, 2, mesh.shape["tp"]), SP_TP)
    return jax.shard_map(
        local,
        mesh=torus,
        in_specs=(
            P(SP, "tp"),
            P(None, SP, "tp"),
            P(SP, "tp"),
            P(SP, "tp"),
            P("tp"),
            P(SP, "tp"),
            P(),
            P("tp", None),
            P(SP, None),
            P(),
            P(SP, "tp"),
            P(SP, "tp"),
            P("tp", SP),
        ),
        out_specs=P(SP_TP, None),
        check_vma=False,
    )
```

```python
import jax
import jax.numpy as jnp
from jax import lax
from jax.experimental import pallas as pl
from jax.experimental.pallas import tpu as pltpu
from jax.sharding import Mesh
from jax.sharding import PartitionSpec as P

SP = ("z_hi", "z_lo", "y", "core")
SP_TP = SP + ("tp",)
NORM_EPS = 1e-06
F32 = jnp.float32
BF16 = jnp.bfloat16
HEAD = 128


def nt_dot(a, b):
    return lax.dot_general(a, b, (((1,), (1,)), ((), ())), preferred_element_type=F32)


def tn_dot(a, b):
    return lax.dot_general(a, b, (((0,), (0,)), ((), ())), preferred_element_type=F32)


def in_three(a):
    high = a.astype(BF16)
    rest = a - high.astype(F32)
    middle = rest.astype(BF16)
    return high, middle, (rest - middle.astype(F32)).astype(BF16)


def local_body(q_ref, f_ref, v_ref, slack_ref, spike_ref, send_ref, near_ref, reach_ref):
    rows = q_ref.shape[0]
    heads = spike_ref.shape[0]
    chunk = send_ref.shape[1] - 8
    pieces = HEAD // chunk
    at_row = lax.broadcasted_iota(jnp.int32, (rows, rows), 0)
    at_col = lax.broadcasted_iota(jnp.int32, (rows, rows), 1)
    spikes = []
    for w in range(2):
        keep = at_row >= at_col if w == 0 else at_row <= at_col
        ones = keep.astype(BF16)
        high, middle, low = in_three(spike_ref[...])
        spikes.append(nt_dot(ones, low) + nt_dot(ones, middle) + nt_dot(ones, high))
    for h in range(heads):
        cols = slice(h * HEAD, (h + 1) * HEAD)
        q = q_ref[:, cols].astype(F32)
        q = q * jax.nn.sigmoid(q) * HEAD ** (-0.5)
        v = v_ref[:, cols]
        scores = jnp.zeros((rows, rows), F32)
        for w in range(2):
            keep = at_row >= at_col if w == 0 else at_row <= at_col
            key = slack_ref[:, cols] * jax.nn.sigmoid(-f_ref[w, :, cols].astype(F32))
            decay = jnp.log1p(-key)
            ones = keep.astype(BF16)
            high, middle, low = in_three(decay)
            running = (
                jnp.dot(ones, low, preferred_element_type=F32)
                + jnp.dot(ones, middle, preferred_element_type=F32)
                + jnp.dot(ones, high, preferred_element_type=F32)
                + spikes[w][:, h : h + 1]
            )
            final = running[rows - 1 : rows] if w == 0 else running[0:1]
            q_scaled = (q * jnp.exp(running)).astype(BF16)
            k_scaled = (key * jnp.exp(-running)).astype(BF16)
            scores = scores + jnp.where(keep, nt_dot(q_scaled, k_scaled), 0.0)
            k_end = (key * jnp.exp(final - running)).astype(BF16)
            state = tn_dot(v, k_end).astype(BF16)
            reach_ref[w, :, cols] = q_scaled
            at = (w * heads + h) * pieces
            send_ref[at : at + pieces, 0:chunk, :] = state.reshape(pieces, chunk, HEAD)
            total = jnp.concatenate([t.astype(F32) for t in in_three(jnp.exp(final))], axis=0)
            total = jnp.concatenate([total, jnp.zeros((5, HEAD), F32)], axis=0).astype(BF16)
            send_ref[at : at + pieces, chunk : chunk + 8, :] = jnp.broadcast_to(
                total[None], (pieces, 8, HEAD)
            )
        near_ref[:, cols] = jnp.dot(scores.astype(BF16), v, preferred_element_type=F32)


def scan_body(back_ref, got_ref, give_ref):
    blocks, wide, _ = got_ref.shape
    chunk = wide - 8
    back = back_ref[0]
    state = jnp.zeros((chunk, HEAD), F32)
    for b in range(blocks):
        at = jnp.where(back == 1, blocks - 1 - b, b)
        give_ref[at] = state.astype(BF16)
        piece = got_ref[at].astype(F32)
        total = piece[chunk : chunk + 1] + piece[chunk + 1 : chunk + 2] + piece[chunk + 2 : chunk + 3]
        state = total * state + piece[0:chunk]


def project_body(
    own_ref, near_ref, reach_ref, enter_ref, gate_ref, gain_ref, weight_ref, o0, o1, o2, o3, mixed_ref
):
    heads = near_ref.shape[1] // HEAD
    gain = gain_ref[...].astype(F32)
    for h in range(heads):
        cols = slice(h * HEAD, (h + 1) * HEAD)
        mix = near_ref[:, cols]
        mix = mix + nt_dot(reach_ref[0, :, cols], enter_ref[h])
        mix = mix + nt_dot(reach_ref[1, :, cols], enter_ref[heads + h])
        scale = lax.rsqrt(jnp.mean(mix * mix, axis=-1, keepdims=True) + NORM_EPS)
        g = gate_ref[:, cols].astype(F32)
        mixed_ref[:, cols] = (mix * scale * gain * (g * jax.nn.sigmoid(g))).astype(BF16)
    outs = (o0, o1, o2, o3)
    part = o0.shape[0]
    own = own_ref[0]
    for d in range(len(outs)):
        at = pl.multiple_of(lax.rem(own + d, len(outs)) * part, part)
        outs[d][...] = jnp.dot(
            mixed_ref[pl.ds(at, part), :], weight_ref[...], preferred_element_type=F32
        ).astype(BF16)


def halves_body(core_ref, gate_ref, up_ref, down_ref, keep_ref, give_ref):
    hidden = gate_ref.shape[1]
    width = keep_ref.shape[1] // 3

    def write(out_ref, start):
        for k, ref in enumerate((gate_ref, up_ref, down_ref)):
            out_ref[:, k * width : (k + 1) * width] = ref[:, start : start + width]

    @pl.when(core_ref[0] == 0)
    def _():
        write(keep_ref, 0)
        write(give_ref, hidden - width)

    @pl.when(core_ref[0] != 0)
    def _():
        write(keep_ref, hidden - width)
        write(give_ref, 0)


def mixer_body(
    at_ref, own_ref, theirs_ref, *refs, hidden
):
    pieces, (mine_ref, give_ref, tokens_ref, weights_ref, sems) = refs[:8], refs[8:]
    z_hi, y, core, x = at_ref[0], at_ref[1], at_ref[2], at_ref[3]
    step = jnp.where(core == 0, 1, 3)
    copies = []
    for color in range(2):
        row_core = core if color == 0 else 1 - core
        for s in range(4):
            moved = lax.rem((x if color == 0 else y) + 4 - lax.rem(step * s, 4), 4)
            for k in range(4):
                turned = lax.rem((y if color == 0 else x) + 4 - k, 4)
                at_x, at_y = (moved, turned) if color == 0 else (turned, moved)
                for j in range(2):
                    at_z = z_hi if j == 0 else 1 - z_hi
                    index = (color * 4 + s) * 8 + k * 2 + j
                    copies.append(
                        pltpu.make_async_copy(
                            pieces[color * 4 + s].at[k, j],
                            weights_ref.at[at_z, at_x, at_y, row_core],
                            sems.at[index],
                        )
                    )
    for copy in copies:
        copy.start()
    rows = own_ref.shape[0]
    tokens_ref[0:rows, :] = own_ref[...]
    tokens_ref[rows : 2 * rows, :] = theirs_ref[...]
    for copy in copies:
        copy.wait()
    model = tokens_ref.shape[1]
    wide = weights_ref.shape[5]
    width = wide // 3
    weights = weights_ref.reshape(model, wide)
    act = jnp.dot(tokens_ref[...], weights[:, : 2 * width], preferred_element_type=F32)
    gate, up = act[:, :width], act[:, width:]
    inner = gate * jax.nn.sigmoid(gate) * up
    lane = lax.broadcasted_iota(jnp.int32, inner.shape, 1)
    low = jnp.where(core == 0, 0, width - hidden // 2)
    inner = jnp.where((lane >= low) & (lane < low + hidden // 2), inner, 0.0).astype(BF16)
    lowered = nt_dot(inner, weights[:, 2 * width :])
    mine_ref[...] = lowered[:rows]
    give_ref[...] = lowered[rows:].astype(BF16)


VMEM = pl.BlockSpec(memory_space=pltpu.VMEM)
SMEM = pl.BlockSpec(memory_space=pltpu.SMEM)
ANY = pl.BlockSpec(memory_space=pl.ANY)


def shift(array, axis, by):
    size = lax.axis_size(axis)
    return lax.ppermute(array, axis, [(k, (k + by) % size) for k in range(size)])


def local(
    queries,
    forget_logits,
    value_matrix,
    output_gate_logits,
    forget_slack,
    spike_log_forget,
    head_norm_gain,
    output_weight,
    residual,
    mixer_norm_gain,
    mixer_gate_weight,
    mixer_up_weight,
    mixer_down_weight,
):
    rows, width = queries.shape
    heads = spike_log_forget.shape[1]
    model = output_weight.shape[1]
    hidden = mixer_gate_weight.shape[1]
    blocks = lax.axis_size(SP)
    n_tp = lax.axis_size("tp")
    sp_at = lax.axis_index(SP)
    tp_at = lax.axis_index("tp")
    core_at = lax.axis_index("core")
    chunk = 2 * heads * HEAD // blocks
    half = (hidden // 2 + HEAD - 1) // HEAD * HEAD
    slab = mixer_gate_weight.shape[0]

    halves = pl.pallas_call(
        halves_body,
        out_shape=(jax.ShapeDtypeStruct((slab, 3 * half), BF16),) * 2,
        in_specs=[SMEM] + [VMEM] * 3,
        out_specs=(VMEM,) * 2,
        name="weight_halves",
    )(core_at[None], mixer_gate_weight, mixer_up_weight, mixer_down_weight.T)

    def to_quads(array, i, j):
        moves = []
        for z_hi in range(2):
            for z_lo in range(4):
                for c in range(2):
                    for x in range(4):
                        start = ((z_hi * 4 + z_lo) * 2 + c) * 4 + x
                        stop = (((z_hi ^ j) * 4 + x) * 2 + (c ^ i)) * 4 + z_lo
                        moves.append((start, stop))
        return lax.ppermute(array, ("z_hi", "z_lo", "core", "tp"), moves)

    quads = [[to_quads(halves[i], i, j) for j in range(2)] for i in range(2)]
    send, near, reach = pl.pallas_call(
        local_body,
        out_shape=(
            jax.ShapeDtypeStruct((blocks, chunk + 8, HEAD), BF16),
            jax.ShapeDtypeStruct((rows, width), F32),
            jax.ShapeDtypeStruct((2, rows, width), BF16),
        ),
        in_specs=[VMEM] * 5,
        out_specs=(VMEM,) * 3,
        name="local_sweep",
    )(queries, forget_logits, value_matrix, forget_slack[None], spike_log_forget.T)
    quads, send = lax.optimization_barrier((quads, send))
    slabs = [jnp.stack(pair) for pair in quads]
    pieces = []
    for i, (first, second) in enumerate((("y", "tp"), ("tp", "y"))):
        line = jnp.stack([slabs[i]] + [shift(slabs[i], first, d) for d in range(1, 4)])
        pieces.append(line)
        size = lax.axis_size(second)
        axes = (second, "core") if second == "y" else ("core", second)
        moves = []
        for k in range(size):
            for c in range(2):
                to = (k + (1 if c == 0 else size - 1)) % size
                moves.append((k * 2 + c, to * 2 + c) if second == "y" else (c * size + k, c * size + to))
        for _ in range(size - 1):
            line = lax.ppermute(line, axes, moves)
            pieces.append(line)

    got = lax.all_to_all(send, SP, 0, 0, tiled=True)
    give = pl.pallas_call(
        scan_body,
        out_shape=jax.ShapeDtypeStruct((blocks, chunk, HEAD), BF16),
        in_specs=[SMEM, VMEM],
        out_specs=VMEM,
        name="block_scan",
    )((sp_at >= blocks // 2).astype(jnp.int32)[None], got)
    enter = lax.all_to_all(give, SP, 0, 0, tiled=True).reshape(2 * heads, HEAD, HEAD)

    part = rows // n_tp
    parts = pl.pallas_call(
        project_body,
        out_shape=(jax.ShapeDtypeStruct((part, model), BF16),) * n_tp,
        in_specs=[SMEM] + [VMEM] * 6,
        out_specs=(VMEM,) * n_tp,
        scratch_shapes=[pltpu.VMEM((rows, width), BF16)],
        name="norm_project",
    )(tp_at[None], near, reach, enter, output_gate_logits, head_norm_gain[None], output_weight)

    arrived = [parts[0]] + [shift(parts[d], "tp", d) for d in range(1, n_tp)]
    own_resid = lax.dynamic_slice_in_dim(residual, tp_at * part, part, 0)
    hidden_f = own_resid.astype(F32)
    for a in arrived:
        hidden_f = hidden_f + a.astype(F32)
    hidden_state = hidden_f.astype(BF16)
    held = hidden_state.astype(F32)
    normed = (
        held
        * lax.rsqrt(jnp.mean(held * held, axis=-1, keepdims=True) + NORM_EPS)
        * mixer_norm_gain.astype(F32)
    ).astype(BF16)
    quad = lax.axis_size("z_lo")
    own = jnp.concatenate([normed] + [shift(normed, "z_lo", d) for d in range(1, quad)], axis=0)
    theirs = shift(own, "core", 1)
    at = jnp.stack([lax.axis_index("z_hi"), lax.axis_index("y"), core_at, tp_at])
    mine, other = pl.pallas_call(
        lambda *refs: mixer_body(*refs, hidden=hidden),
        out_shape=(
            jax.ShapeDtypeStruct((quad * part, model), F32),
            jax.ShapeDtypeStruct((quad * part, model), BF16),
        ),
        in_specs=[SMEM, VMEM, VMEM] + [ANY] * 8,
        out_specs=(VMEM, VMEM),
        scratch_shapes=[
            pltpu.VMEM((2 * quad * part, model), BF16),
            pltpu.VMEM((2, 4, 4, 2, slab, 3 * half), BF16),
            pltpu.SemaphoreType.DMA((64,)),
        ],
        compiler_params=pltpu.CompilerParams(vmem_limit_bytes=48 * 1024 * 1024),
        name="channel_mixer",
    )(at, own, theirs, *pieces)
    lowered = mine + shift(other, "core", 1).astype(F32)
    out = hidden_state.astype(F32) + lowered[:part]
    for d in range(1, quad):
        back = lowered[d * part : (d + 1) * part].astype(BF16)
        out = out + shift(back, "z_lo", quad - d).astype(F32)
    return out.astype(BF16)


def solution(mesh):
    torus = Mesh(mesh.devices.reshape(2, 4, 4, 2, mesh.shape["tp"]), SP_TP)
    return jax.shard_map(
        local,
        mesh=torus,
        in_specs=(
            P(SP, "tp"),
            P(None, SP, "tp"),
            P(SP, "tp"),
            P(SP, "tp"),
            P("tp"),
            P(SP, "tp"),
            P(),
            P("tp", None),
            P(SP, None),
            P(),
            P(SP, "tp"),
            P(SP, "tp"),
            P("tp", SP),
        ),
        out_specs=P(SP_TP, None),
        check_vma=False,
    )
```

```python
import jax
import jax.numpy as jnp
from jax import lax
from jax.experimental import pallas as pl
from jax.experimental.pallas import tpu as pltpu
from jax.sharding import Mesh
from jax.sharding import PartitionSpec as P

SP = ("sp_0", "sp_1", "sp_2")
SP_TP = ("sp_0", "sp_1", "sp_2", "tp")
NORM_EPS = 1e-06
F32 = jnp.float32
BF16 = jnp.bfloat16
HEAD = 128


def nt_dot(a, b):
    return lax.dot_general(a, b, (((1,), (1,)), ((), ())), preferred_element_type=F32)


def tn_dot(a, b):
    return lax.dot_general(a, b, (((0,), (0,)), ((), ())), preferred_element_type=F32)


def in_three(a):
    high = a.astype(BF16)
    rest = a - high.astype(F32)
    middle = rest.astype(BF16)
    return high, middle, (rest - middle.astype(F32)).astype(BF16)


def local_body(q_ref, f_ref, v_ref, slack_ref, spike_ref, send_ref, near_ref, reach_ref):
    rows = q_ref.shape[0]
    heads = spike_ref.shape[0]
    chunk = send_ref.shape[1] - 8
    pieces = HEAD // chunk
    at_row = lax.broadcasted_iota(jnp.int32, (rows, rows), 0)
    at_col = lax.broadcasted_iota(jnp.int32, (rows, rows), 1)
    spikes = []
    for w in range(2):
        keep = at_row >= at_col if w == 0 else at_row <= at_col
        ones = keep.astype(BF16)
        high, middle, low = in_three(spike_ref[...])
        spikes.append(nt_dot(ones, low) + nt_dot(ones, middle) + nt_dot(ones, high))
    for h in range(heads):
        cols = slice(h * HEAD, (h + 1) * HEAD)
        q = q_ref[:, cols].astype(F32)
        q = q * jax.nn.sigmoid(q) * HEAD ** (-0.5)
        v = v_ref[:, cols]
        scores = jnp.zeros((rows, rows), F32)
        for w in range(2):
            keep = at_row >= at_col if w == 0 else at_row <= at_col
            key = slack_ref[:, cols] * jax.nn.sigmoid(-f_ref[w, :, cols].astype(F32))
            decay = jnp.log1p(-key)
            ones = keep.astype(BF16)
            high, middle, low = in_three(decay)
            running = (
                jnp.dot(ones, low, preferred_element_type=F32)
                + jnp.dot(ones, middle, preferred_element_type=F32)
                + jnp.dot(ones, high, preferred_element_type=F32)
                + spikes[w][:, h : h + 1]
            )
            final = running[rows - 1 : rows] if w == 0 else running[0:1]
            q_scaled = (q * jnp.exp(running)).astype(BF16)
            k_scaled = (key * jnp.exp(-running)).astype(BF16)
            scores = scores + jnp.where(keep, nt_dot(q_scaled, k_scaled), 0.0)
            k_end = (key * jnp.exp(final - running)).astype(BF16)
            state = tn_dot(v, k_end).astype(BF16)
            reach_ref[w, :, cols] = q_scaled
            at = (w * heads + h) * pieces
            send_ref[at : at + pieces, 0:chunk, :] = state.reshape(pieces, chunk, HEAD)
            total = jnp.concatenate([t.astype(F32) for t in in_three(jnp.exp(final))], axis=0)
            total = jnp.concatenate([total, jnp.zeros((5, HEAD), F32)], axis=0).astype(BF16)
            send_ref[at : at + pieces, chunk : chunk + 8, :] = jnp.broadcast_to(
                total[None], (pieces, 8, HEAD)
            )
        near_ref[:, cols] = jnp.dot(scores.astype(BF16), v, preferred_element_type=F32)


def scan_body(back_ref, got_ref, give_ref):
    blocks, wide, _ = got_ref.shape
    chunk = wide - 8
    back = back_ref[0]
    state = jnp.zeros((chunk, HEAD), F32)
    for b in range(blocks):
        at = jnp.where(back == 1, blocks - 1 - b, b)
        give_ref[at] = state.astype(BF16)
        piece = got_ref[at].astype(F32)
        total = piece[chunk : chunk + 1] + piece[chunk + 1 : chunk + 2] + piece[chunk + 2 : chunk + 3]
        state = total * state + piece[0:chunk]


def project_body(
    own_ref, near_ref, reach_ref, enter_ref, gate_ref, gain_ref, weight_ref, o0, o1, o2, o3, mixed_ref
):
    heads = near_ref.shape[1] // HEAD
    gain = gain_ref[...].astype(F32)
    for h in range(heads):
        cols = slice(h * HEAD, (h + 1) * HEAD)
        mix = near_ref[:, cols]
        mix = mix + nt_dot(reach_ref[0, :, cols], enter_ref[h])
        mix = mix + nt_dot(reach_ref[1, :, cols], enter_ref[heads + h])
        scale = lax.rsqrt(jnp.mean(mix * mix, axis=-1, keepdims=True) + NORM_EPS)
        g = gate_ref[:, cols].astype(F32)
        mixed_ref[:, cols] = (mix * scale * gain * (g * jax.nn.sigmoid(g))).astype(BF16)
    outs = (o0, o1, o2, o3)
    part = o0.shape[0]
    own = own_ref[0]
    for d in range(len(outs)):
        at = pl.multiple_of(lax.rem(own + d, len(outs)) * part, part)
        outs[d][...] = jnp.dot(
            mixed_ref[pl.ds(at, part), :], weight_ref[...], preferred_element_type=F32
        ).astype(BF16)


def mixer_body(tokens_ref, whole_ref, o0, o1, o2, o3, pair_ref, down_ref, act_ref, sems):
    model = tokens_ref.shape[1]
    hidden = down_ref.shape[1]
    chunks = sems.shape[0] - 1
    step = model // chunks
    copies = []
    for k in range(chunks):
        at = slice(k * step, (k + 1) * step)
        copies.append(
            pltpu.make_async_copy(whole_ref.at[at, : 2 * hidden], pair_ref.at[at], sems.at[k])
        )
    copies.append(pltpu.make_async_copy(whole_ref.at[:, 2 * hidden :], down_ref, sems.at[chunks]))
    for copy in copies:
        copy.start()
    for k in range(chunks):
        copies[k].wait()
        at = slice(k * step, (k + 1) * step)
        term = jnp.dot(tokens_ref[:, at], pair_ref[at, :], preferred_element_type=F32)
        if k == 0:
            act_ref[...] = term
        else:
            act_ref[...] += term
    gate, up = act_ref[:, :hidden], act_ref[:, hidden:]
    inner = (gate * jax.nn.sigmoid(gate) * up).astype(BF16)
    copies[chunks].wait()
    lowered = nt_dot(down_ref[...], inner).T
    part = o0.shape[0]
    for d, out_ref in enumerate((o0, o1, o2, o3)):
        out_ref[...] = lowered[d * part : (d + 1) * part].astype(out_ref.dtype)


VMEM = pl.BlockSpec(memory_space=pltpu.VMEM)
ANY = pl.BlockSpec(memory_space=pl.ANY)
SMEM = pl.BlockSpec(memory_space=pltpu.SMEM)


def shift(array, axis, by):
    size = lax.axis_size(axis)
    return lax.ppermute(array, axis, [(k, (k + by) % size) for k in range(size)])


def local(
    queries,
    forget_logits,
    value_matrix,
    output_gate_logits,
    forget_slack,
    spike_log_forget,
    head_norm_gain,
    output_weight,
    residual,
    mixer_norm_gain,
    mixer_gate_weight,
    mixer_up_weight,
    mixer_down_weight,
):
    rows, width = queries.shape
    heads = spike_log_forget.shape[1]
    model = output_weight.shape[1]
    hidden = mixer_gate_weight.shape[1]
    blocks = lax.axis_size(SP)
    n_tp = lax.axis_size("tp")
    sp_at = lax.axis_index(SP)
    tp_at = lax.axis_index("tp")
    chunk = 2 * heads * HEAD // blocks

    packed = jnp.concatenate([mixer_gate_weight, mixer_up_weight, mixer_down_weight.T], axis=1)
    whole = lax.all_gather(packed, SP, axis=0, tiled=True)

    send, near, reach = pl.pallas_call(
        local_body,
        out_shape=(
            jax.ShapeDtypeStruct((blocks, chunk + 8, HEAD), BF16),
            jax.ShapeDtypeStruct((rows, width), F32),
            jax.ShapeDtypeStruct((2, rows, width), BF16),
        ),
        in_specs=[VMEM] * 5,
        out_specs=(VMEM,) * 3,
        name="local_sweep",
    )(queries, forget_logits, value_matrix, forget_slack[None], spike_log_forget.T)
    got = lax.all_to_all(send, SP, 0, 0, tiled=True)
    give = pl.pallas_call(
        scan_body,
        out_shape=jax.ShapeDtypeStruct((blocks, chunk, HEAD), BF16),
        in_specs=[SMEM, VMEM],
        out_specs=VMEM,
        name="block_scan",
    )((sp_at >= blocks // 2).astype(jnp.int32)[None], got)
    enter = lax.all_to_all(give, SP, 0, 0, tiled=True).reshape(2 * heads, HEAD, HEAD)

    part = rows // n_tp
    parts = pl.pallas_call(
        project_body,
        out_shape=(jax.ShapeDtypeStruct((part, model), BF16),) * n_tp,
        in_specs=[SMEM] + [VMEM] * 6,
        out_specs=(VMEM,) * n_tp,
        scratch_shapes=[pltpu.VMEM((rows, width), BF16)],
        name="norm_project",
    )(tp_at[None], near, reach, enter, output_gate_logits, head_norm_gain[None], output_weight)

    arrived = [parts[0]] + [shift(parts[d], "tp", d) for d in range(1, n_tp)]
    own_resid = lax.dynamic_slice_in_dim(residual, tp_at * part, part, 0)
    hidden_f = own_resid.astype(F32)
    for a in arrived:
        hidden_f = hidden_f + a.astype(F32)
    hidden_state = hidden_f.astype(BF16)
    held = hidden_state.astype(F32)
    normed = (
        held
        * lax.rsqrt(jnp.mean(held * held, axis=-1, keepdims=True) + NORM_EPS)
        * mixer_norm_gain.astype(F32)
    ).astype(BF16)
    everyone = jnp.concatenate([normed] + [shift(normed, "tp", d) for d in range(1, n_tp)], axis=0)
    lowered = pl.pallas_call(
        mixer_body,
        out_shape=(jax.ShapeDtypeStruct((part, model), F32),)
        + (jax.ShapeDtypeStruct((part, model), BF16),) * (n_tp - 1),
        in_specs=[VMEM, ANY],
        out_specs=(VMEM,) * n_tp,
        scratch_shapes=[
            pltpu.VMEM((model, 2 * hidden), BF16),
            pltpu.VMEM((model, hidden), BF16),
            pltpu.VMEM((rows, 2 * hidden), F32),
            pltpu.SemaphoreType.DMA((5,)),
        ],
        compiler_params=pltpu.CompilerParams(vmem_limit_bytes=48 * 1024 * 1024),
        name="channel_mixer",
    )(everyone, whole)
    out = hidden_state.astype(F32) + lowered[0]
    for d in range(1, n_tp):
        out = out + shift(lowered[d], "tp", n_tp - d).astype(F32)
    return out.astype(BF16)


def solution(mesh):
    torus = Mesh(mesh.devices.reshape(8, 4, 2, mesh.shape["tp"]), ("sp_0", "sp_1", "sp_2", "tp"))
    return jax.shard_map(
        local,
        mesh=torus,
        in_specs=(
            P(SP, "tp"),
            P(None, SP, "tp"),
            P(SP, "tp"),
            P(SP, "tp"),
            P("tp"),
            P(SP, "tp"),
            P(),
            P("tp", None),
            P(SP, None),
            P(),
            P(SP, "tp"),
            P(SP, "tp"),
            P("tp", SP),
        ),
        out_specs=P(SP_TP, None),
        check_vma=False,
    )
```

```python
import jax
import jax.numpy as jnp
from jax import lax
from jax.experimental import pallas as pl
from jax.experimental.pallas import tpu as pltpu
from jax.sharding import Mesh
from jax.sharding import PartitionSpec as P


SP = ("sp_0", "sp_1", "sp_2")
SP_TP = ("sp_0", "sp_1", "sp_2", "tp")
NORM_EPS = 1e-06
F32 = jnp.float32
BF16 = jnp.bfloat16
HEAD = 128


def nt_dot(a, b):
    return lax.dot_general(a, b, (((1,), (1,)), ((), ())), preferred_element_type=F32)


def tn_dot(a, b):
    return lax.dot_general(a, b, (((0,), (0,)), ((), ())), preferred_element_type=F32)


def in_three(a):
    high = a.astype(BF16)
    rest = a - high.astype(F32)
    middle = rest.astype(BF16)
    return high, middle, (rest - middle.astype(F32)).astype(BF16)


def local_body(q_ref, f_ref, v_ref, slack_ref, spike_ref, send_ref, near_ref, reach_ref):
    rows = q_ref.shape[0]
    heads = spike_ref.shape[0]
    chunk = send_ref.shape[1] - 8
    pieces = HEAD // chunk
    at_row = lax.broadcasted_iota(jnp.int32, (rows, rows), 0)
    at_col = lax.broadcasted_iota(jnp.int32, (rows, rows), 1)
    spikes = []
    for w in range(2):
        keep = at_row >= at_col if w == 0 else at_row <= at_col
        ones = keep.astype(BF16)
        high, middle, low = in_three(spike_ref[...])
        spikes.append(nt_dot(ones, low) + nt_dot(ones, middle) + nt_dot(ones, high))
    for h in range(heads):
        cols = slice(h * HEAD, (h + 1) * HEAD)
        q = q_ref[:, cols].astype(F32)
        q = q * jax.nn.sigmoid(q) * HEAD ** (-0.5)
        v = v_ref[:, cols]
        scores = jnp.zeros((rows, rows), F32)
        for w in range(2):
            keep = at_row >= at_col if w == 0 else at_row <= at_col
            key = slack_ref[:, cols] * jax.nn.sigmoid(-f_ref[w, :, cols].astype(F32))
            decay = jnp.log1p(-key)
            ones = keep.astype(BF16)
            high, middle, low = in_three(decay)
            running = (
                jnp.dot(ones, low, preferred_element_type=F32)
                + jnp.dot(ones, middle, preferred_element_type=F32)
                + jnp.dot(ones, high, preferred_element_type=F32)
                + spikes[w][:, h : h + 1]
            )
            final = running[rows - 1 : rows] if w == 0 else running[0:1]
            q_scaled = (q * jnp.exp(running)).astype(BF16)
            k_scaled = (key * jnp.exp(-running)).astype(BF16)
            scores = scores + jnp.where(keep, nt_dot(q_scaled, k_scaled), 0.0)
            k_end = (key * jnp.exp(final - running)).astype(BF16)
            state = tn_dot(v, k_end).astype(BF16)
            reach_ref[w, :, cols] = q_scaled
            at = (w * heads + h) * pieces
            send_ref[at : at + pieces, 0:chunk, :] = state.reshape(pieces, chunk, HEAD)
            total = jnp.concatenate([t.astype(F32) for t in in_three(jnp.exp(final))], axis=0)
            total = jnp.concatenate([total, jnp.zeros((5, HEAD), F32)], axis=0).astype(BF16)
            send_ref[at : at + pieces, chunk : chunk + 8, :] = jnp.broadcast_to(
                total[None], (pieces, 8, HEAD)
            )
        near_ref[:, cols] = jnp.dot(scores.astype(BF16), v, preferred_element_type=F32)


def scan_body(back_ref, got_ref, give_ref):
    blocks, wide, _ = got_ref.shape
    chunk = wide - 8
    back = back_ref[0]
    state = jnp.zeros((chunk, HEAD), F32)
    for b in range(blocks):
        at = jnp.where(back == 1, blocks - 1 - b, b)
        give_ref[at] = state.astype(BF16)
        piece = got_ref[at].astype(F32)
        total = piece[chunk : chunk + 1] + piece[chunk + 1 : chunk + 2] + piece[chunk + 2 : chunk + 3]
        state = total * state + piece[0:chunk]


def project_body(
    own_ref, near_ref, reach_ref, enter_ref, gate_ref, gain_ref, weight_ref, o0, o1, o2, o3, mixed_ref
):
    heads = near_ref.shape[1] // HEAD
    gain = gain_ref[...].astype(F32)
    for h in range(heads):
        cols = slice(h * HEAD, (h + 1) * HEAD)
        mix = near_ref[:, cols]
        mix = mix + nt_dot(reach_ref[0, :, cols], enter_ref[h])
        mix = mix + nt_dot(reach_ref[1, :, cols], enter_ref[heads + h])
        scale = lax.rsqrt(jnp.mean(mix * mix, axis=-1, keepdims=True) + NORM_EPS)
        g = gate_ref[:, cols].astype(F32)
        mixed_ref[:, cols] = (mix * scale * gain * (g * jax.nn.sigmoid(g))).astype(BF16)
    outs = (o0, o1, o2, o3)
    part = o0.shape[0]
    own = own_ref[0]
    for d in range(len(outs)):
        at = pl.multiple_of(lax.rem(own + d, len(outs)) * part, part)
        outs[d][...] = jnp.dot(
            mixed_ref[pl.ds(at, part), :], weight_ref[...], preferred_element_type=F32
        ).astype(BF16)


def mixer_body(at_ref, tokens_ref, late_ref, early_ref, *refs):
    lines, (o0, o1, o2, o3, late_all, early_all, act_ref, sems) = refs[:6], refs[6:]
    z_size, y_size, cores, _, wide = late_all.shape
    model = tokens_ref.shape[1]
    y, core = at_ref[0], at_ref[1]
    chunks = 4
    z_step = z_size // chunks
    step = model // chunks
    late, early = [], []
    for n in range(chunks):
        z = slice(n * z_step, (n + 1) * z_step)
        late.append([])
        for c in range(cores):
            for k in range(y_size):
                late[n].append(
                    pltpu.make_async_copy(
                        late_ref.at[z, c, k],
                        late_all.at[z, lax.rem(y + y_size - k, y_size), c],
                        sems.at[(n * cores + c) * y_size + k],
                    )
                )
    base = chunks * cores * y_size
    early.append(pltpu.make_async_copy(early_ref, early_all.at[:, y], sems.at[base]))
    per_core = y_size - 1
    z_half = z_size // cores
    for c in range(cores):
        row_core = core if c == 0 else 1 - core
        turn = jnp.where(row_core == 0, y_size - 1, 1)
        for k in range(1, y_size):
            early.append(
                pltpu.make_async_copy(
                    lines[c * per_core + k - 1],
                    early_all.at[pl.ds(row_core * z_half, z_half), lax.rem(y + turn * k, y_size)],
                    sems.at[base + c * per_core + k],
                )
            )
    for copy in sum(late, []) + early:
        copy.start()
    hidden = early_all.shape[4] + wide
    hidden = hidden // 3
    first = wide // 2
    late_rows = late_all.reshape(model, wide)
    early_rows = early_all.reshape(model, early_all.shape[4])
    for n in range(chunks):
        for copy in late[n]:
            copy.wait()
        at = slice(n * step, (n + 1) * step)
        term = jnp.dot(tokens_ref[:, at], late_rows[at, :], preferred_element_type=F32)
        if n == 0:
            act_ref[...] = term
        else:
            act_ref[...] += term
    for copy in early:
        copy.wait()
    rest = jnp.dot(tokens_ref[...], early_rows[:, hidden:], preferred_element_type=F32)
    second = rest.shape[1] // 2
    gate = jnp.concatenate([act_ref[:, :first], rest[:, :second]], axis=1)
    up = jnp.concatenate([act_ref[:, first:], rest[:, second:]], axis=1)
    inner = (gate * jax.nn.sigmoid(gate) * up).astype(BF16)
    lowered = nt_dot(early_rows[:, :hidden], inner).T
    part = o0.shape[0]
    for d, out_ref in enumerate((o0, o1, o2, o3)):
        out_ref[...] = lowered[d * part : (d + 1) * part].astype(out_ref.dtype)


VMEM = pl.BlockSpec(memory_space=pltpu.VMEM)
ANY = pl.BlockSpec(memory_space=pl.ANY)
SMEM = pl.BlockSpec(memory_space=pltpu.SMEM)


def shift(array, axis, by):
    size = lax.axis_size(axis)
    return lax.ppermute(array, axis, [(k, (k + by) % size) for k in range(size)])


def local(
    queries,
    forget_logits,
    value_matrix,
    output_gate_logits,
    forget_slack,
    spike_log_forget,
    head_norm_gain,
    output_weight,
    residual,
    mixer_norm_gain,
    mixer_gate_weight,
    mixer_up_weight,
    mixer_down_weight,
):
    rows, width = queries.shape
    heads = spike_log_forget.shape[1]
    model = output_weight.shape[1]
    hidden = mixer_gate_weight.shape[1]
    blocks = lax.axis_size(SP)
    n_tp = lax.axis_size("tp")
    sp_at = lax.axis_index(SP)
    tp_at = lax.axis_index("tp")
    chunk = 2 * heads * HEAD // blocks

    z_size, y_size, cores = (lax.axis_size(axis) for axis in SP)
    slab = mixer_gate_weight.shape[0]
    first = hidden // HEAD * 3 // 4 * HEAD
    first_part = jnp.concatenate([mixer_gate_weight[:, :first], mixer_up_weight[:, :first]], axis=1)
    second_part = jnp.concatenate(
        [mixer_down_weight.T, mixer_gate_weight[:, first:], mixer_up_weight[:, first:]], axis=1
    )
    early = lax.all_gather(second_part, ("sp_0", "sp_2"), axis=0, tiled=True)
    early = early.reshape(z_size, cores, slab, second_part.shape[1])

    send, near, reach = pl.pallas_call(
        local_body,
        out_shape=(
            jax.ShapeDtypeStruct((blocks, chunk + 8, HEAD), BF16),
            jax.ShapeDtypeStruct((rows, width), F32),
            jax.ShapeDtypeStruct((2, rows, width), BF16),
        ),
        in_specs=[VMEM] * 5,
        out_specs=(VMEM,) * 3,
        name="local_sweep",
    )(queries, forget_logits, value_matrix, forget_slack[None], spike_log_forget.T)
    first_part, send = lax.optimization_barrier((first_part, send))
    got = lax.all_to_all(send, SP, 0, 0, tiled=True)
    late = jnp.stack([first_part] + [shift(first_part, "sp_1", d) for d in range(1, y_size)])
    late = lax.all_gather(late.reshape(y_size * slab, 2 * first), ("sp_0", "sp_2"), axis=0, tiled=True)
    late = late.reshape(z_size, cores, y_size, slab, 2 * first)
    turns = []
    for k in range(y_size):
        for c in range(cores):
            turns.append((k * cores + c, (k + (1 if c == 0 else y_size - 1)) % y_size * cores + c))
    z_half = z_size // cores
    early, got = lax.optimization_barrier((early, got))
    lines, theirs = [], []
    line = lax.dynamic_slice_in_dim(early, lax.axis_index("sp_2") * z_half, z_half, 0)
    line = lax.ppermute(line, ("sp_1", "sp_2"), turns)
    give = pl.pallas_call(
        scan_body,
        out_shape=jax.ShapeDtypeStruct((blocks, chunk, HEAD), BF16),
        in_specs=[SMEM, VMEM],
        out_specs=VMEM,
        name="block_scan",
    )((sp_at >= blocks // 2).astype(jnp.int32)[None], got)
    enter = lax.all_to_all(give, SP, 0, 0, tiled=True)
    line, enter = lax.optimization_barrier((line, enter))
    enter = enter.reshape(2 * heads, HEAD, HEAD)
    lines.append(line)
    theirs.append(shift(line, "sp_2", 1))
    line = lax.ppermute(line, ("sp_1", "sp_2"), turns)

    part = rows // n_tp
    parts = pl.pallas_call(
        project_body,
        out_shape=(jax.ShapeDtypeStruct((part, model), BF16),) * n_tp,
        in_specs=[SMEM] + [VMEM] * 6,
        out_specs=(VMEM,) * n_tp,
        scratch_shapes=[pltpu.VMEM((rows, width), BF16)],
        name="norm_project",
    )(tp_at[None], near, reach, enter, output_gate_logits, head_norm_gain[None], output_weight)

    arrived = [parts[0]] + [shift(parts[d], "tp", d) for d in range(1, n_tp)]
    own_resid = lax.dynamic_slice_in_dim(residual, tp_at * part, part, 0)
    hidden_f = own_resid.astype(F32)
    for a in arrived:
        hidden_f = hidden_f + a.astype(F32)
    hidden_state = hidden_f.astype(BF16)
    held = hidden_state.astype(F32)
    normed = (
        held
        * lax.rsqrt(jnp.mean(held * held, axis=-1, keepdims=True) + NORM_EPS)
        * mixer_norm_gain.astype(F32)
    ).astype(BF16)
    line, normed = lax.optimization_barrier((line, normed))
    lines.append(line)
    theirs.append(shift(line, "sp_2", 1))
    line = lax.ppermute(line, ("sp_1", "sp_2"), turns)
    everyone = jnp.concatenate([normed] + [shift(normed, "tp", d) for d in range(1, n_tp)], axis=0)
    line, everyone = lax.optimization_barrier((line, everyone))
    lines.append(line)
    theirs.append(shift(line, "sp_2", 1))
    at = jnp.stack([lax.axis_index("sp_1"), lax.axis_index("sp_2")])
    lowered = pl.pallas_call(
        mixer_body,
        out_shape=(jax.ShapeDtypeStruct((part, model), F32),)
        + (jax.ShapeDtypeStruct((part, model), BF16),) * (n_tp - 1),
        in_specs=[SMEM, VMEM] + [ANY] * (2 + 2 * len(lines)),
        out_specs=(VMEM,) * n_tp,
        scratch_shapes=[
            pltpu.VMEM((z_size, y_size, cores, slab, 2 * first), BF16),
            pltpu.VMEM((z_size, y_size, cores, slab, 3 * hidden - 2 * first), BF16),
            pltpu.VMEM((rows, 2 * first), F32),
            pltpu.SemaphoreType.DMA((39,)),
        ],
        compiler_params=pltpu.CompilerParams(vmem_limit_bytes=48 * 1024 * 1024),
        name="channel_mixer",
    )(at, everyone, late, early, *lines, *theirs)
    out = hidden_state.astype(F32) + lowered[0]
    for d in range(1, n_tp):
        out = out + shift(lowered[d], "tp", n_tp - d).astype(F32)
    return out.astype(BF16)


def solution(mesh):
    torus = Mesh(mesh.devices.reshape(8, 4, 2, mesh.shape["tp"]), ("sp_0", "sp_1", "sp_2", "tp"))
    return jax.shard_map(
        local,
        mesh=torus,
        in_specs=(
            P(SP, "tp"),
            P(None, SP, "tp"),
            P(SP, "tp"),
            P(SP, "tp"),
            P("tp"),
            P(SP, "tp"),
            P(),
            P("tp", None),
            P(SP, None),
            P(),
            P(SP, "tp"),
            P(SP, "tp"),
            P("tp", SP),
        ),
        out_specs=P(SP_TP, None),
        check_vma=False,
    )
```

```python
import jax
import jax.numpy as jnp
from jax import lax
from jax.experimental import pallas as pl
from jax.experimental.pallas import tpu as pltpu
from jax.sharding import Mesh
from jax.sharding import PartitionSpec as P


SP = ("sp_0", "sp_1", "sp_2")
SP_TP = ("sp_0", "sp_1", "sp_2", "tp")
NORM_EPS = 1e-06
F32 = jnp.float32
BF16 = jnp.bfloat16
HEAD = 128


def nt_dot(a, b):
    return lax.dot_general(a, b, (((1,), (1,)), ((), ())), preferred_element_type=F32)


def tn_dot(a, b):
    return lax.dot_general(a, b, (((0,), (0,)), ((), ())), preferred_element_type=F32)


def in_three(a):
    high = a.astype(BF16)
    rest = a - high.astype(F32)
    middle = rest.astype(BF16)
    return high, middle, (rest - middle.astype(F32)).astype(BF16)


def local_body(q_ref, f_ref, v_ref, slack_ref, spike_ref, send_ref, near_ref, reach_ref):
    rows = q_ref.shape[0]
    heads = spike_ref.shape[0]
    chunk = send_ref.shape[1] - 8
    pieces = HEAD // chunk
    at_row = lax.broadcasted_iota(jnp.int32, (rows, rows), 0)
    at_col = lax.broadcasted_iota(jnp.int32, (rows, rows), 1)
    spikes = []
    for w in range(2):
        keep = at_row >= at_col if w == 0 else at_row <= at_col
        ones = keep.astype(BF16)
        high, middle, low = in_three(spike_ref[...])
        spikes.append(nt_dot(ones, low) + nt_dot(ones, middle) + nt_dot(ones, high))
    for h in range(heads):
        cols = slice(h * HEAD, (h + 1) * HEAD)
        q = q_ref[:, cols].astype(F32)
        q = q * jax.nn.sigmoid(q) * HEAD ** (-0.5)
        v = v_ref[:, cols]
        scores = jnp.zeros((rows, rows), F32)
        for w in range(2):
            keep = at_row >= at_col if w == 0 else at_row <= at_col
            key = slack_ref[:, cols] * jax.nn.sigmoid(-f_ref[w, :, cols].astype(F32))
            decay = jnp.log1p(-key)
            ones = keep.astype(BF16)
            high, middle, low = in_three(decay)
            running = (
                jnp.dot(ones, low, preferred_element_type=F32)
                + jnp.dot(ones, middle, preferred_element_type=F32)
                + jnp.dot(ones, high, preferred_element_type=F32)
                + spikes[w][:, h : h + 1]
            )
            final = running[rows - 1 : rows] if w == 0 else running[0:1]
            q_scaled = (q * jnp.exp(running)).astype(BF16)
            k_scaled = (key * jnp.exp(-running)).astype(BF16)
            scores = scores + jnp.where(keep, nt_dot(q_scaled, k_scaled), 0.0)
            k_end = (key * jnp.exp(final - running)).astype(BF16)
            state = tn_dot(v, k_end).astype(BF16)
            reach_ref[w, :, cols] = q_scaled
            at = (w * heads + h) * pieces
            send_ref[at : at + pieces, 0:chunk, :] = state.reshape(pieces, chunk, HEAD)
            total = jnp.concatenate([t.astype(F32) for t in in_three(jnp.exp(final))], axis=0)
            total = jnp.concatenate([total, jnp.zeros((5, HEAD), F32)], axis=0).astype(BF16)
            send_ref[at : at + pieces, chunk : chunk + 8, :] = jnp.broadcast_to(
                total[None], (pieces, 8, HEAD)
            )
        near_ref[:, cols] = jnp.dot(scores.astype(BF16), v, preferred_element_type=F32)


def scan_body(back_ref, got_ref, give_ref):
    blocks, wide, _ = got_ref.shape
    chunk = wide - 8
    back = back_ref[0]
    state = jnp.zeros((chunk, HEAD), F32)
    for b in range(blocks):
        at = jnp.where(back == 1, blocks - 1 - b, b)
        give_ref[at] = state.astype(BF16)
        piece = got_ref[at].astype(F32)
        total = piece[chunk : chunk + 1] + piece[chunk + 1 : chunk + 2] + piece[chunk + 2 : chunk + 3]
        state = total * state + piece[0:chunk]


def project_body(
    own_ref, near_ref, reach_ref, enter_ref, gate_ref, gain_ref, weight_ref, o0, o1, o2, o3, mixed_ref
):
    heads = near_ref.shape[1] // HEAD
    gain = gain_ref[...].astype(F32)
    for h in range(heads):
        cols = slice(h * HEAD, (h + 1) * HEAD)
        mix = near_ref[:, cols]
        mix = mix + nt_dot(reach_ref[0, :, cols], enter_ref[h])
        mix = mix + nt_dot(reach_ref[1, :, cols], enter_ref[heads + h])
        scale = lax.rsqrt(jnp.mean(mix * mix, axis=-1, keepdims=True) + NORM_EPS)
        g = gate_ref[:, cols].astype(F32)
        mixed_ref[:, cols] = (mix * scale * gain * (g * jax.nn.sigmoid(g))).astype(BF16)
    outs = (o0, o1, o2, o3)
    part = o0.shape[0]
    own = own_ref[0]
    for d in range(len(outs)):
        at = pl.multiple_of(lax.rem(own + d, len(outs)) * part, part)
        outs[d][...] = jnp.dot(
            mixed_ref[pl.ds(at, part), :], weight_ref[...], preferred_element_type=F32
        ).astype(BF16)


def halves_body(core_ref, gate_ref, up_ref, down_ref, keep_ref, give_ref):
    hidden = gate_ref.shape[1]
    width = keep_ref.shape[1] // 3

    def write(out_ref, start):
        for k, ref in enumerate((gate_ref, up_ref, down_ref)):
            out_ref[:, k * width : (k + 1) * width] = ref[:, start : start + width]

    @pl.when(core_ref[0] == 0)
    def _():
        write(keep_ref, 0)
        write(give_ref, hidden - width)

    @pl.when(core_ref[0] != 0)
    def _():
        write(keep_ref, hidden - width)
        write(give_ref, 0)


def mixer_body(at_ref, own_ref, theirs_ref, *refs, hidden):
    (line, y_up, y_down, y_far, y_far_back), b_refs = refs[:5], refs[5:14]
    mine_ref, give_ref, tokens_ref, weights_ref, act_ref, sems = refs[14:]
    z_size, y_size, cores, slab, wide = weights_ref.shape
    z, y, core = at_ref[0], at_ref[1], at_ref[2]
    ahead = z_size // 2
    groups = []
    for k in range(z_size):
        at_z = lax.rem(z + z_size - k, z_size)
        far = y_far.at[k] if k < ahead else y_far_back.at[k - ahead]
        pieces = [(line.at[k], 0, core), (y_up.at[k], 1, core), (far, 2, core), (y_down.at[k], 3, core)]
        for m in range(y_size):
            if k == ahead:
                source = b_refs[k].at[m] if m < 2 else b_refs[k + 1].at[m - 2]
            else:
                source = b_refs[k if k < ahead else k + 1].at[m]
            pieces.append((source, m, 1 - core))
        group = []
        for n, (source, back, row_core) in enumerate(pieces):
            at_y = lax.rem(y + y_size - back, y_size)
            group.append(
                pltpu.make_async_copy(
                    source, weights_ref.at[at_z, at_y, row_core], sems.at[k * len(pieces) + n]
                )
            )
        groups.append((at_z, group))
    for _, group in groups:
        for copy in group:
            copy.start()
    rows = own_ref.shape[0]
    tokens_ref[0:rows, :] = own_ref[...]
    tokens_ref[rows : 2 * rows, :] = theirs_ref[...]
    width = wide // 3
    step = y_size * cores * slab
    for k, (at_z, group) in enumerate(groups):
        for copy in group:
            copy.wait()
        tokens = tokens_ref[:, pl.ds(pl.multiple_of(at_z * step, step), step)]
        pair = weights_ref[at_z, :, :, :, : 2 * width].reshape(step, 2 * width)
        term = jnp.dot(tokens, pair, preferred_element_type=F32)
        if k == 0:
            act_ref[...] = term
        else:
            act_ref[...] += term
    gate, up = act_ref[:, :width], act_ref[:, width:]
    inner = gate * jax.nn.sigmoid(gate) * up
    lane = lax.broadcasted_iota(jnp.int32, inner.shape, 1)
    low = jnp.where(core == 0, 0, width - hidden // 2)
    inner = jnp.where((lane >= low) & (lane < low + hidden // 2), inner, 0.0).astype(BF16)
    down = weights_ref[:, :, :, :, 2 * width :].reshape(z_size * step, width)
    lowered = nt_dot(down, inner).T
    mine_ref[...] = lowered[:rows]
    give_ref[...] = lowered[rows:].astype(BF16)


VMEM = pl.BlockSpec(memory_space=pltpu.VMEM)
ANY = pl.BlockSpec(memory_space=pl.ANY)
SMEM = pl.BlockSpec(memory_space=pltpu.SMEM)


def shift(array, axis, by):
    size = lax.axis_size(axis)
    return lax.ppermute(array, axis, [(k, (k + by) % size) for k in range(size)])


def local(
    queries,
    forget_logits,
    value_matrix,
    output_gate_logits,
    forget_slack,
    spike_log_forget,
    head_norm_gain,
    output_weight,
    residual,
    mixer_norm_gain,
    mixer_gate_weight,
    mixer_up_weight,
    mixer_down_weight,
):
    rows, width = queries.shape
    heads = spike_log_forget.shape[1]
    model = output_weight.shape[1]
    hidden = mixer_gate_weight.shape[1]
    blocks = lax.axis_size(SP)
    n_tp = lax.axis_size("tp")
    sp_at = lax.axis_index(SP)
    tp_at = lax.axis_index("tp")
    chunk = 2 * heads * HEAD // blocks

    z_size, y_size, cores = (lax.axis_size(axis) for axis in SP)
    core_at = lax.axis_index("sp_2")
    slab = mixer_gate_weight.shape[0]
    half = (hidden // 2 + HEAD - 1) // HEAD * HEAD
    keep, give = pl.pallas_call(
        halves_body,
        out_shape=(jax.ShapeDtypeStruct((slab, 3 * half), BF16),) * 2,
        in_specs=[SMEM] + [VMEM] * 3,
        out_specs=(VMEM,) * 2,
        name="weight_halves",
    )(core_at[None], mixer_gate_weight, mixer_up_weight, mixer_down_weight.T)
    a0, b0 = keep, shift(give, "sp_2", 1)
    a_up, a_down = [shift(a0, "sp_0", 1)], [shift(a0, "sp_0", z_size - 1)]
    b_y = [shift(b0, "sp_1", d) for d in range(1, y_size)]

    send, near, reach = pl.pallas_call(
        local_body,
        out_shape=(
            jax.ShapeDtypeStruct((blocks, chunk + 8, HEAD), BF16),
            jax.ShapeDtypeStruct((rows, width), F32),
            jax.ShapeDtypeStruct((2, rows, width), BF16),
        ),
        in_specs=[VMEM] * 5,
        out_specs=(VMEM,) * 3,
        name="local_sweep",
    )(queries, forget_logits, value_matrix, forget_slack[None], spike_log_forget.T)

    a_up[0], a_down[0], b_y, send = lax.optimization_barrier((a_up[0], a_down[0], b_y, send))
    b_line = jnp.stack([b0] + b_y)
    b_up, b_down = [shift(b_line, "sp_0", 1)], [shift(b_line, "sp_0", z_size - 1)]
    a_up.append(shift(a_up[0], "sp_0", 1))
    a_down.append(shift(a_down[0], "sp_0", z_size - 1))
    got = lax.all_to_all(send, SP, 0, 0, tiled=True)
    b_up.append(shift(b_up[0], "sp_0", 1))
    b_down.append(shift(b_down[0], "sp_0", z_size - 1))
    a_up.append(shift(a_up[1], "sp_0", 1))
    a_down.append(shift(a_down[1], "sp_0", z_size - 1))
    a_up[2], a_down[2], got = lax.optimization_barrier((a_up[2], a_down[2], got))
    a_far = shift(a_up[2][: slab // 2], "sp_0", 1)
    a_far_back = shift(a_down[2][slab // 2 :], "sp_0", z_size - 1)
    give = pl.pallas_call(
        scan_body,
        out_shape=jax.ShapeDtypeStruct((blocks, chunk, HEAD), BF16),
        in_specs=[SMEM, VMEM],
        out_specs=VMEM,
        name="block_scan",
    )((sp_at >= blocks // 2).astype(jnp.int32)[None], got)
    enter = lax.all_to_all(give, SP, 0, 0, tiled=True)
    a_line = jnp.stack([a0] + a_up + [jnp.concatenate([a_far, a_far_back])] + a_down[::-1])
    b_up.append(shift(b_up[1], "sp_0", 1))
    b_down.append(shift(b_down[1], "sp_0", z_size - 1))
    y_up = shift(a_line, "sp_1", 1)
    y_down = shift(a_line, "sp_1", y_size - 1)
    enter = enter.reshape(2 * heads, HEAD, HEAD)

    part = rows // n_tp
    parts = pl.pallas_call(
        project_body,
        out_shape=(jax.ShapeDtypeStruct((part, model), BF16),) * n_tp,
        in_specs=[SMEM] + [VMEM] * 6,
        out_specs=(VMEM,) * n_tp,
        scratch_shapes=[pltpu.VMEM((rows, width), BF16)],
        name="norm_project",
    )(tp_at[None], near, reach, enter, output_gate_logits, head_norm_gain[None], output_weight)

    b_up[2], b_down[2], parts = lax.optimization_barrier((b_up[2], b_down[2], parts))
    b_far = shift(b_up[2][: y_size // 2], "sp_0", 1)
    b_far_back = shift(b_down[2][y_size // 2 :], "sp_0", z_size - 1)
    arrived = [parts[0]] + [shift(parts[d], "tp", d) for d in range(1, n_tp)]
    own_resid = lax.dynamic_slice_in_dim(residual, tp_at * part, part, 0)
    hidden_f = own_resid.astype(F32)
    for a in arrived:
        hidden_f = hidden_f + a.astype(F32)
    hidden_state = hidden_f.astype(BF16)
    held = hidden_state.astype(F32)
    normed = (
        held
        * lax.rsqrt(jnp.mean(held * held, axis=-1, keepdims=True) + NORM_EPS)
        * mixer_norm_gain.astype(F32)
    ).astype(BF16)
    b_far, b_far_back, y_up, y_down, normed = lax.optimization_barrier(
        (b_far, b_far_back, y_up, y_down, normed)
    )
    y_far = shift(y_up[: z_size // 2], "sp_1", 1)
    y_far_back = shift(y_down[z_size // 2 :], "sp_1", y_size - 1)
    own = jnp.concatenate([normed] + [shift(normed, "tp", d) for d in range(1, n_tp)], axis=0)
    theirs = shift(own, "sp_2", 1)
    at = jnp.stack([lax.axis_index("sp_0"), lax.axis_index("sp_1"), core_at])
    pieces = [a_line, y_up, y_down, y_far, y_far_back]
    pieces += [b_line] + b_up + [b_far, b_far_back] + b_down[::-1]
    mine, other = pl.pallas_call(
        lambda *refs: mixer_body(*refs, hidden=hidden),
        out_shape=(
            jax.ShapeDtypeStruct((rows, model), F32),
            jax.ShapeDtypeStruct((rows, model), BF16),
        ),
        in_specs=[SMEM, VMEM, VMEM] + [ANY] * len(pieces),
        out_specs=(VMEM, VMEM),
        scratch_shapes=[
            pltpu.VMEM((cores * rows, model), BF16),
            pltpu.VMEM((z_size, y_size, cores, slab, 3 * half), BF16),
            pltpu.VMEM((cores * rows, 2 * half), F32),
            pltpu.SemaphoreType.DMA((z_size * y_size * cores,)),
        ],
        compiler_params=pltpu.CompilerParams(vmem_limit_bytes=32 * 1024 * 1024),
        name="channel_mixer",
    )(at, own, theirs, *pieces)
    lowered = mine + shift(other, "sp_2", 1).astype(F32)
    out = hidden_state.astype(F32) + lowered[:part]
    for d in range(1, n_tp):
        back = lowered[d * part : (d + 1) * part].astype(BF16)
        out = out + shift(back, "tp", n_tp - d).astype(F32)
    return out.astype(BF16)


def solution(mesh):
    torus = Mesh(mesh.devices.reshape(8, 4, 2, mesh.shape["tp"]), ("sp_0", "sp_1", "sp_2", "tp"))
    return jax.shard_map(
        local,
        mesh=torus,
        in_specs=(
            P(SP, "tp"),
            P(None, SP, "tp"),
            P(SP, "tp"),
            P(SP, "tp"),
            P("tp"),
            P(SP, "tp"),
            P(),
            P("tp", None),
            P(SP, None),
            P(),
            P(SP, "tp"),
            P(SP, "tp"),
            P("tp", SP),
        ),
        out_specs=P(SP_TP, None),
        check_vma=False,
    )
```

```python
import jax
import jax.numpy as jnp
from jax import lax
from jax.experimental import pallas as pl
from jax.experimental.pallas import tpu as pltpu
from jax.sharding import Mesh
from jax.sharding import PartitionSpec as P


SP = ("sp_0", "sp_1", "sp_2")
SP_TP = ("sp_0", "sp_1", "sp_2", "tp")
NORM_EPS = 1e-06
F32 = jnp.float32
BF16 = jnp.bfloat16
HEAD = 128


def nt_dot(a, b):
    return lax.dot_general(a, b, (((1,), (1,)), ((), ())), preferred_element_type=F32)


def tn_dot(a, b):
    return lax.dot_general(a, b, (((0,), (0,)), ((), ())), preferred_element_type=F32)


def in_three(a):
    high = a.astype(BF16)
    rest = a - high.astype(F32)
    middle = rest.astype(BF16)
    return high, middle, (rest - middle.astype(F32)).astype(BF16)


def local_body(q_ref, f_ref, v_ref, slack_ref, spike_ref, send_ref, near_ref, reach_ref):
    rows = q_ref.shape[0]
    heads = spike_ref.shape[0]
    chunk = send_ref.shape[1] - 8
    pieces = HEAD // chunk
    at_row = lax.broadcasted_iota(jnp.int32, (rows, rows), 0)
    at_col = lax.broadcasted_iota(jnp.int32, (rows, rows), 1)
    spikes = []
    for w in range(2):
        keep = at_row >= at_col if w == 0 else at_row <= at_col
        ones = keep.astype(BF16)
        high, middle, low = in_three(spike_ref[...])
        spikes.append(nt_dot(ones, low) + nt_dot(ones, middle) + nt_dot(ones, high))
    for h in range(heads):
        cols = slice(h * HEAD, (h + 1) * HEAD)
        q = q_ref[:, cols].astype(F32)
        q = q * jax.nn.sigmoid(q) * HEAD ** (-0.5)
        v = v_ref[:, cols]
        scores = jnp.zeros((rows, rows), F32)
        for w in range(2):
            keep = at_row >= at_col if w == 0 else at_row <= at_col
            key = slack_ref[:, cols] * jax.nn.sigmoid(-f_ref[w, :, cols].astype(F32))
            decay = jnp.log1p(-key)
            ones = keep.astype(BF16)
            high, middle, low = in_three(decay)
            running = (
                jnp.dot(ones, low, preferred_element_type=F32)
                + jnp.dot(ones, middle, preferred_element_type=F32)
                + jnp.dot(ones, high, preferred_element_type=F32)
                + spikes[w][:, h : h + 1]
            )
            final = running[rows - 1 : rows] if w == 0 else running[0:1]
            q_scaled = (q * jnp.exp(running)).astype(BF16)
            k_scaled = (key * jnp.exp(-running)).astype(BF16)
            scores = scores + jnp.where(keep, nt_dot(q_scaled, k_scaled), 0.0)
            k_end = (key * jnp.exp(final - running)).astype(BF16)
            state = tn_dot(v, k_end).astype(BF16)
            reach_ref[w, :, cols] = q_scaled
            at = (w * heads + h) * pieces
            send_ref[at : at + pieces, 0:chunk, :] = state.reshape(pieces, chunk, HEAD)
            total = jnp.concatenate([t.astype(F32) for t in in_three(jnp.exp(final))], axis=0)
            total = jnp.concatenate([total, jnp.zeros((5, HEAD), F32)], axis=0).astype(BF16)
            send_ref[at : at + pieces, chunk : chunk + 8, :] = jnp.broadcast_to(
                total[None], (pieces, 8, HEAD)
            )
        near_ref[:, cols] = jnp.dot(scores.astype(BF16), v, preferred_element_type=F32)


def scan_body(back_ref, got_ref, give_ref):
    blocks, wide, _ = got_ref.shape
    chunk = wide - 8
    back = back_ref[0]
    state = jnp.zeros((chunk, HEAD), F32)
    for b in range(blocks):
        at = jnp.where(back == 1, blocks - 1 - b, b)
        give_ref[at] = state.astype(BF16)
        piece = got_ref[at].astype(F32)
        total = piece[chunk : chunk + 1] + piece[chunk + 1 : chunk + 2] + piece[chunk + 2 : chunk + 3]
        state = total * state + piece[0:chunk]


def project_body(
    own_ref, near_ref, reach_ref, enter_ref, gate_ref, gain_ref, weight_ref, o0, o1, o2, o3, mixed_ref
):
    heads = near_ref.shape[1] // HEAD
    gain = gain_ref[...].astype(F32)
    for h in range(heads):
        cols = slice(h * HEAD, (h + 1) * HEAD)
        mix = near_ref[:, cols]
        mix = mix + nt_dot(reach_ref[0, :, cols], enter_ref[h])
        mix = mix + nt_dot(reach_ref[1, :, cols], enter_ref[heads + h])
        scale = lax.rsqrt(jnp.mean(mix * mix, axis=-1, keepdims=True) + NORM_EPS)
        g = gate_ref[:, cols].astype(F32)
        mixed_ref[:, cols] = (mix * scale * gain * (g * jax.nn.sigmoid(g))).astype(BF16)
    outs = (o0, o1, o2, o3)
    part = o0.shape[0]
    own = own_ref[0]
    for d in range(len(outs)):
        at = pl.multiple_of(lax.rem(own + d, len(outs)) * part, part)
        outs[d][...] = jnp.dot(
            mixed_ref[pl.ds(at, part), :], weight_ref[...], preferred_element_type=F32
        ).astype(BF16)


def halves_body(parity_ref, gate_ref, up_ref, down_ref, keep_ref, give_ref):
    hidden = gate_ref.shape[1]
    width = keep_ref.shape[1] // 3

    def write(out_ref, start):
        for k, ref in enumerate((gate_ref, up_ref, down_ref)):
            out_ref[:, k * width : (k + 1) * width] = ref[:, start : start + width]

    @pl.when(parity_ref[0] == 0)
    def _():
        write(keep_ref, 0)
        write(give_ref, hidden - width)

    @pl.when(parity_ref[0] != 0)
    def _():
        write(keep_ref, hidden - width)
        write(give_ref, 0)


def mixer_body(at_ref, tokens_ref, whole_ref, o0, o1, o2, o3, weights_ref, act_ref, sems, *, hidden):
    z_size, y_size, cores, _, wide = weights_ref.shape
    model = tokens_ref.shape[1]
    y = at_ref[0]
    chunks = 2
    z_step = z_size // chunks
    step = model // chunks
    width = wide // 3
    groups = []
    for n in range(chunks):
        z = slice(n * z_step, (n + 1) * z_step)
        group = []
        for c in range(cores):
            for k in range(y_size):
                group.append(
                    pltpu.make_async_copy(
                        whole_ref.at[z, c, k],
                        weights_ref.at[z, lax.rem(y + y_size - k, y_size), c],
                        sems.at[(n * cores + c) * y_size + k],
                    )
                )
        groups.append(group)
    for group in groups:
        for copy in group:
            copy.start()
    weights = weights_ref.reshape(model, wide)
    for n, group in enumerate(groups):
        for copy in group:
            copy.wait()
        at = slice(n * step, (n + 1) * step)
        term = jnp.dot(tokens_ref[:, at], weights[at, : 2 * width], preferred_element_type=F32)
        if n == 0:
            act_ref[...] = term
        else:
            act_ref[...] += term
    gate, up = act_ref[:, :width], act_ref[:, width:]
    inner = gate * jax.nn.sigmoid(gate) * up
    lane = lax.broadcasted_iota(jnp.int32, inner.shape, 1)
    low = jnp.where(lax.rem(y, 2) == 0, 0, width - hidden // 2)
    inner = jnp.where((lane >= low) & (lane < low + hidden // 2), inner, 0.0).astype(BF16)
    lowered = nt_dot(inner, weights[:, 2 * width :])
    part = o0.shape[0]
    for d, out_ref in enumerate((o0, o1, o2, o3)):
        out_ref[...] = lowered[d * part : (d + 1) * part].astype(out_ref.dtype)


VMEM = pl.BlockSpec(memory_space=pltpu.VMEM)
ANY = pl.BlockSpec(memory_space=pl.ANY)
SMEM = pl.BlockSpec(memory_space=pltpu.SMEM)


def shift(array, axis, by):
    size = lax.axis_size(axis)
    return lax.ppermute(array, axis, [(k, (k + by) % size) for k in range(size)])


def local(
    queries,
    forget_logits,
    value_matrix,
    output_gate_logits,
    forget_slack,
    spike_log_forget,
    head_norm_gain,
    output_weight,
    residual,
    mixer_norm_gain,
    mixer_gate_weight,
    mixer_up_weight,
    mixer_down_weight,
):
    rows, width = queries.shape
    heads = spike_log_forget.shape[1]
    model = output_weight.shape[1]
    hidden = mixer_gate_weight.shape[1]
    blocks = lax.axis_size(SP)
    n_tp = lax.axis_size("tp")
    sp_at = lax.axis_index(SP)
    tp_at = lax.axis_index("tp")
    chunk = 2 * heads * HEAD // blocks

    z_size, y_size, cores = (lax.axis_size(axis) for axis in SP)
    y_at = lax.axis_index("sp_1")
    slab = mixer_gate_weight.shape[0]
    half = (hidden // 2 + HEAD - 1) // HEAD * HEAD
    send, near, reach = pl.pallas_call(
        local_body,
        out_shape=(
            jax.ShapeDtypeStruct((blocks, chunk + 8, HEAD), BF16),
            jax.ShapeDtypeStruct((rows, width), F32),
            jax.ShapeDtypeStruct((2, rows, width), BF16),
        ),
        in_specs=[VMEM] * 5,
        out_specs=(VMEM,) * 3,
        name="local_sweep",
    )(queries, forget_logits, value_matrix, forget_slack[None], spike_log_forget.T)
    weights = (mixer_gate_weight, mixer_up_weight, mixer_down_weight.T)
    weights, send = lax.optimization_barrier((weights, send))
    got = lax.all_to_all(send, SP, 0, 0, tiled=True)
    keep, give = pl.pallas_call(
        halves_body,
        out_shape=(jax.ShapeDtypeStruct((slab, 3 * half), BF16),) * 2,
        in_specs=[SMEM] + [VMEM] * 3,
        out_specs=(VMEM,) * 2,
        name="weight_halves",
    )((y_at % 2)[None], *weights)
    line = [keep] + [shift(give if d % 2 else keep, "sp_1", d) for d in range(1, y_size)]
    whole = lax.all_gather(
        jnp.concatenate(line, axis=0), ("sp_0", "sp_2"), axis=0, tiled=True
    ).reshape(z_size, cores, y_size, slab, 3 * half)
    give = pl.pallas_call(
        scan_body,
        out_shape=jax.ShapeDtypeStruct((blocks, chunk, HEAD), BF16),
        in_specs=[SMEM, VMEM],
        out_specs=VMEM,
        name="block_scan",
    )((sp_at >= blocks // 2).astype(jnp.int32)[None], got)
    enter = lax.all_to_all(give, SP, 0, 0, tiled=True).reshape(2 * heads, HEAD, HEAD)

    part = rows // n_tp
    parts = pl.pallas_call(
        project_body,
        out_shape=(jax.ShapeDtypeStruct((part, model), BF16),) * n_tp,
        in_specs=[SMEM] + [VMEM] * 6,
        out_specs=(VMEM,) * n_tp,
        scratch_shapes=[pltpu.VMEM((rows, width), BF16)],
        name="norm_project",
    )(tp_at[None], near, reach, enter, output_gate_logits, head_norm_gain[None], output_weight)

    arrived = [parts[0]] + [shift(parts[d], "tp", d) for d in range(1, n_tp)]
    own_resid = lax.dynamic_slice_in_dim(residual, tp_at * part, part, 0)
    hidden_f = own_resid.astype(F32)
    for a in arrived:
        hidden_f = hidden_f + a.astype(F32)
    hidden_state = hidden_f.astype(BF16)
    held = hidden_state.astype(F32)
    normed = (
        held
        * lax.rsqrt(jnp.mean(held * held, axis=-1, keepdims=True) + NORM_EPS)
        * mixer_norm_gain.astype(F32)
    ).astype(BF16)
    swap = [(k, k ^ 1) for k in range(y_size)]
    both = jnp.concatenate([normed, lax.ppermute(normed, "sp_1", swap)], axis=0)
    tokens = jnp.concatenate([both] + [shift(both, "tp", d) for d in range(1, n_tp)], axis=0)
    lowered = pl.pallas_call(
        lambda *refs: mixer_body(*refs, hidden=hidden),
        out_shape=(jax.ShapeDtypeStruct((2 * part, model), F32),)
        + (jax.ShapeDtypeStruct((2 * part, model), BF16),) * (n_tp - 1),
        in_specs=[SMEM, VMEM, ANY],
        out_specs=(VMEM,) * n_tp,
        scratch_shapes=[
            pltpu.VMEM((z_size, y_size, cores, slab, 3 * half), BF16),
            pltpu.VMEM((2 * rows, 2 * half), F32),
            pltpu.SemaphoreType.DMA((2 * y_size * cores,)),
        ],
        compiler_params=pltpu.CompilerParams(vmem_limit_bytes=56 * 1024 * 1024),
        name="channel_mixer",
    )(y_at[None], tokens, whole)
    summed = lowered[0]
    for d in range(1, n_tp):
        summed = summed + shift(lowered[d], "tp", n_tp - d).astype(F32)
    theirs = lax.ppermute(summed[part:].astype(BF16), "sp_1", swap)
    return (hidden_state.astype(F32) + summed[:part] + theirs.astype(F32)).astype(BF16)


def solution(mesh):
    torus = Mesh(mesh.devices.reshape(8, 4, 2, mesh.shape["tp"]), ("sp_0", "sp_1", "sp_2", "tp"))
    return jax.shard_map(
        local,
        mesh=torus,
        in_specs=(
            P(SP, "tp"),
            P(None, SP, "tp"),
            P(SP, "tp"),
            P(SP, "tp"),
            P("tp"),
            P(SP, "tp"),
            P(),
            P("tp", None),
            P(SP, None),
            P(),
            P(SP, "tp"),
            P(SP, "tp"),
            P("tp", SP),
        ),
        out_specs=P(SP_TP, None),
        check_vma=False,
    )
```

```python
import jax
import jax.numpy as jnp
from jax import lax
from jax.experimental import pallas as pl
from jax.experimental.pallas import tpu as pltpu
from jax.sharding import Mesh
from jax.sharding import PartitionSpec as P


SP = ("sp_0", "sp_1", "sp_2")
SP_TP = ("sp_0", "sp_1", "sp_2", "tp")
NORM_EPS = 1e-06
F32 = jnp.float32
BF16 = jnp.bfloat16
HEAD = 128


def nt_dot(a, b):
    return lax.dot_general(a, b, (((1,), (1,)), ((), ())), preferred_element_type=F32)


def tn_dot(a, b):
    return lax.dot_general(a, b, (((0,), (0,)), ((), ())), preferred_element_type=F32)


def in_three(a):
    high = a.astype(BF16)
    rest = a - high.astype(F32)
    middle = rest.astype(BF16)
    return high, middle, (rest - middle.astype(F32)).astype(BF16)


def local_body(q_ref, f_ref, v_ref, slack_ref, spike_ref, send_ref, near_ref, reach_ref):
    rows = q_ref.shape[0]
    heads = spike_ref.shape[0]
    chunk = send_ref.shape[1] - 8
    pieces = HEAD // chunk
    at_row = lax.broadcasted_iota(jnp.int32, (rows, rows), 0)
    at_col = lax.broadcasted_iota(jnp.int32, (rows, rows), 1)
    spikes = []
    for w in range(2):
        keep = at_row >= at_col if w == 0 else at_row <= at_col
        ones = keep.astype(BF16)
        high, middle, low = in_three(spike_ref[...])
        spikes.append(nt_dot(ones, low) + nt_dot(ones, middle) + nt_dot(ones, high))
    for h in range(heads):
        cols = slice(h * HEAD, (h + 1) * HEAD)
        q = q_ref[:, cols].astype(F32)
        q = q * jax.nn.sigmoid(q) * HEAD ** (-0.5)
        v = v_ref[:, cols]
        scores = jnp.zeros((rows, rows), F32)
        for w in range(2):
            keep = at_row >= at_col if w == 0 else at_row <= at_col
            key = slack_ref[:, cols] * jax.nn.sigmoid(-f_ref[w, :, cols].astype(F32))
            decay = jnp.log1p(-key)
            ones = keep.astype(BF16)
            high, middle, low = in_three(decay)
            running = (
                jnp.dot(ones, low, preferred_element_type=F32)
                + jnp.dot(ones, middle, preferred_element_type=F32)
                + jnp.dot(ones, high, preferred_element_type=F32)
                + spikes[w][:, h : h + 1]
            )
            final = running[rows - 1 : rows] if w == 0 else running[0:1]
            q_scaled = (q * jnp.exp(running)).astype(BF16)
            k_scaled = (key * jnp.exp(-running)).astype(BF16)
            scores = scores + jnp.where(keep, nt_dot(q_scaled, k_scaled), 0.0)
            k_end = (key * jnp.exp(final - running)).astype(BF16)
            state = tn_dot(v, k_end).astype(BF16)
            reach_ref[w, :, cols] = q_scaled
            at = (w * heads + h) * pieces
            send_ref[at : at + pieces, 0:chunk, :] = state.reshape(pieces, chunk, HEAD)
            total = jnp.concatenate([t.astype(F32) for t in in_three(jnp.exp(final))], axis=0)
            total = jnp.concatenate([total, jnp.zeros((5, HEAD), F32)], axis=0).astype(BF16)
            send_ref[at : at + pieces, chunk : chunk + 8, :] = jnp.broadcast_to(
                total[None], (pieces, 8, HEAD)
            )
        near_ref[:, cols] = jnp.dot(scores.astype(BF16), v, preferred_element_type=F32)


def scan_body(back_ref, got_ref, give_ref):
    blocks, wide, _ = got_ref.shape
    chunk = wide - 8
    back = back_ref[0]
    state = jnp.zeros((chunk, HEAD), F32)
    for b in range(blocks):
        at = jnp.where(back == 1, blocks - 1 - b, b)
        give_ref[at] = state.astype(BF16)
        piece = got_ref[at].astype(F32)
        total = piece[chunk : chunk + 1] + piece[chunk + 1 : chunk + 2] + piece[chunk + 2 : chunk + 3]
        state = total * state + piece[0:chunk]


def project_body(
    own_ref, near_ref, reach_ref, enter_ref, gate_ref, gain_ref, weight_ref, o0, o1, o2, o3, mixed_ref
):
    heads = near_ref.shape[1] // HEAD
    gain = gain_ref[...].astype(F32)
    for h in range(heads):
        cols = slice(h * HEAD, (h + 1) * HEAD)
        mix = near_ref[:, cols]
        mix = mix + nt_dot(reach_ref[0, :, cols], enter_ref[h])
        mix = mix + nt_dot(reach_ref[1, :, cols], enter_ref[heads + h])
        scale = lax.rsqrt(jnp.mean(mix * mix, axis=-1, keepdims=True) + NORM_EPS)
        g = gate_ref[:, cols].astype(F32)
        mixed_ref[:, cols] = (mix * scale * gain * (g * jax.nn.sigmoid(g))).astype(BF16)
    outs = (o0, o1, o2, o3)
    part = o0.shape[0]
    own = own_ref[0]
    turned = jnp.concatenate(
        [
            mixed_ref[pl.ds(pl.multiple_of(lax.rem(own + d, len(outs)) * part, part), part), :]
            for d in range(len(outs))
        ],
        axis=0,
    )
    lowered = jnp.dot(turned, weight_ref[...], preferred_element_type=F32).astype(BF16)
    for d, out_ref in enumerate(outs):
        out_ref[...] = lowered[d * part : (d + 1) * part]


def halves_body(parity_ref, gate_ref, up_ref, down_ref, keep_ref, give_ref):
    hidden = gate_ref.shape[1]
    width = keep_ref.shape[1] // 3

    def write(out_ref, start):
        for k, ref in enumerate((gate_ref, up_ref, down_ref)):
            out_ref[:, k * width : (k + 1) * width] = ref[:, start : start + width]

    @pl.when(parity_ref[0] == 0)
    def _():
        write(keep_ref, 0)
        write(give_ref, hidden - width)

    @pl.when(parity_ref[0] != 0)
    def _():
        write(keep_ref, hidden - width)
        write(give_ref, 0)


def mixer_body(at_ref, *refs, hidden):
    rows_in, whole_ref, outs = refs[:8], refs[8], refs[9:17]
    tokens_ref, weights_ref, act_ref, sems = refs[17:]
    z_size, y_size, cores, _, wide = weights_ref.shape
    model = tokens_ref.shape[1]
    y = at_ref[0]
    chunks = 2
    z_step = z_size // chunks
    step = model // chunks
    width = wide // 3
    groups = []
    for n in range(chunks):
        z = slice(n * z_step, (n + 1) * z_step)
        group = []
        for c in range(cores):
            for k in range(y_size):
                group.append(
                    pltpu.make_async_copy(
                        whole_ref.at[z, c, k],
                        weights_ref.at[z, lax.rem(y + y_size - k, y_size), c],
                        sems.at[(n * cores + c) * y_size + k],
                    )
                )
        groups.append(group)
    for group in groups:
        for copy in group:
            copy.start()
    part = outs[0].shape[0]
    for n, ref in enumerate(rows_in):
        tokens_ref[n * part : (n + 1) * part, :] = ref[...]
    weights = weights_ref.reshape(model, wide)
    for n, group in enumerate(groups):
        for copy in group:
            copy.wait()
        at = slice(n * step, (n + 1) * step)
        term = jnp.dot(tokens_ref[:, at], weights[at, : 2 * width], preferred_element_type=F32)
        if n == 0:
            act_ref[...] = term
        else:
            act_ref[...] += term
    gate, up = act_ref[:, :width], act_ref[:, width:]
    inner = gate * jax.nn.sigmoid(gate) * up
    lane = lax.broadcasted_iota(jnp.int32, inner.shape, 1)
    low = jnp.where(lax.rem(y, 2) == 0, 0, width - hidden // 2)
    inner = jnp.where((lane >= low) & (lane < low + hidden // 2), inner, 0.0).astype(BF16)
    lowered = nt_dot(inner, weights[:, 2 * width :])
    for d, out_ref in enumerate(outs):
        out_ref[...] = lowered[d * part : (d + 1) * part].astype(out_ref.dtype)


VMEM = pl.BlockSpec(memory_space=pltpu.VMEM)
ANY = pl.BlockSpec(memory_space=pl.ANY)
SMEM = pl.BlockSpec(memory_space=pltpu.SMEM)


def shift(array, axis, by):
    size = lax.axis_size(axis)
    return lax.ppermute(array, axis, [(k, (k + by) % size) for k in range(size)])


def local(
    queries,
    forget_logits,
    value_matrix,
    output_gate_logits,
    forget_slack,
    spike_log_forget,
    head_norm_gain,
    output_weight,
    residual,
    mixer_norm_gain,
    mixer_gate_weight,
    mixer_up_weight,
    mixer_down_weight,
):
    rows, width = queries.shape
    heads = spike_log_forget.shape[1]
    model = output_weight.shape[1]
    hidden = mixer_gate_weight.shape[1]
    blocks = lax.axis_size(SP)
    n_tp = lax.axis_size("tp")
    sp_at = lax.axis_index(SP)
    tp_at = lax.axis_index("tp")
    chunk = 2 * heads * HEAD // blocks

    z_size, y_size, cores = (lax.axis_size(axis) for axis in SP)
    y_at = lax.axis_index("sp_1")
    slab = mixer_gate_weight.shape[0]
    half = (hidden // 2 + HEAD - 1) // HEAD * HEAD
    send, near, reach = pl.pallas_call(
        local_body,
        out_shape=(
            jax.ShapeDtypeStruct((blocks, chunk + 8, HEAD), BF16),
            jax.ShapeDtypeStruct((rows, width), F32),
            jax.ShapeDtypeStruct((2, rows, width), BF16),
        ),
        in_specs=[VMEM] * 5,
        out_specs=(VMEM,) * 3,
        name="local_sweep",
    )(queries, forget_logits, value_matrix, forget_slack[None], spike_log_forget.T)
    weights = (mixer_gate_weight, mixer_up_weight, mixer_down_weight.T)
    weights, send = lax.optimization_barrier((weights, send))
    got = lax.all_to_all(send, SP, 0, 0, tiled=True)
    keep, give = pl.pallas_call(
        halves_body,
        out_shape=(jax.ShapeDtypeStruct((slab, 3 * half), BF16),) * 2,
        in_specs=[SMEM] + [VMEM] * 3,
        out_specs=(VMEM,) * 2,
        name="weight_halves",
    )((y_at % 2)[None], *weights)
    line = [keep] + [shift(give if d % 2 else keep, "sp_1", d) for d in range(1, y_size)]
    whole = lax.all_gather(
        jnp.concatenate(line, axis=0), ("sp_0", "sp_2"), axis=0, tiled=True
    ).reshape(z_size, cores, y_size, slab, 3 * half)
    give = pl.pallas_call(
        scan_body,
        out_shape=jax.ShapeDtypeStruct((blocks, chunk, HEAD), BF16),
        in_specs=[SMEM, VMEM],
        out_specs=VMEM,
        name="block_scan",
    )((sp_at >= blocks // 2).astype(jnp.int32)[None], got)
    enter = lax.all_to_all(give, SP, 0, 0, tiled=True).reshape(2 * heads, HEAD, HEAD)

    part = rows // n_tp
    parts = pl.pallas_call(
        project_body,
        out_shape=(jax.ShapeDtypeStruct((part, model), BF16),) * n_tp,
        in_specs=[SMEM] + [VMEM] * 6,
        out_specs=(VMEM,) * n_tp,
        scratch_shapes=[pltpu.VMEM((rows, width), BF16)],
        name="norm_project",
    )(tp_at[None], near, reach, enter, output_gate_logits, head_norm_gain[None], output_weight)

    arrived = [parts[0]] + [shift(parts[d], "tp", d) for d in range(1, n_tp)]
    own_resid = lax.dynamic_slice_in_dim(residual, tp_at * part, part, 0)
    hidden_f = own_resid.astype(F32)
    for a in arrived:
        hidden_f = hidden_f + a.astype(F32)
    hidden_state = hidden_f.astype(BF16)
    held = hidden_state.astype(F32)
    normed = (
        held
        * lax.rsqrt(jnp.mean(held * held, axis=-1, keepdims=True) + NORM_EPS)
        * mixer_norm_gain.astype(F32)
    ).astype(BF16)
    swap = [(k, k ^ 1) for k in range(y_size)]
    theirs = lax.ppermute(normed, "sp_1", swap)
    tokens = [normed] + [shift(normed, "tp", d) for d in range(1, n_tp)]
    tokens += [theirs] + [shift(theirs, "tp", d) for d in range(1, n_tp)]
    kept = (jax.ShapeDtypeStruct((part, model), F32),)
    sent = (jax.ShapeDtypeStruct((part, model), BF16),) * (n_tp - 1)
    lowered = pl.pallas_call(
        lambda *refs: mixer_body(*refs, hidden=hidden),
        out_shape=(kept + sent) * 2,
        in_specs=[SMEM] + [VMEM] * (2 * n_tp) + [ANY],
        out_specs=(VMEM,) * (2 * n_tp),
        scratch_shapes=[
            pltpu.VMEM((2 * rows, model), BF16),
            pltpu.VMEM((z_size, y_size, cores, slab, 3 * half), BF16),
            pltpu.VMEM((2 * rows, 2 * half), F32),
            pltpu.SemaphoreType.DMA((2 * y_size * cores,)),
        ],
        compiler_params=pltpu.CompilerParams(vmem_limit_bytes=54 * 1024 * 1024),
        name="channel_mixer",
    )(y_at[None], *tokens, whole)
    mine, other = lowered[:n_tp], lowered[n_tp:]
    other = [other[0]] + [shift(other[d], "tp", n_tp - d) for d in range(1, n_tp)]
    mine = [mine[0]] + [shift(mine[d], "tp", n_tp - d) for d in range(1, n_tp)]
    theirs = lax.ppermute(sum(a.astype(F32) for a in other).astype(BF16), "sp_1", swap)
    return (sum((a.astype(F32) for a in mine), hidden_state.astype(F32)) + theirs.astype(F32)).astype(BF16)


def solution(mesh):
    torus = Mesh(mesh.devices.reshape(8, 4, 2, mesh.shape["tp"]), ("sp_0", "sp_1", "sp_2", "tp"))
    return jax.shard_map(
        local,
        mesh=torus,
        in_specs=(
            P(SP, "tp"),
            P(None, SP, "tp"),
            P(SP, "tp"),
            P(SP, "tp"),
            P("tp"),
            P(SP, "tp"),
            P(),
            P("tp", None),
            P(SP, None),
            P(),
            P(SP, "tp"),
            P(SP, "tp"),
            P("tp", SP),
        ),
        out_specs=P(SP_TP, None),
        check_vma=False,
    )
```

```python
import jax
import jax.numpy as jnp
from jax import lax
from jax.experimental import pallas as pl
from jax.experimental.pallas import tpu as pltpu
from jax.sharding import Mesh
from jax.sharding import PartitionSpec as P


SP = ("sp_0", "sp_1", "sp_2")
SP_TP = ("sp_0", "sp_1", "sp_2", "tp")
NORM_EPS = 1e-06
F32 = jnp.float32
BF16 = jnp.bfloat16
HEAD = 128


def nt_dot(a, b):
    return lax.dot_general(a, b, (((1,), (1,)), ((), ())), preferred_element_type=F32)


def tn_dot(a, b):
    return lax.dot_general(a, b, (((0,), (0,)), ((), ())), preferred_element_type=F32)


def in_three(a):
    high = a.astype(BF16)
    rest = a - high.astype(F32)
    middle = rest.astype(BF16)
    return high, middle, (rest - middle.astype(F32)).astype(BF16)


def local_body(q_ref, f_ref, v_ref, slack_ref, spike_ref, send_ref, near_ref, reach_ref):
    rows = q_ref.shape[0]
    heads = spike_ref.shape[0]
    chunk = send_ref.shape[1] - 8
    pieces = HEAD // chunk
    at_row = lax.broadcasted_iota(jnp.int32, (rows, rows), 0)
    at_col = lax.broadcasted_iota(jnp.int32, (rows, rows), 1)
    spikes = []
    for w in range(2):
        keep = at_row >= at_col if w == 0 else at_row <= at_col
        ones = keep.astype(BF16)
        high, middle, low = in_three(spike_ref[...])
        spikes.append(nt_dot(ones, low) + nt_dot(ones, middle) + nt_dot(ones, high))
    for h in range(heads):
        cols = slice(h * HEAD, (h + 1) * HEAD)
        q = q_ref[:, cols].astype(F32)
        q = q * jax.nn.sigmoid(q) * HEAD ** (-0.5)
        v = v_ref[:, cols]
        scores = jnp.zeros((rows, rows), F32)
        for w in range(2):
            keep = at_row >= at_col if w == 0 else at_row <= at_col
            key = slack_ref[:, cols] * jax.nn.sigmoid(-f_ref[w, :, cols].astype(F32))
            decay = jnp.log1p(-key)
            ones = keep.astype(BF16)
            high, middle, low = in_three(decay)
            running = (
                jnp.dot(ones, low, preferred_element_type=F32)
                + jnp.dot(ones, middle, preferred_element_type=F32)
                + jnp.dot(ones, high, preferred_element_type=F32)
                + spikes[w][:, h : h + 1]
            )
            final = running[rows - 1 : rows] if w == 0 else running[0:1]
            q_scaled = (q * jnp.exp(running)).astype(BF16)
            k_scaled = (key * jnp.exp(-running)).astype(BF16)
            scores = scores + jnp.where(keep, nt_dot(q_scaled, k_scaled), 0.0)
            k_end = (key * jnp.exp(final - running)).astype(BF16)
            state = tn_dot(v, k_end).astype(BF16)
            reach_ref[w, :, cols] = q_scaled
            at = (w * heads + h) * pieces
            send_ref[at : at + pieces, 0:chunk, :] = state.reshape(pieces, chunk, HEAD)
            total = jnp.concatenate([t.astype(F32) for t in in_three(jnp.exp(final))], axis=0)
            total = jnp.concatenate([total, jnp.zeros((5, HEAD), F32)], axis=0).astype(BF16)
            send_ref[at : at + pieces, chunk : chunk + 8, :] = jnp.broadcast_to(
                total[None], (pieces, 8, HEAD)
            )
        near_ref[:, cols] = jnp.dot(scores.astype(BF16), v, preferred_element_type=F32)


def scan_body(back_ref, got_ref, give_ref):
    blocks, wide, _ = got_ref.shape
    chunk = wide - 8
    back = back_ref[0]
    state = jnp.zeros((chunk, HEAD), F32)
    for b in range(blocks):
        at = jnp.where(back == 1, blocks - 1 - b, b)
        give_ref[at] = state.astype(BF16)
        piece = got_ref[at].astype(F32)
        total = piece[chunk : chunk + 1] + piece[chunk + 1 : chunk + 2] + piece[chunk + 2 : chunk + 3]
        state = total * state + piece[0:chunk]


def project_body(
    own_ref, near_ref, reach_ref, enter_ref, gate_ref, gain_ref, weight_ref, o0, o1, o2, o3, mixed_ref
):
    heads = near_ref.shape[1] // HEAD
    gain = gain_ref[...].astype(F32)
    for h in range(heads):
        cols = slice(h * HEAD, (h + 1) * HEAD)
        mix = near_ref[:, cols]
        mix = mix + nt_dot(reach_ref[0, :, cols], enter_ref[h])
        mix = mix + nt_dot(reach_ref[1, :, cols], enter_ref[heads + h])
        scale = lax.rsqrt(jnp.mean(mix * mix, axis=-1, keepdims=True) + NORM_EPS)
        g = gate_ref[:, cols].astype(F32)
        mixed_ref[:, cols] = (mix * scale * gain * (g * jax.nn.sigmoid(g))).astype(BF16)
    outs = (o0, o1, o2, o3)
    part = o0.shape[0]
    own = own_ref[0]
    turned = jnp.concatenate(
        [
            mixed_ref[pl.ds(pl.multiple_of(lax.rem(own + d, len(outs)) * part, part), part), :]
            for d in range(len(outs))
        ],
        axis=0,
    )
    lowered = jnp.dot(turned, weight_ref[...], preferred_element_type=F32).astype(BF16)
    for d, out_ref in enumerate(outs):
        out_ref[...] = lowered[d * part : (d + 1) * part]


def halves_body(parity_ref, gate_ref, up_ref, down_ref, keep_ref, give_ref):
    hidden = gate_ref.shape[1]
    width = keep_ref.shape[1] // 3

    def write(out_ref, start):
        for k, ref in enumerate((gate_ref, up_ref, down_ref)):
            out_ref[:, k * width : (k + 1) * width] = ref[:, start : start + width]

    @pl.when(parity_ref[0] == 0)
    def _():
        write(keep_ref, 0)
        write(give_ref, hidden - width)

    @pl.when(parity_ref[0] != 0)
    def _():
        write(keep_ref, hidden - width)
        write(give_ref, 0)


def mixer_body(at_ref, *refs, hidden):
    (own_ref, near_ref), x_refs, whole_ref, outs = refs[:2], refs[2:6], refs[6], refs[7:13]
    tokens_ref, weights_ref, act_ref, sems = refs[13:]
    z_size, y_size, cores, _, wide = weights_ref.shape
    model = tokens_ref.shape[1]
    y = at_ref[0]
    chunks = 4
    z_step = z_size // chunks
    step = model // chunks
    width = wide // 3
    groups = []
    for n in range(chunks):
        z = slice(n * z_step, (n + 1) * z_step)
        group = []
        for c in range(cores):
            for k in range(y_size):
                group.append(
                    pltpu.make_async_copy(
                        whole_ref.at[z, c, k],
                        weights_ref.at[z, lax.rem(y + y_size - k, y_size), c],
                        sems.at[(n * cores + c) * y_size + k],
                    )
                )
        groups.append(group)
    for group in groups:
        for copy in group:
            copy.start()
    split = model // 2
    rows = own_ref.shape[0]
    part = rows // len(x_refs)
    tokens_ref[:rows, :split] = own_ref[...]
    tokens_ref[rows:, :split] = near_ref[...]
    for d, ref in enumerate(x_refs):
        tokens_ref[d * part : (d + 1) * part, split:] = ref[:part]
        tokens_ref[rows + d * part : rows + (d + 1) * part, split:] = ref[part:]
    weights = weights_ref.reshape(model, wide)
    for n, group in enumerate(groups):
        for copy in group:
            copy.wait()
        at = slice(n * step, (n + 1) * step)
        term = jnp.dot(tokens_ref[:, at], weights[at, : 2 * width], preferred_element_type=F32)
        if n == 0:
            act_ref[...] = term
        else:
            act_ref[...] += term
    gate, up = act_ref[:, :width], act_ref[:, width:]
    inner = gate * jax.nn.sigmoid(gate) * up
    lane = lax.broadcasted_iota(jnp.int32, inner.shape, 1)
    low = jnp.where(lax.rem(y, 2) == 0, 0, width - hidden // 2)
    inner = jnp.where((lane >= low) & (lane < low + hidden // 2), inner, 0.0).astype(BF16)
    lowered = nt_dot(inner, weights[:, 2 * width :])
    for d, out_ref in enumerate(outs[:4]):
        at = slice(d * part, (d + 1) * part)
        out_ref[:part] = lowered[:rows][at, :split].astype(out_ref.dtype)
        out_ref[part:] = lowered[rows:][at, :split].astype(out_ref.dtype)
    outs[4][...] = lowered[:rows, split:]
    outs[5][...] = lowered[rows:, split:].astype(BF16)


VMEM = pl.BlockSpec(memory_space=pltpu.VMEM)
ANY = pl.BlockSpec(memory_space=pl.ANY)
SMEM = pl.BlockSpec(memory_space=pltpu.SMEM)


def shift(array, axis, by):
    size = lax.axis_size(axis)
    return lax.ppermute(array, axis, [(k, (k + by) % size) for k in range(size)])


def local(
    queries,
    forget_logits,
    value_matrix,
    output_gate_logits,
    forget_slack,
    spike_log_forget,
    head_norm_gain,
    output_weight,
    residual,
    mixer_norm_gain,
    mixer_gate_weight,
    mixer_up_weight,
    mixer_down_weight,
):
    rows, width = queries.shape
    heads = spike_log_forget.shape[1]
    model = output_weight.shape[1]
    hidden = mixer_gate_weight.shape[1]
    blocks = lax.axis_size(SP)
    n_tp = lax.axis_size("tp")
    sp_at = lax.axis_index(SP)
    tp_at = lax.axis_index("tp")
    chunk = 2 * heads * HEAD // blocks

    z_size, y_size, cores = (lax.axis_size(axis) for axis in SP)
    y_at = lax.axis_index("sp_1")
    slab = mixer_gate_weight.shape[0]
    half = (hidden // 2 + HEAD - 1) // HEAD * HEAD
    send, near, reach = pl.pallas_call(
        local_body,
        out_shape=(
            jax.ShapeDtypeStruct((blocks, chunk + 8, HEAD), BF16),
            jax.ShapeDtypeStruct((rows, width), F32),
            jax.ShapeDtypeStruct((2, rows, width), BF16),
        ),
        in_specs=[VMEM] * 5,
        out_specs=(VMEM,) * 3,
        name="local_sweep",
    )(queries, forget_logits, value_matrix, forget_slack[None], spike_log_forget.T)
    weights = (mixer_gate_weight, mixer_up_weight, mixer_down_weight.T)
    weights, send = lax.optimization_barrier((weights, send))
    got = lax.all_to_all(send, SP, 0, 0, tiled=True)
    keep, give = pl.pallas_call(
        halves_body,
        out_shape=(jax.ShapeDtypeStruct((slab, 3 * half), BF16),) * 2,
        in_specs=[SMEM] + [VMEM] * 3,
        out_specs=(VMEM,) * 2,
        name="weight_halves",
    )((y_at % 2)[None], *weights)
    line = [keep] + [shift(give if d % 2 else keep, "sp_1", d) for d in range(1, y_size)]
    line = jnp.concatenate(line, axis=0)
    whole = lax.all_gather(line, ("sp_0", "sp_2"), axis=0, tiled=True).reshape(z_size, cores, y_size, slab, 3 * half)
    give = pl.pallas_call(
        scan_body,
        out_shape=jax.ShapeDtypeStruct((blocks, chunk, HEAD), BF16),
        in_specs=[SMEM, VMEM],
        out_specs=VMEM,
        name="block_scan",
    )((sp_at >= blocks // 2).astype(jnp.int32)[None], got)
    enter = lax.all_to_all(give, SP, 0, 0, tiled=True).reshape(2 * heads, HEAD, HEAD)

    part = rows // n_tp
    parts = pl.pallas_call(
        project_body,
        out_shape=(jax.ShapeDtypeStruct((part, model), BF16),) * n_tp,
        in_specs=[SMEM] + [VMEM] * 6,
        out_specs=(VMEM,) * n_tp,
        scratch_shapes=[pltpu.VMEM((rows, width), BF16)],
        name="norm_project",
    )(tp_at[None], near, reach, enter, output_gate_logits, head_norm_gain[None], output_weight)

    arrived = [parts[0]] + [shift(parts[d], "tp", d) for d in range(1, n_tp)]
    own_resid = lax.dynamic_slice_in_dim(residual, tp_at * part, part, 0)
    hidden_f = own_resid.astype(F32)
    for a in arrived:
        hidden_f = hidden_f + a.astype(F32)
    hidden_state = hidden_f.astype(BF16)
    held = hidden_state.astype(F32)
    normed = (
        held
        * lax.rsqrt(jnp.mean(held * held, axis=-1, keepdims=True) + NORM_EPS)
        * mixer_norm_gain.astype(F32)
    ).astype(BF16)
    swap = [(k, k ^ 1) for k in range(y_size)]
    split = model // 2
    left, right = normed[:, :split], normed[:, split:]
    both = jnp.concatenate([right, lax.ppermute(right, "sp_1", swap)], axis=0)
    own = jnp.concatenate([left] + [shift(left, "tp", d) for d in range(1, n_tp)], axis=0)
    tokens = [own, lax.ppermute(own, "sp_1", swap)]
    tokens += [both] + [shift(both, "tp", d) for d in range(1, n_tp)]
    lowered = pl.pallas_call(
        lambda *refs: mixer_body(*refs, hidden=hidden),
        out_shape=(jax.ShapeDtypeStruct((2 * part, split), F32),)
        + (jax.ShapeDtypeStruct((2 * part, split), BF16),) * (n_tp - 1)
        + (jax.ShapeDtypeStruct((rows, split), F32), jax.ShapeDtypeStruct((rows, split), BF16)),
        in_specs=[SMEM] + [VMEM] * len(tokens) + [ANY],
        out_specs=(VMEM,) * (n_tp + 2),
        scratch_shapes=[
            pltpu.VMEM((2 * rows, model), BF16),
            pltpu.VMEM((z_size, y_size, cores, slab, 3 * half), BF16),
            pltpu.VMEM((2 * rows, 2 * half), F32),
            pltpu.SemaphoreType.DMA((4 * y_size * cores,)),
        ],
        compiler_params=pltpu.CompilerParams(vmem_limit_bytes=54 * 1024 * 1024),
        name="channel_mixer",
    )(y_at[None], *tokens, whole)
    crossed = lax.ppermute(lowered[n_tp + 1], "sp_1", swap)
    sums = lowered[0]
    for d in range(1, n_tp):
        sums = sums + shift(lowered[d], "tp", n_tp - d).astype(F32)
    added = lowered[n_tp] + crossed.astype(F32)
    out_right = hidden_state[:, split:].astype(F32) + added[:part]
    for d in range(1, n_tp):
        back = added[d * part : (d + 1) * part].astype(BF16)
        out_right = out_right + shift(back, "tp", n_tp - d).astype(F32)
    theirs = lax.ppermute(sums[part:].astype(BF16), "sp_1", swap)
    out_left = hidden_state[:, :split].astype(F32) + sums[:part] + theirs.astype(F32)
    return jnp.concatenate([out_left, out_right], axis=1).astype(BF16)


def solution(mesh):
    torus = Mesh(mesh.devices.reshape(8, 4, 2, mesh.shape["tp"]), ("sp_0", "sp_1", "sp_2", "tp"))
    return jax.shard_map(
        local,
        mesh=torus,
        in_specs=(
            P(SP, "tp"),
            P(None, SP, "tp"),
            P(SP, "tp"),
            P(SP, "tp"),
            P("tp"),
            P(SP, "tp"),
            P(),
            P("tp", None),
            P(SP, None),
            P(),
            P(SP, "tp"),
            P(SP, "tp"),
            P("tp", SP),
        ),
        out_specs=P(SP_TP, None),
        check_vma=False,
    )
```

```python
import jax
import jax.numpy as jnp
from jax import lax
from jax.experimental import pallas as pl
from jax.experimental.pallas import tpu as pltpu
from jax.sharding import Mesh
from jax.sharding import PartitionSpec as P


SP = ("sp_0", "sp_1", "sp_2")
SP_TP = ("sp_0", "sp_1", "sp_2", "tp")
NORM_EPS = 1e-06
F32 = jnp.float32
BF16 = jnp.bfloat16
HEAD = 128


def nt_dot(a, b):
    return lax.dot_general(a, b, (((1,), (1,)), ((), ())), preferred_element_type=F32)


def tn_dot(a, b):
    return lax.dot_general(a, b, (((0,), (0,)), ((), ())), preferred_element_type=F32)


def in_three(a):
    high = a.astype(BF16)
    rest = a - high.astype(F32)
    middle = rest.astype(BF16)
    return high, middle, (rest - middle.astype(F32)).astype(BF16)


def local_body(
    parity_ref,
    q_ref,
    f_ref,
    v_ref,
    slack_ref,
    spike_ref,
    w_gate_ref,
    w_up_ref,
    w_down_ref,
    send_ref,
    near_ref,
    reach_ref,
    keep_ref,
    give_ref,
):
    halves_body(parity_ref, w_gate_ref, w_up_ref, w_down_ref, keep_ref, give_ref)
    rows = q_ref.shape[0]
    heads = spike_ref.shape[0]
    chunk = send_ref.shape[1] - 8
    pieces = HEAD // chunk
    at_row = lax.broadcasted_iota(jnp.int32, (rows, rows), 0)
    at_col = lax.broadcasted_iota(jnp.int32, (rows, rows), 1)
    spikes = []
    for w in range(2):
        keep = at_row >= at_col if w == 0 else at_row <= at_col
        ones = keep.astype(BF16)
        high, middle, low = in_three(spike_ref[...])
        spikes.append(nt_dot(ones, low) + nt_dot(ones, middle) + nt_dot(ones, high))
    for h in range(heads):
        cols = slice(h * HEAD, (h + 1) * HEAD)
        q = q_ref[:, cols].astype(F32)
        q = q * jax.nn.sigmoid(q) * HEAD ** (-0.5)
        v = v_ref[:, cols]
        scores = jnp.zeros((rows, rows), F32)
        for w in range(2):
            keep = at_row >= at_col if w == 0 else at_row <= at_col
            key = slack_ref[:, cols] * jax.nn.sigmoid(-f_ref[w, :, cols].astype(F32))
            decay = jnp.log1p(-key)
            ones = keep.astype(BF16)
            high, middle, low = in_three(decay)
            running = (
                jnp.dot(ones, low, preferred_element_type=F32)
                + jnp.dot(ones, middle, preferred_element_type=F32)
                + jnp.dot(ones, high, preferred_element_type=F32)
                + spikes[w][:, h : h + 1]
            )
            final = running[rows - 1 : rows] if w == 0 else running[0:1]
            q_scaled = (q * jnp.exp(running)).astype(BF16)
            k_scaled = (key * jnp.exp(-running)).astype(BF16)
            scores = scores + jnp.where(keep, nt_dot(q_scaled, k_scaled), 0.0)
            k_end = (key * jnp.exp(final - running)).astype(BF16)
            state = tn_dot(v, k_end).astype(BF16)
            reach_ref[w, :, cols] = q_scaled
            at = (w * heads + h) * pieces
            send_ref[at : at + pieces, 0:chunk, :] = state.reshape(pieces, chunk, HEAD)
            total = jnp.concatenate([t.astype(F32) for t in in_three(jnp.exp(final))], axis=0)
            total = jnp.concatenate([total, jnp.zeros((5, HEAD), F32)], axis=0).astype(BF16)
            send_ref[at : at + pieces, chunk : chunk + 8, :] = jnp.broadcast_to(
                total[None], (pieces, 8, HEAD)
            )
        near_ref[:, cols] = jnp.dot(scores.astype(BF16), v, preferred_element_type=F32)


def scan_body(back_ref, got_ref, give_ref):
    blocks, wide, _ = got_ref.shape
    chunk = wide - 8
    back = back_ref[0]
    state = jnp.zeros((chunk, HEAD), F32)
    for b in range(blocks):
        at = jnp.where(back == 1, blocks - 1 - b, b)
        give_ref[at] = state.astype(BF16)
        piece = got_ref[at].astype(F32)
        total = piece[chunk : chunk + 1] + piece[chunk + 1 : chunk + 2] + piece[chunk + 2 : chunk + 3]
        state = total * state + piece[0:chunk]


def project_body(
    own_ref, near_ref, reach_ref, enter_ref, gate_ref, gain_ref, weight_ref, o0, o1, o2, o3, mixed_ref
):
    heads = near_ref.shape[1] // HEAD
    gain = gain_ref[...].astype(F32)
    for h in range(heads):
        cols = slice(h * HEAD, (h + 1) * HEAD)
        mix = near_ref[:, cols]
        mix = mix + nt_dot(reach_ref[0, :, cols], enter_ref[h])
        mix = mix + nt_dot(reach_ref[1, :, cols], enter_ref[heads + h])
        scale = lax.rsqrt(jnp.mean(mix * mix, axis=-1, keepdims=True) + NORM_EPS)
        g = gate_ref[:, cols].astype(F32)
        mixed_ref[:, cols] = (mix * scale * gain * (g * jax.nn.sigmoid(g))).astype(BF16)
    outs = (o0, o1, o2, o3)
    part = o0.shape[0]
    own = own_ref[0]
    turned = jnp.concatenate(
        [
            mixed_ref[pl.ds(pl.multiple_of(lax.rem(own + d, len(outs)) * part, part), part), :]
            for d in range(len(outs))
        ],
        axis=0,
    )
    lowered = jnp.dot(turned, weight_ref[...], preferred_element_type=F32).astype(BF16)
    for d, out_ref in enumerate(outs):
        out_ref[...] = lowered[d * part : (d + 1) * part]


def halves_body(parity_ref, gate_ref, up_ref, down_ref, keep_ref, give_ref):
    hidden = gate_ref.shape[1]
    width = keep_ref.shape[1] // 3

    def write(out_ref, start):
        for k, ref in enumerate((gate_ref, up_ref, down_ref)):
            out_ref[:, k * width : (k + 1) * width] = ref[:, start : start + width]

    @pl.when(parity_ref[0] == 0)
    def _():
        write(keep_ref, 0)
        write(give_ref, hidden - width)

    @pl.when(parity_ref[0] != 0)
    def _():
        write(keep_ref, hidden - width)
        write(give_ref, 0)


def in_order_body(at_ref, whole_ref, weights_ref, sems):
    _, y_size, cores, _, _ = weights_ref.shape
    y = at_ref[0]
    copies = []
    for c in range(cores):
        for k in range(y_size):
            copies.append(
                pltpu.make_async_copy(
                    whole_ref.at[:, c, k],
                    weights_ref.at[:, lax.rem(y + y_size - k, y_size), c],
                    sems.at[c * y_size + k],
                )
            )
    for copy in copies:
        copy.start()
    for copy in copies:
        copy.wait()


def mixer_body(at_ref, *refs, hidden):
    (own_ref, near_ref), x_refs, weights_ref, outs = refs[:2], refs[2:6], refs[6], refs[7:13]
    tokens_ref = refs[13]
    model, wide = weights_ref.shape
    y = at_ref[0]
    width = wide // 3
    split = model // 2
    rows = own_ref.shape[0]
    part = rows // len(x_refs)
    tokens_ref[:rows, :split] = own_ref[...]
    tokens_ref[rows:, :split] = near_ref[...]
    for d, ref in enumerate(x_refs):
        tokens_ref[d * part : (d + 1) * part, split:] = ref[:part]
        tokens_ref[rows + d * part : rows + (d + 1) * part, split:] = ref[part:]
    act = jnp.dot(tokens_ref[...], weights_ref[:, : 2 * width], preferred_element_type=F32)
    gate, up = act[:, :width], act[:, width:]
    inner = gate * jax.nn.sigmoid(gate) * up
    lane = lax.broadcasted_iota(jnp.int32, inner.shape, 1)
    low = jnp.where(lax.rem(y, 2) == 0, 0, width - hidden // 2)
    inner = jnp.where((lane >= low) & (lane < low + hidden // 2), inner, 0.0).astype(BF16)
    lowered = nt_dot(inner, weights_ref[:, 2 * width :])
    for d, out_ref in enumerate(outs[:4]):
        at = slice(d * part, (d + 1) * part)
        out_ref[:part] = lowered[:rows][at, :split].astype(out_ref.dtype)
        out_ref[part:] = lowered[rows:][at, :split].astype(out_ref.dtype)
    outs[4][...] = lowered[:rows, split:]
    outs[5][...] = lowered[rows:, split:].astype(BF16)


VMEM = pl.BlockSpec(memory_space=pltpu.VMEM)
ANY = pl.BlockSpec(memory_space=pl.ANY)
SMEM = pl.BlockSpec(memory_space=pltpu.SMEM)


def shift(array, axis, by):
    size = lax.axis_size(axis)
    return lax.ppermute(array, axis, [(k, (k + by) % size) for k in range(size)])


def local(
    queries,
    forget_logits,
    value_matrix,
    output_gate_logits,
    forget_slack,
    spike_log_forget,
    head_norm_gain,
    output_weight,
    residual,
    mixer_norm_gain,
    mixer_gate_weight,
    mixer_up_weight,
    mixer_down_weight,
):
    rows, width = queries.shape
    heads = spike_log_forget.shape[1]
    model = output_weight.shape[1]
    hidden = mixer_gate_weight.shape[1]
    blocks = lax.axis_size(SP)
    n_tp = lax.axis_size("tp")
    sp_at = lax.axis_index(SP)
    tp_at = lax.axis_index("tp")
    chunk = 2 * heads * HEAD // blocks

    z_size, y_size, cores = (lax.axis_size(axis) for axis in SP)
    y_at = lax.axis_index("sp_1")
    slab = mixer_gate_weight.shape[0]
    half = (hidden // 2 + HEAD - 1) // HEAD * HEAD
    send, near, reach, keep, give = pl.pallas_call(
        local_body,
        out_shape=(
            jax.ShapeDtypeStruct((blocks, chunk + 8, HEAD), BF16),
            jax.ShapeDtypeStruct((rows, width), F32),
            jax.ShapeDtypeStruct((2, rows, width), BF16),
            jax.ShapeDtypeStruct((slab, 3 * half), BF16),
            jax.ShapeDtypeStruct((slab, 3 * half), BF16),
        ),
        in_specs=[SMEM] + [VMEM] * 8,
        out_specs=(VMEM,) * 5,
        name="local_sweep",
    )(
        (y_at % 2)[None],
        queries,
        forget_logits,
        value_matrix,
        forget_slack[None],
        spike_log_forget.T,
        mixer_gate_weight,
        mixer_up_weight,
        mixer_down_weight.T,
    )
    got = lax.all_to_all(send, SP, 0, 0, tiled=True)
    line = [keep] + [shift(give if d % 2 else keep, "sp_1", d) for d in range(1, y_size)]
    line = jnp.concatenate(line, axis=0)
    whole = lax.all_gather(line, ("sp_0", "sp_2"), axis=0, tiled=True).reshape(z_size, cores, y_size, slab, 3 * half)
    give = pl.pallas_call(
        scan_body,
        out_shape=jax.ShapeDtypeStruct((blocks, chunk, HEAD), BF16),
        in_specs=[SMEM, VMEM],
        out_specs=VMEM,
        compiler_params=pltpu.CompilerParams(vmem_limit_bytes=12 * 1024 * 1024),
        name="block_scan",
    )((sp_at >= blocks // 2).astype(jnp.int32)[None], got)
    enter = lax.all_to_all(give, SP, 0, 0, tiled=True).reshape(2 * heads, HEAD, HEAD)

    part = rows // n_tp
    parts = pl.pallas_call(
        project_body,
        out_shape=(jax.ShapeDtypeStruct((part, model), BF16),) * n_tp,
        in_specs=[SMEM] + [VMEM] * 6,
        out_specs=(VMEM,) * n_tp,
        scratch_shapes=[pltpu.VMEM((rows, width), BF16)],
        name="norm_project",
    )(tp_at[None], near, reach, enter, output_gate_logits, head_norm_gain[None], output_weight)

    arrived = [parts[0]] + [shift(parts[d], "tp", d) for d in range(1, n_tp)]
    own_resid = lax.dynamic_slice_in_dim(residual, tp_at * part, part, 0)
    hidden_f = own_resid.astype(F32)
    for a in arrived:
        hidden_f = hidden_f + a.astype(F32)
    hidden_state = hidden_f.astype(BF16)
    held = hidden_state.astype(F32)
    normed = (
        held
        * lax.rsqrt(jnp.mean(held * held, axis=-1, keepdims=True) + NORM_EPS)
        * mixer_norm_gain.astype(F32)
    ).astype(BF16)
    swap = [(k, k ^ 1) for k in range(y_size)]
    split = model // 2
    left, right = normed[:, :split], normed[:, split:]
    both = jnp.concatenate([right, lax.ppermute(right, "sp_1", swap)], axis=0)
    own = jnp.concatenate([left] + [shift(left, "tp", d) for d in range(1, n_tp)], axis=0)
    lines = [both] + [shift(both, "tp", d) for d in range(1, n_tp)]
    tokens = [own, lax.ppermute(own, "sp_1", swap)] + lines
    weights = pl.pallas_call(
        in_order_body,
        out_shape=jax.ShapeDtypeStruct((z_size, y_size, cores, slab, 3 * half), BF16),
        in_specs=[SMEM, ANY],
        out_specs=VMEM,
        scratch_shapes=[pltpu.SemaphoreType.DMA((y_size * cores,))],
        compiler_params=pltpu.CompilerParams(vmem_limit_bytes=40 * 1024 * 1024),
        name="weights_in_order",
    )(y_at[None], whole)
    weights = weights.reshape(model, 3 * half)
    lowered = pl.pallas_call(
        lambda *refs: mixer_body(*refs, hidden=hidden),
        out_shape=(jax.ShapeDtypeStruct((2 * part, split), F32),)
        + (jax.ShapeDtypeStruct((2 * part, split), BF16),) * (n_tp - 1)
        + (jax.ShapeDtypeStruct((rows, split), F32), jax.ShapeDtypeStruct((rows, split), BF16)),
        in_specs=[SMEM] + [VMEM] * (len(tokens) + 1),
        out_specs=(VMEM,) * (n_tp + 2),
        scratch_shapes=[pltpu.VMEM((2 * rows, model), BF16)],
        compiler_params=pltpu.CompilerParams(vmem_limit_bytes=24 * 1024 * 1024),
        name="channel_mixer",
    )(y_at[None], *tokens, weights)
    crossed = lax.ppermute(lowered[n_tp + 1], "sp_1", swap)
    sums = lowered[0]
    for d in range(1, n_tp):
        sums = sums + shift(lowered[d], "tp", n_tp - d).astype(F32)
    added = lowered[n_tp] + crossed.astype(F32)
    out_right = hidden_state[:, split:].astype(F32) + added[:part]
    for d in range(1, n_tp):
        back = added[d * part : (d + 1) * part].astype(BF16)
        out_right = out_right + shift(back, "tp", n_tp - d).astype(F32)
    theirs = lax.ppermute(sums[part:].astype(BF16), "sp_1", swap)
    out_left = hidden_state[:, :split].astype(F32) + sums[:part] + theirs.astype(F32)
    return jnp.concatenate([out_left, out_right], axis=1).astype(BF16)


def solution(mesh):
    torus = Mesh(mesh.devices.reshape(8, 4, 2, mesh.shape["tp"]), ("sp_0", "sp_1", "sp_2", "tp"))
    return jax.shard_map(
        local,
        mesh=torus,
        in_specs=(
            P(SP, "tp"),
            P(None, SP, "tp"),
            P(SP, "tp"),
            P(SP, "tp"),
            P("tp"),
            P(SP, "tp"),
            P(),
            P("tp", None),
            P(SP, None),
            P(),
            P(SP, "tp"),
            P(SP, "tp"),
            P("tp", SP),
        ),
        out_specs=P(SP_TP, None),
        check_vma=False,
    )
```

```python
import jax
import jax.numpy as jnp
from jax import lax
from jax.experimental import pallas as pl
from jax.experimental.pallas import tpu as pltpu
from jax.sharding import Mesh
from jax.sharding import PartitionSpec as P


SP = ("sp_0", "sp_1", "sp_2")
SP_TP = ("sp_0", "sp_1", "sp_2", "tp")
NORM_EPS = 1e-06
F32 = jnp.float32
BF16 = jnp.bfloat16
HEAD = 128


def nt_dot(a, b):
    return lax.dot_general(a, b, (((1,), (1,)), ((), ())), preferred_element_type=F32)


def tn_dot(a, b):
    return lax.dot_general(a, b, (((0,), (0,)), ((), ())), preferred_element_type=F32)


def in_three(a):
    high = a.astype(BF16)
    rest = a - high.astype(F32)
    middle = rest.astype(BF16)
    return high, middle, (rest - middle.astype(F32)).astype(BF16)


def local_body(
    parity_ref,
    q_ref,
    f_ref,
    v_ref,
    slack_ref,
    spike_ref,
    w_gate_ref,
    w_up_ref,
    w_down_ref,
    send_ref,
    near_ref,
    reach_ref,
    keep_ref,
    give_ref,
):
    halves_body(parity_ref, w_gate_ref, w_up_ref, w_down_ref, keep_ref, give_ref)
    rows = q_ref.shape[0]
    heads = spike_ref.shape[0]
    chunk = send_ref.shape[1] - 8
    pieces = HEAD // chunk
    at_row = lax.broadcasted_iota(jnp.int32, (rows, rows), 0)
    at_col = lax.broadcasted_iota(jnp.int32, (rows, rows), 1)
    spikes = []
    for w in range(2):
        keep = at_row >= at_col if w == 0 else at_row <= at_col
        ones = keep.astype(BF16)
        high, middle, low = in_three(spike_ref[...])
        spikes.append(nt_dot(ones, low) + nt_dot(ones, middle) + nt_dot(ones, high))
    for h in range(heads):
        cols = slice(h * HEAD, (h + 1) * HEAD)
        q = q_ref[:, cols].astype(F32)
        q = q * jax.nn.sigmoid(q) * HEAD ** (-0.5)
        v = v_ref[:, cols]
        scores = jnp.zeros((rows, rows), F32)
        for w in range(2):
            keep = at_row >= at_col if w == 0 else at_row <= at_col
            key = slack_ref[:, cols] * jax.nn.sigmoid(-f_ref[w, :, cols].astype(F32))
            decay = jnp.log1p(-key)
            ones = keep.astype(BF16)
            high, middle, low = in_three(decay)
            running = (
                jnp.dot(ones, low, preferred_element_type=F32)
                + jnp.dot(ones, middle, preferred_element_type=F32)
                + jnp.dot(ones, high, preferred_element_type=F32)
                + spikes[w][:, h : h + 1]
            )
            final = running[rows - 1 : rows] if w == 0 else running[0:1]
            q_scaled = (q * jnp.exp(running)).astype(BF16)
            k_scaled = (key * jnp.exp(-running)).astype(BF16)
            scores = scores + jnp.where(keep, nt_dot(q_scaled, k_scaled), 0.0)
            k_end = (key * jnp.exp(final - running)).astype(BF16)
            state = tn_dot(v, k_end).astype(BF16)
            reach_ref[w, :, cols] = q_scaled
            at = (w * heads + h) * pieces
            send_ref[at : at + pieces, 0:chunk, :] = state.reshape(pieces, chunk, HEAD)
            total = jnp.concatenate([t.astype(F32) for t in in_three(jnp.exp(final))], axis=0)
            total = jnp.concatenate([total, jnp.zeros((5, HEAD), F32)], axis=0).astype(BF16)
            send_ref[at : at + pieces, chunk : chunk + 8, :] = jnp.broadcast_to(
                total[None], (pieces, 8, HEAD)
            )
        near_ref[:, cols] = jnp.dot(scores.astype(BF16), v, preferred_element_type=F32)


def scan_body(back_ref, got_ref, give_ref):
    blocks, wide, _ = got_ref.shape
    chunk = wide - 8
    back = back_ref[0]
    state = jnp.zeros((chunk, HEAD), F32)
    for b in range(blocks):
        at = jnp.where(back == 1, blocks - 1 - b, b)
        give_ref[at] = state.astype(BF16)
        piece = got_ref[at].astype(F32)
        total = piece[chunk : chunk + 1] + piece[chunk + 1 : chunk + 2] + piece[chunk + 2 : chunk + 3]
        state = total * state + piece[0:chunk]


def project_body(
    own_ref, near_ref, reach_ref, enter_ref, gate_ref, gain_ref, weight_ref, o0, o1, o2, o3, mixed_ref
):
    heads = near_ref.shape[1] // HEAD
    gain = gain_ref[...].astype(F32)
    for h in range(heads):
        cols = slice(h * HEAD, (h + 1) * HEAD)
        mix = near_ref[:, cols]
        mix = mix + nt_dot(reach_ref[0, :, cols], enter_ref[h])
        mix = mix + nt_dot(reach_ref[1, :, cols], enter_ref[heads + h])
        scale = lax.rsqrt(jnp.mean(mix * mix, axis=-1, keepdims=True) + NORM_EPS)
        g = gate_ref[:, cols].astype(F32)
        mixed_ref[:, cols] = (mix * scale * gain * (g * jax.nn.sigmoid(g))).astype(BF16)
    outs = (o0, o1, o2, o3)
    part = o0.shape[0]
    own = own_ref[0]
    turned = jnp.concatenate(
        [
            mixed_ref[pl.ds(pl.multiple_of(lax.rem(own + d, len(outs)) * part, part), part), :]
            for d in range(len(outs))
        ],
        axis=0,
    )
    lowered = jnp.dot(turned, weight_ref[...], preferred_element_type=F32).astype(BF16)
    for d, out_ref in enumerate(outs):
        out_ref[...] = lowered[d * part : (d + 1) * part]


def halves_body(parity_ref, gate_ref, up_ref, down_ref, keep_ref, give_ref):
    hidden = gate_ref.shape[1]
    full = hidden // HEAD // 2 * HEAD
    shared = slice(full, full + HEAD)
    gate = gate_ref[:, shared].astype(F32)
    up = pltpu.roll(up_ref[:, shared].astype(F32), HEAD // 2, 1)
    lane = lax.broadcasted_iota(jnp.int32, gate.shape, 1)

    def write(out_ref, second):
        start = hidden - full if second else 0
        for k, ref in enumerate((gate_ref, up_ref)):
            out_ref[:, k * full : (k + 1) * full] = ref[:, start : start + full]
        at = 2 * full + HEAD
        joint = jnp.where(lane < HEAD // 2, up, gate) if second else jnp.where(lane < HEAD // 2, gate, up)
        out_ref[:, 2 * full : at] = joint.astype(BF16)
        out_ref[:, at : at + full] = down_ref[:, start : start + full]
        out_ref[:, at + full :] = down_ref[:, shared]

    @pl.when(parity_ref[0] == 0)
    def _():
        write(keep_ref, False)
        write(give_ref, True)

    @pl.when(parity_ref[0] != 0)
    def _():
        write(keep_ref, True)
        write(give_ref, False)


def in_order_body(at_ref, whole_ref, weights_ref, sems):
    _, y_size, cores, _, _ = weights_ref.shape
    y = at_ref[0]
    copies = []
    for c in range(cores):
        for k in range(y_size):
            copies.append(
                pltpu.make_async_copy(
                    whole_ref.at[:, c, k],
                    weights_ref.at[:, lax.rem(y + y_size - k, y_size), c],
                    sems.at[c * y_size + k],
                )
            )
    for copy in copies:
        copy.start()
    for copy in copies:
        copy.wait()


def mixer_body(at_ref, *refs, hidden):
    (own_ref, near_ref), x_refs, weights_ref, outs = refs[:2], refs[2:6], refs[6], refs[7:13]
    tokens_ref = refs[13]
    model, _ = weights_ref.shape
    y = at_ref[0]
    full = hidden // HEAD // 2 * HEAD
    split = model // 2
    rows = own_ref.shape[0]
    part = rows // len(x_refs)
    tokens_ref[:rows, :split] = own_ref[...]
    tokens_ref[rows:, :split] = near_ref[...]
    for d, ref in enumerate(x_refs):
        tokens_ref[d * part : (d + 1) * part, split:] = ref[:part]
        tokens_ref[rows + d * part : rows + (d + 1) * part, split:] = ref[part:]
    at = 2 * full + HEAD
    act = jnp.dot(tokens_ref[...], weights_ref[:, :at], preferred_element_type=F32)
    gate, up, joint = act[:, :full], act[:, full : 2 * full], act[:, 2 * full :]
    inner = gate * jax.nn.sigmoid(gate) * up
    shared = joint * jax.nn.sigmoid(joint) * pltpu.roll(joint, HEAD // 2, 1)
    lane = lax.broadcasted_iota(jnp.int32, shared.shape, 1)
    low = jnp.where(lax.rem(y, 2) == 0, 0, HEAD // 2)
    shared = jnp.where((lane >= low) & (lane < low + HEAD // 2), shared, 0.0)
    inner = jnp.concatenate([inner.astype(BF16), shared.astype(BF16)], axis=1)
    lowered = nt_dot(inner, weights_ref[:, at:])
    for d, out_ref in enumerate(outs[:4]):
        at = slice(d * part, (d + 1) * part)
        out_ref[:part] = lowered[:rows][at, :split].astype(out_ref.dtype)
        out_ref[part:] = lowered[rows:][at, :split].astype(out_ref.dtype)
    outs[4][...] = lowered[:rows, split:]
    outs[5][...] = lowered[rows:, split:].astype(BF16)


VMEM = pl.BlockSpec(memory_space=pltpu.VMEM)
ANY = pl.BlockSpec(memory_space=pl.ANY)
SMEM = pl.BlockSpec(memory_space=pltpu.SMEM)


def shift(array, axis, by):
    size = lax.axis_size(axis)
    return lax.ppermute(array, axis, [(k, (k + by) % size) for k in range(size)])


def local(
    queries,
    forget_logits,
    value_matrix,
    output_gate_logits,
    forget_slack,
    spike_log_forget,
    head_norm_gain,
    output_weight,
    residual,
    mixer_norm_gain,
    mixer_gate_weight,
    mixer_up_weight,
    mixer_down_weight,
):
    rows, width = queries.shape
    heads = spike_log_forget.shape[1]
    model = output_weight.shape[1]
    hidden = mixer_gate_weight.shape[1]
    blocks = lax.axis_size(SP)
    n_tp = lax.axis_size("tp")
    sp_at = lax.axis_index(SP)
    tp_at = lax.axis_index("tp")
    chunk = 2 * heads * HEAD // blocks

    z_size, y_size, cores = (lax.axis_size(axis) for axis in SP)
    y_at = lax.axis_index("sp_1")
    slab = mixer_gate_weight.shape[0]
    wide = hidden // HEAD // 2 * HEAD * 3 + 2 * HEAD
    send, near, reach, keep, give = pl.pallas_call(
        local_body,
        out_shape=(
            jax.ShapeDtypeStruct((blocks, chunk + 8, HEAD), BF16),
            jax.ShapeDtypeStruct((rows, width), F32),
            jax.ShapeDtypeStruct((2, rows, width), BF16),
            jax.ShapeDtypeStruct((slab, wide), BF16),
            jax.ShapeDtypeStruct((slab, wide), BF16),
        ),
        in_specs=[SMEM] + [VMEM] * 8,
        out_specs=(VMEM,) * 5,
        name="local_sweep",
    )(
        (y_at % 2)[None],
        queries,
        forget_logits,
        value_matrix,
        forget_slack[None],
        spike_log_forget.T,
        mixer_gate_weight,
        mixer_up_weight,
        mixer_down_weight.T,
    )
    got = lax.all_to_all(send, SP, 0, 0, tiled=True)
    line = [keep] + [shift(give if d % 2 else keep, "sp_1", d) for d in range(1, y_size)]
    line = jnp.concatenate(line, axis=0)
    whole = lax.all_gather(line, ("sp_0", "sp_2"), axis=0, tiled=True).reshape(z_size, cores, y_size, slab, wide)
    give = pl.pallas_call(
        scan_body,
        out_shape=jax.ShapeDtypeStruct((blocks, chunk, HEAD), BF16),
        in_specs=[SMEM, VMEM],
        out_specs=VMEM,
        compiler_params=pltpu.CompilerParams(vmem_limit_bytes=12 * 1024 * 1024),
        name="block_scan",
    )((sp_at >= blocks // 2).astype(jnp.int32)[None], got)
    enter = lax.all_to_all(give, SP, 0, 0, tiled=True).reshape(2 * heads, HEAD, HEAD)

    part = rows // n_tp
    parts = pl.pallas_call(
        project_body,
        out_shape=(jax.ShapeDtypeStruct((part, model), BF16),) * n_tp,
        in_specs=[SMEM] + [VMEM] * 6,
        out_specs=(VMEM,) * n_tp,
        scratch_shapes=[pltpu.VMEM((rows, width), BF16)],
        name="norm_project",
    )(tp_at[None], near, reach, enter, output_gate_logits, head_norm_gain[None], output_weight)

    arrived = [parts[0]] + [shift(parts[d], "tp", d) for d in range(1, n_tp)]
    own_resid = lax.dynamic_slice_in_dim(residual, tp_at * part, part, 0)
    hidden_f = own_resid.astype(F32)
    for a in arrived:
        hidden_f = hidden_f + a.astype(F32)
    hidden_state = hidden_f.astype(BF16)
    held = hidden_state.astype(F32)
    normed = (
        held
        * lax.rsqrt(jnp.mean(held * held, axis=-1, keepdims=True) + NORM_EPS)
        * mixer_norm_gain.astype(F32)
    ).astype(BF16)
    swap = [(k, k ^ 1) for k in range(y_size)]
    split = model // 2
    left, right = normed[:, :split], normed[:, split:]
    both = jnp.concatenate([right, lax.ppermute(right, "sp_1", swap)], axis=0)
    own = jnp.concatenate([left] + [shift(left, "tp", d) for d in range(1, n_tp)], axis=0)
    lines = [both] + [shift(both, "tp", d) for d in range(1, n_tp)]
    tokens = [own, lax.ppermute(own, "sp_1", swap)] + lines
    weights = pl.pallas_call(
        in_order_body,
        out_shape=jax.ShapeDtypeStruct((z_size, y_size, cores, slab, wide), BF16),
        in_specs=[SMEM, ANY],
        out_specs=VMEM,
        scratch_shapes=[pltpu.SemaphoreType.DMA((y_size * cores,))],
        compiler_params=pltpu.CompilerParams(vmem_limit_bytes=40 * 1024 * 1024),
        name="weights_in_order",
    )(y_at[None], whole)
    weights = weights.reshape(model, wide)
    lowered = pl.pallas_call(
        lambda *refs: mixer_body(*refs, hidden=hidden),
        out_shape=(jax.ShapeDtypeStruct((2 * part, split), F32),)
        + (jax.ShapeDtypeStruct((2 * part, split), BF16),) * (n_tp - 1)
        + (jax.ShapeDtypeStruct((rows, split), F32), jax.ShapeDtypeStruct((rows, split), BF16)),
        in_specs=[SMEM] + [VMEM] * (len(tokens) + 1),
        out_specs=(VMEM,) * (n_tp + 2),
        scratch_shapes=[pltpu.VMEM((2 * rows, model), BF16)],
        compiler_params=pltpu.CompilerParams(vmem_limit_bytes=24 * 1024 * 1024),
        name="channel_mixer",
    )(y_at[None], *tokens, weights)
    crossed = lax.ppermute(lowered[n_tp + 1], "sp_1", swap)
    sums = lowered[0]
    for d in range(1, n_tp):
        sums = sums + shift(lowered[d], "tp", n_tp - d).astype(F32)
    added = lowered[n_tp] + crossed.astype(F32)
    out_right = hidden_state[:, split:].astype(F32) + added[:part]
    for d in range(1, n_tp):
        back = added[d * part : (d + 1) * part].astype(BF16)
        out_right = out_right + shift(back, "tp", n_tp - d).astype(F32)
    theirs = lax.ppermute(sums[part:].astype(BF16), "sp_1", swap)
    out_left = hidden_state[:, :split].astype(F32) + sums[:part] + theirs.astype(F32)
    return jnp.concatenate([out_left, out_right], axis=1).astype(BF16)


def solution(mesh):
    torus = Mesh(mesh.devices.reshape(8, 4, 2, mesh.shape["tp"]), ("sp_0", "sp_1", "sp_2", "tp"))
    return jax.shard_map(
        local,
        mesh=torus,
        in_specs=(
            P(SP, "tp"),
            P(None, SP, "tp"),
            P(SP, "tp"),
            P(SP, "tp"),
            P("tp"),
            P(SP, "tp"),
            P(),
            P("tp", None),
            P(SP, None),
            P(),
            P(SP, "tp"),
            P(SP, "tp"),
            P("tp", SP),
        ),
        out_specs=P(SP_TP, None),
        check_vma=False,
    )
```

```python
import jax
import jax.numpy as jnp
from jax import lax
from jax.experimental import pallas as pl
from jax.experimental.pallas import tpu as pltpu
from jax.sharding import Mesh
from jax.sharding import PartitionSpec as P


SP = ("sp_0", "sp_1", "sp_2")
SP_TP = ("sp_0", "sp_1", "sp_2", "tp")
NORM_EPS = 1e-06
F32 = jnp.float32
BF16 = jnp.bfloat16
HEAD = 128


def nt_dot(a, b):
    return lax.dot_general(a, b, (((1,), (1,)), ((), ())), preferred_element_type=F32)


def tn_dot(a, b):
    return lax.dot_general(a, b, (((0,), (0,)), ((), ())), preferred_element_type=F32)


def in_three(a):
    high = a.astype(BF16)
    rest = a - high.astype(F32)
    middle = rest.astype(BF16)
    return high, middle, (rest - middle.astype(F32)).astype(BF16)


def local_body(
    parity_ref,
    q_ref,
    f_ref,
    v_ref,
    slack_ref,
    spike_ref,
    w_gate_ref,
    w_up_ref,
    w_down_ref,
    send_ref,
    near_ref,
    reach_ref,
    keep_ref,
    give_ref,
):
    halves_body(parity_ref, w_gate_ref, w_up_ref, w_down_ref, keep_ref, give_ref)
    rows = q_ref.shape[0]
    heads = spike_ref.shape[0]
    chunk = send_ref.shape[1] - 8
    pieces = HEAD // chunk
    at_row = lax.broadcasted_iota(jnp.int32, (rows, rows), 0)
    at_col = lax.broadcasted_iota(jnp.int32, (rows, rows), 1)
    spikes = []
    for w in range(2):
        keep = at_row >= at_col if w == 0 else at_row <= at_col
        ones = keep.astype(BF16)
        high, middle, low = in_three(spike_ref[...])
        spikes.append(nt_dot(ones, low) + nt_dot(ones, middle) + nt_dot(ones, high))
    for h in range(heads):
        cols = slice(h * HEAD, (h + 1) * HEAD)
        q = q_ref[:, cols].astype(F32)
        q = q * jax.nn.sigmoid(q) * HEAD ** (-0.5)
        v = v_ref[:, cols]
        scores = jnp.zeros((rows, rows), F32)
        for w in range(2):
            keep = at_row >= at_col if w == 0 else at_row <= at_col
            key = slack_ref[:, cols] * jax.nn.sigmoid(-f_ref[w, :, cols].astype(F32))
            decay = jnp.log1p(-key)
            ones = keep.astype(BF16)
            high, middle, low = in_three(decay)
            running = (
                jnp.dot(ones, low, preferred_element_type=F32)
                + jnp.dot(ones, middle, preferred_element_type=F32)
                + jnp.dot(ones, high, preferred_element_type=F32)
                + spikes[w][:, h : h + 1]
            )
            final = running[rows - 1 : rows] if w == 0 else running[0:1]
            q_scaled = (q * jnp.exp(running)).astype(BF16)
            k_scaled = (key * jnp.exp(-running)).astype(BF16)
            scores = scores + jnp.where(keep, nt_dot(q_scaled, k_scaled), 0.0)
            k_end = (key * jnp.exp(final - running)).astype(BF16)
            state = tn_dot(v, k_end).astype(BF16)
            reach_ref[w, :, cols] = q_scaled
            at = (w * heads + h) * pieces
            send_ref[at : at + pieces, 0:chunk, :] = state.reshape(pieces, chunk, HEAD)
            total = jnp.concatenate([t.astype(F32) for t in in_three(jnp.exp(final))], axis=0)
            total = jnp.concatenate([total, jnp.zeros((5, HEAD), F32)], axis=0).astype(BF16)
            send_ref[at : at + pieces, chunk : chunk + 8, :] = jnp.broadcast_to(
                total[None], (pieces, 8, HEAD)
            )
        near_ref[:, cols] = jnp.dot(scores.astype(BF16), v, preferred_element_type=F32)


def scan_body(back_ref, got_ref, give_ref):
    blocks, wide, _ = got_ref.shape
    chunk = wide - 8
    back = back_ref[0]
    state = jnp.zeros((chunk, HEAD), F32)
    for b in range(blocks):
        at = jnp.where(back == 1, blocks - 1 - b, b)
        give_ref[at] = state.astype(BF16)
        piece = got_ref[at].astype(F32)
        total = piece[chunk : chunk + 1] + piece[chunk + 1 : chunk + 2] + piece[chunk + 2 : chunk + 3]
        state = total * state + piece[0:chunk]


def project_body(
    own_ref, near_ref, reach_ref, enter_ref, gate_ref, gain_ref, weight_ref, o0, o1, o2, o3, mixed_ref
):
    heads = near_ref.shape[1] // HEAD
    gain = gain_ref[...].astype(F32)
    for h in range(heads):
        cols = slice(h * HEAD, (h + 1) * HEAD)
        mix = near_ref[:, cols]
        mix = mix + nt_dot(reach_ref[0, :, cols], enter_ref[h])
        mix = mix + nt_dot(reach_ref[1, :, cols], enter_ref[heads + h])
        scale = lax.rsqrt(jnp.mean(mix * mix, axis=-1, keepdims=True) + NORM_EPS)
        g = gate_ref[:, cols].astype(F32)
        mixed_ref[:, cols] = (mix * scale * gain * (g * jax.nn.sigmoid(g))).astype(BF16)
    outs = (o0, o1, o2, o3)
    part = o0.shape[0]
    own = own_ref[0]
    turned = jnp.concatenate(
        [
            mixed_ref[pl.ds(pl.multiple_of(lax.rem(own + d, len(outs)) * part, part), part), :]
            for d in range(len(outs))
        ],
        axis=0,
    )
    lowered = jnp.dot(turned, weight_ref[...], preferred_element_type=F32).astype(BF16)
    for d, out_ref in enumerate(outs):
        out_ref[...] = lowered[d * part : (d + 1) * part]


def halves_body(parity_ref, gate_ref, up_ref, down_ref, keep_ref, give_ref):
    hidden = gate_ref.shape[1]
    full = hidden // HEAD // 2 * HEAD
    shared = slice(full, full + HEAD)
    gate = gate_ref[:, shared].astype(F32)
    up = pltpu.roll(up_ref[:, shared].astype(F32), HEAD // 2, 1)
    lane = lax.broadcasted_iota(jnp.int32, gate.shape, 1)

    def write(out_ref, second):
        start = hidden - full if second else 0
        for k, ref in enumerate((gate_ref, up_ref)):
            out_ref[:, k * full : (k + 1) * full] = ref[:, start : start + full]
        at = 2 * full + HEAD
        joint = jnp.where(lane < HEAD // 2, up, gate) if second else jnp.where(lane < HEAD // 2, gate, up)
        out_ref[:, 2 * full : at] = joint.astype(BF16)
        out_ref[:, at : at + full] = down_ref[:, start : start + full]
        out_ref[:, at + full :] = down_ref[:, shared]

    @pl.when(parity_ref[0] == 0)
    def _():
        write(keep_ref, False)
        write(give_ref, True)

    @pl.when(parity_ref[0] != 0)
    def _():
        write(keep_ref, True)
        write(give_ref, False)


def in_order_body(at_ref, *refs):
    pieces, (weights_ref, sems) = refs[:18], refs[18:]
    z_size, y_size, cores, _, _ = weights_ref.shape
    y, z, core = at_ref[0], at_ref[1], at_ref[2]
    ahead = z_size // 2
    copies = []
    for c in range(cores):
        lines = pieces[9 * c : 9 * c + 9]
        row_core = core if c == 0 else 1 - core
        for back in range(z_size):
            at_z = lax.rem(z + z_size - back, z_size)
            for k in range(y_size):
                if back == ahead:
                    source = lines[ahead].at[k] if k < 2 else lines[ahead + 1].at[k - 2]
                else:
                    source = lines[back if back < ahead else back + 1].at[k]
                copies.append(
                    pltpu.make_async_copy(
                        source,
                        weights_ref.at[at_z, lax.rem(y + y_size - k, y_size), row_core],
                        sems.at[(c * z_size + back) * y_size + k],
                    )
                )
    for copy in copies:
        copy.start()
    for copy in copies:
        copy.wait()


def mixer_body(at_ref, *refs, hidden):
    (own_ref, near_ref), x_refs, weights_ref, outs = refs[:2], refs[2:6], refs[6], refs[7:13]
    tokens_ref = refs[13]
    model, _ = weights_ref.shape
    y = at_ref[0]
    full = hidden // HEAD // 2 * HEAD
    split = model // 2
    rows = own_ref.shape[0]
    part = rows // len(x_refs)
    tokens_ref[:rows, :split] = own_ref[...]
    tokens_ref[rows:, :split] = near_ref[...]
    for d, ref in enumerate(x_refs):
        tokens_ref[d * part : (d + 1) * part, split:] = ref[:part]
        tokens_ref[rows + d * part : rows + (d + 1) * part, split:] = ref[part:]
    at = 2 * full + HEAD
    act = jnp.dot(tokens_ref[...], weights_ref[:, :at], preferred_element_type=F32)
    gate, up, joint = act[:, :full], act[:, full : 2 * full], act[:, 2 * full :]
    inner = gate * jax.nn.sigmoid(gate) * up
    shared = joint * jax.nn.sigmoid(joint) * pltpu.roll(joint, HEAD // 2, 1)
    lane = lax.broadcasted_iota(jnp.int32, shared.shape, 1)
    low = jnp.where(lax.rem(y, 2) == 0, 0, HEAD // 2)
    shared = jnp.where((lane >= low) & (lane < low + HEAD // 2), shared, 0.0)
    inner = jnp.concatenate([inner.astype(BF16), shared.astype(BF16)], axis=1)
    lowered = nt_dot(inner, weights_ref[:, at:])
    for d, out_ref in enumerate(outs[:4]):
        at = slice(d * part, (d + 1) * part)
        out_ref[:part] = lowered[:rows][at, :split].astype(out_ref.dtype)
        out_ref[part:] = lowered[rows:][at, :split].astype(out_ref.dtype)
    outs[4][...] = lowered[:rows, split:]
    outs[5][...] = lowered[rows:, split:].astype(BF16)


VMEM = pl.BlockSpec(memory_space=pltpu.VMEM)
ANY = pl.BlockSpec(memory_space=pl.ANY)
SMEM = pl.BlockSpec(memory_space=pltpu.SMEM)


def shift(array, axis, by):
    size = lax.axis_size(axis)
    return lax.ppermute(array, axis, [(k, (k + by) % size) for k in range(size)])


def local(
    queries,
    forget_logits,
    value_matrix,
    output_gate_logits,
    forget_slack,
    spike_log_forget,
    head_norm_gain,
    output_weight,
    residual,
    mixer_norm_gain,
    mixer_gate_weight,
    mixer_up_weight,
    mixer_down_weight,
):
    rows, width = queries.shape
    heads = spike_log_forget.shape[1]
    model = output_weight.shape[1]
    hidden = mixer_gate_weight.shape[1]
    blocks = lax.axis_size(SP)
    n_tp = lax.axis_size("tp")
    sp_at = lax.axis_index(SP)
    tp_at = lax.axis_index("tp")
    chunk = 2 * heads * HEAD // blocks

    z_size, y_size, cores = (lax.axis_size(axis) for axis in SP)
    y_at = lax.axis_index("sp_1")
    slab = mixer_gate_weight.shape[0]
    wide = hidden // HEAD // 2 * HEAD * 3 + 2 * HEAD
    send, near, reach, keep, give = pl.pallas_call(
        local_body,
        out_shape=(
            jax.ShapeDtypeStruct((blocks, chunk + 8, HEAD), BF16),
            jax.ShapeDtypeStruct((rows, width), F32),
            jax.ShapeDtypeStruct((2, rows, width), BF16),
            jax.ShapeDtypeStruct((slab, wide), BF16),
            jax.ShapeDtypeStruct((slab, wide), BF16),
        ),
        in_specs=[SMEM] + [VMEM] * 8,
        out_specs=(VMEM,) * 5,
        name="local_sweep",
    )(
        (y_at % 2)[None],
        queries,
        forget_logits,
        value_matrix,
        forget_slack[None],
        spike_log_forget.T,
        mixer_gate_weight,
        mixer_up_weight,
        mixer_down_weight.T,
    )
    got = lax.all_to_all(send, SP, 0, 0, tiled=True)
    line = [keep] + [shift(give if d % 2 else keep, "sp_1", d) for d in range(1, y_size)]
    line = jnp.concatenate(line, axis=0)
    line = line.reshape(y_size, slab, wide)
    ups, downs = [shift(line, "sp_0", 1)], [shift(line, "sp_0", z_size - 1)]
    give = pl.pallas_call(
        scan_body,
        out_shape=jax.ShapeDtypeStruct((blocks, chunk, HEAD), BF16),
        in_specs=[SMEM, VMEM],
        out_specs=VMEM,
        compiler_params=pltpu.CompilerParams(vmem_limit_bytes=12 * 1024 * 1024),
        name="block_scan",
    )((sp_at >= blocks // 2).astype(jnp.int32)[None], got)
    enter = lax.all_to_all(give, SP, 0, 0, tiled=True)
    ups.append(shift(ups[0], "sp_0", 1))
    downs.append(shift(downs[0], "sp_0", z_size - 1))
    crossed = [shift(piece, "sp_2", 1) for piece in (line, ups[0], downs[0])]
    crossed, enter = lax.optimization_barrier((crossed, enter))
    enter = enter.reshape(2 * heads, HEAD, HEAD)

    part = rows // n_tp
    parts = pl.pallas_call(
        project_body,
        out_shape=(jax.ShapeDtypeStruct((part, model), BF16),) * n_tp,
        in_specs=[SMEM] + [VMEM] * 6,
        out_specs=(VMEM,) * n_tp,
        scratch_shapes=[pltpu.VMEM((rows, width), BF16)],
        name="norm_project",
    )(tp_at[None], near, reach, enter, output_gate_logits, head_norm_gain[None], output_weight)

    ups[1], downs[1], parts = lax.optimization_barrier((ups[1], downs[1], parts))
    ups.append(shift(ups[1], "sp_0", 1))
    downs.append(shift(downs[1], "sp_0", z_size - 1))
    crossed += [shift(piece, "sp_2", 1) for piece in (ups[1], downs[1])]
    arrived = [parts[0]] + [shift(parts[d], "tp", d) for d in range(1, n_tp)]
    own_resid = lax.dynamic_slice_in_dim(residual, tp_at * part, part, 0)
    hidden_f = own_resid.astype(F32)
    for a in arrived:
        hidden_f = hidden_f + a.astype(F32)
    hidden_state = hidden_f.astype(BF16)
    held = hidden_state.astype(F32)
    normed = (
        held
        * lax.rsqrt(jnp.mean(held * held, axis=-1, keepdims=True) + NORM_EPS)
        * mixer_norm_gain.astype(F32)
    ).astype(BF16)
    swap = [(k, k ^ 1) for k in range(y_size)]
    ups[2], downs[2], crossed, normed = lax.optimization_barrier((ups[2], downs[2], crossed, normed))
    far = shift(ups[2][: y_size // 2], "sp_0", 1)
    far_back = shift(downs[2][y_size // 2 :], "sp_0", z_size - 1)
    crossed = crossed + [shift(piece, "sp_2", 1) for piece in (ups[2], downs[2])]
    split = model // 2
    left, right = normed[:, :split], normed[:, split:]
    both = jnp.concatenate([right, lax.ppermute(right, "sp_1", swap)], axis=0)
    own = jnp.concatenate([left] + [shift(left, "tp", d) for d in range(1, n_tp)], axis=0)
    lines = [both] + [shift(both, "tp", d) for d in range(1, n_tp)]
    tokens = [own, lax.ppermute(own, "sp_1", swap)] + lines
    crossed = crossed + [shift(piece, "sp_2", 1) for piece in (far, far_back)]
    near_line, u1, d1, u2, d2, u3, d3, f, g = crossed
    pieces = [line] + ups + [far, far_back] + downs[::-1]
    pieces += [near_line, u1, u2, u3, f, g, d3, d2, d1]
    at = jnp.stack([y_at, lax.axis_index("sp_0"), lax.axis_index("sp_2")])
    weights = pl.pallas_call(
        in_order_body,
        out_shape=jax.ShapeDtypeStruct((z_size, y_size, cores, slab, wide), BF16),
        in_specs=[SMEM] + [ANY] * len(pieces),
        out_specs=VMEM,
        scratch_shapes=[pltpu.SemaphoreType.DMA((z_size * y_size * cores,))],
        compiler_params=pltpu.CompilerParams(vmem_limit_bytes=28 * 1024 * 1024),
        name="weights_in_order",
    )(at, *pieces)
    weights = weights.reshape(model, wide)
    lowered = pl.pallas_call(
        lambda *refs: mixer_body(*refs, hidden=hidden),
        out_shape=(jax.ShapeDtypeStruct((2 * part, split), F32),)
        + (jax.ShapeDtypeStruct((2 * part, split), BF16),) * (n_tp - 1)
        + (jax.ShapeDtypeStruct((rows, split), F32), jax.ShapeDtypeStruct((rows, split), BF16)),
        in_specs=[SMEM] + [VMEM] * (len(tokens) + 1),
        out_specs=(VMEM,) * (n_tp + 2),
        scratch_shapes=[pltpu.VMEM((2 * rows, model), BF16)],
        compiler_params=pltpu.CompilerParams(vmem_limit_bytes=24 * 1024 * 1024),
        name="channel_mixer",
    )(y_at[None], *tokens, weights)
    crossed = lax.ppermute(lowered[n_tp + 1], "sp_1", swap)
    sums = lowered[0]
    for d in range(1, n_tp):
        sums = sums + shift(lowered[d], "tp", n_tp - d).astype(F32)
    added = lowered[n_tp] + crossed.astype(F32)
    out_right = hidden_state[:, split:].astype(F32) + added[:part]
    for d in range(1, n_tp):
        back = added[d * part : (d + 1) * part].astype(BF16)
        out_right = out_right + shift(back, "tp", n_tp - d).astype(F32)
    theirs = lax.ppermute(sums[part:].astype(BF16), "sp_1", swap)
    out_left = hidden_state[:, :split].astype(F32) + sums[:part] + theirs.astype(F32)
    return jnp.concatenate([out_left, out_right], axis=1).astype(BF16)


def solution(mesh):
    torus = Mesh(mesh.devices.reshape(8, 4, 2, mesh.shape["tp"]), ("sp_0", "sp_1", "sp_2", "tp"))
    return jax.shard_map(
        local,
        mesh=torus,
        in_specs=(
            P(SP, "tp"),
            P(None, SP, "tp"),
            P(SP, "tp"),
            P(SP, "tp"),
            P("tp"),
            P(SP, "tp"),
            P(),
            P("tp", None),
            P(SP, None),
            P(),
            P(SP, "tp"),
            P(SP, "tp"),
            P("tp", SP),
        ),
        out_specs=P(SP_TP, None),
        check_vma=False,
    )
```

```python
import jax
import jax.numpy as jnp
from jax import lax
from jax.experimental import pallas as pl
from jax.experimental.pallas import tpu as pltpu
from jax.sharding import Mesh
from jax.sharding import PartitionSpec as P


SP = ("sp_0", "sp_1", "sp_2")
SP_TP = ("sp_0", "sp_1", "sp_2", "tp")
NORM_EPS = 1e-06
F32 = jnp.float32
BF16 = jnp.bfloat16
HEAD = 128


def nt_dot(a, b):
    return lax.dot_general(a, b, (((1,), (1,)), ((), ())), preferred_element_type=F32)


def tn_dot(a, b):
    return lax.dot_general(a, b, (((0,), (0,)), ((), ())), preferred_element_type=F32)


def in_three(a):
    high = a.astype(BF16)
    rest = a - high.astype(F32)
    middle = rest.astype(BF16)
    return high, middle, (rest - middle.astype(F32)).astype(BF16)


def local_body(
    parity_ref,
    q_ref,
    f_ref,
    v_ref,
    slack_ref,
    spike_ref,
    w_gate_ref,
    w_up_ref,
    w_down_ref,
    send_ref,
    near_ref,
    reach_ref,
    keep_ref,
    give_ref,
):
    halves_body(parity_ref, w_gate_ref, w_up_ref, w_down_ref, keep_ref, give_ref)
    rows = q_ref.shape[0]
    heads = spike_ref.shape[0]
    chunk = send_ref.shape[1] - 8
    pieces = HEAD // chunk
    at_row = lax.broadcasted_iota(jnp.int32, (rows, rows), 0)
    at_col = lax.broadcasted_iota(jnp.int32, (rows, rows), 1)
    spikes = []
    for w in range(2):
        keep = at_row >= at_col if w == 0 else at_row <= at_col
        ones = keep.astype(BF16)
        high, middle, low = in_three(spike_ref[...])
        spikes.append(nt_dot(ones, low) + nt_dot(ones, middle) + nt_dot(ones, high))
    for h in range(heads):
        cols = slice(h * HEAD, (h + 1) * HEAD)
        q = q_ref[:, cols].astype(F32)
        q = q * jax.nn.sigmoid(q) * HEAD ** (-0.5)
        v = v_ref[:, cols]
        scores = jnp.zeros((rows, rows), F32)
        for w in range(2):
            keep = at_row >= at_col if w == 0 else at_row <= at_col
            key = slack_ref[:, cols] * jax.nn.sigmoid(-f_ref[w, :, cols].astype(F32))
            decay = jnp.log1p(-key)
            ones = keep.astype(BF16)
            high, middle, low = in_three(decay)
            running = (
                jnp.dot(ones, low, preferred_element_type=F32)
                + jnp.dot(ones, middle, preferred_element_type=F32)
                + jnp.dot(ones, high, preferred_element_type=F32)
                + spikes[w][:, h : h + 1]
            )
            final = running[rows - 1 : rows] if w == 0 else running[0:1]
            q_scaled = (q * jnp.exp(running)).astype(BF16)
            k_scaled = (key * jnp.exp(-running)).astype(BF16)
            scores = scores + jnp.where(keep, nt_dot(q_scaled, k_scaled), 0.0)
            k_end = (key * jnp.exp(final - running)).astype(BF16)
            state = tn_dot(v, k_end).astype(BF16)
            reach_ref[w, :, cols] = q_scaled
            at = (w * heads + h) * pieces
            send_ref[at : at + pieces, 0:chunk, :] = state.reshape(pieces, chunk, HEAD)
            total = jnp.concatenate([t.astype(F32) for t in in_three(jnp.exp(final))], axis=0)
            total = jnp.concatenate([total, jnp.zeros((5, HEAD), F32)], axis=0).astype(BF16)
            send_ref[at : at + pieces, chunk : chunk + 8, :] = jnp.broadcast_to(
                total[None], (pieces, 8, HEAD)
            )
        near_ref[:, cols] = jnp.dot(scores.astype(BF16), v, preferred_element_type=F32)


def scan_body(back_ref, got_ref, give_ref):
    blocks, wide, _ = got_ref.shape
    chunk = wide - 8
    back = back_ref[0]
    state = jnp.zeros((chunk, HEAD), F32)
    for b in range(blocks):
        at = jnp.where(back == 1, blocks - 1 - b, b)
        give_ref[at] = state.astype(BF16)
        piece = got_ref[at].astype(F32)
        total = piece[chunk : chunk + 1] + piece[chunk + 1 : chunk + 2] + piece[chunk + 2 : chunk + 3]
        state = total * state + piece[0:chunk]


def project_body(
    own_ref, near_ref, reach_ref, enter_ref, gate_ref, gain_ref, weight_ref, o0, o1, o2, o3, mixed_ref
):
    heads = near_ref.shape[1] // HEAD
    gain = gain_ref[...].astype(F32)
    for h in range(heads):
        cols = slice(h * HEAD, (h + 1) * HEAD)
        mix = near_ref[:, cols]
        mix = mix + nt_dot(reach_ref[0, :, cols], enter_ref[h])
        mix = mix + nt_dot(reach_ref[1, :, cols], enter_ref[heads + h])
        scale = lax.rsqrt(jnp.mean(mix * mix, axis=-1, keepdims=True) + NORM_EPS)
        g = gate_ref[:, cols].astype(F32)
        mixed_ref[:, cols] = (mix * scale * gain * (g * jax.nn.sigmoid(g))).astype(BF16)
    outs = (o0, o1, o2, o3)
    part = o0.shape[0]
    own = own_ref[0]
    turned = jnp.concatenate(
        [
            mixed_ref[pl.ds(pl.multiple_of(lax.rem(own + d, len(outs)) * part, part), part), :]
            for d in range(len(outs))
        ],
        axis=0,
    )
    lowered = jnp.dot(turned, weight_ref[...], preferred_element_type=F32).astype(BF16)
    for d, out_ref in enumerate(outs):
        out_ref[...] = lowered[d * part : (d + 1) * part]


def halves_body(parity_ref, gate_ref, up_ref, down_ref, keep_ref, give_ref):
    hidden = gate_ref.shape[1]
    full = hidden // HEAD // 2 * HEAD
    shared = slice(full, full + HEAD)
    gate = gate_ref[:, shared].astype(F32)
    up = pltpu.roll(up_ref[:, shared].astype(F32), HEAD // 2, 1)
    lane = lax.broadcasted_iota(jnp.int32, gate.shape, 1)

    def write(out_ref, second):
        start = hidden - full if second else 0
        for k, ref in enumerate((gate_ref, up_ref)):
            out_ref[:, k * full : (k + 1) * full] = ref[:, start : start + full]
        at = 2 * full + HEAD
        joint = jnp.where(lane < HEAD // 2, up, gate) if second else jnp.where(lane < HEAD // 2, gate, up)
        out_ref[:, 2 * full : at] = joint.astype(BF16)
        out_ref[:, at : at + full] = down_ref[:, start : start + full]
        out_ref[:, at + full :] = down_ref[:, shared]

    @pl.when(parity_ref[0] == 0)
    def _():
        write(keep_ref, False)
        write(give_ref, True)

    @pl.when(parity_ref[0] != 0)
    def _():
        write(keep_ref, True)
        write(give_ref, False)


def in_order_body(at_ref, *refs):
    pieces, weights_ref = refs[:18], refs[18]
    z_size, y_size, cores, _, _ = weights_ref.shape
    y, z, core = at_ref[0], at_ref[1], at_ref[2]
    ahead = z_size // 2
    for c in range(cores):
        lines = pieces[9 * c : 9 * c + 9]
        row_core = core if c == 0 else 1 - core
        for back in range(z_size):
            at_z = lax.rem(z + z_size - back, z_size)
            for k in range(y_size):
                at_y = lax.rem(y + y_size - k, y_size)
                if back == ahead:
                    piece = lines[ahead][k] if k < 2 else lines[ahead + 1][k - 2]
                else:
                    piece = lines[back if back < ahead else back + 1][k]
                weights_ref[at_z, at_y, row_core] = piece


def mixer_body(at_ref, *refs, hidden):
    (own_ref, near_ref), x_refs, weights_ref, outs = refs[:2], refs[2:6], refs[6], refs[7:13]
    tokens_ref = refs[13]
    model, _ = weights_ref.shape
    y = at_ref[0]
    full = hidden // HEAD // 2 * HEAD
    split = model // 2
    rows = own_ref.shape[0]
    part = rows // len(x_refs)
    tokens_ref[:rows, :split] = own_ref[...]
    tokens_ref[rows:, :split] = near_ref[...]
    for d, ref in enumerate(x_refs):
        tokens_ref[d * part : (d + 1) * part, split:] = ref[:part]
        tokens_ref[rows + d * part : rows + (d + 1) * part, split:] = ref[part:]
    at = 2 * full + HEAD
    act = jnp.dot(tokens_ref[...], weights_ref[:, :at], preferred_element_type=F32)
    gate, up, joint = act[:, :full], act[:, full : 2 * full], act[:, 2 * full :]
    inner = gate * jax.nn.sigmoid(gate) * up
    shared = joint * jax.nn.sigmoid(joint) * pltpu.roll(joint, HEAD // 2, 1)
    lane = lax.broadcasted_iota(jnp.int32, shared.shape, 1)
    low = jnp.where(lax.rem(y, 2) == 0, 0, HEAD // 2)
    shared = jnp.where((lane >= low) & (lane < low + HEAD // 2), shared, 0.0)
    inner = jnp.concatenate([inner.astype(BF16), shared.astype(BF16)], axis=1)
    lowered = nt_dot(inner, weights_ref[:, at:])
    for d, out_ref in enumerate(outs[:4]):
        at = slice(d * part, (d + 1) * part)
        out_ref[:part] = lowered[:rows][at, :split].astype(out_ref.dtype)
        out_ref[part:] = lowered[rows:][at, :split].astype(out_ref.dtype)
    outs[4][...] = lowered[:rows, split:]
    outs[5][...] = lowered[rows:, split:].astype(BF16)


VMEM = pl.BlockSpec(memory_space=pltpu.VMEM)
ANY = pl.BlockSpec(memory_space=pl.ANY)
SMEM = pl.BlockSpec(memory_space=pltpu.SMEM)


def shift(array, axis, by):
    size = lax.axis_size(axis)
    return lax.ppermute(array, axis, [(k, (k + by) % size) for k in range(size)])


def local(
    queries,
    forget_logits,
    value_matrix,
    output_gate_logits,
    forget_slack,
    spike_log_forget,
    head_norm_gain,
    output_weight,
    residual,
    mixer_norm_gain,
    mixer_gate_weight,
    mixer_up_weight,
    mixer_down_weight,
):
    rows, width = queries.shape
    heads = spike_log_forget.shape[1]
    model = output_weight.shape[1]
    hidden = mixer_gate_weight.shape[1]
    blocks = lax.axis_size(SP)
    n_tp = lax.axis_size("tp")
    sp_at = lax.axis_index(SP)
    tp_at = lax.axis_index("tp")
    chunk = 2 * heads * HEAD // blocks

    z_size, y_size, cores = (lax.axis_size(axis) for axis in SP)
    y_at = lax.axis_index("sp_1")
    slab = mixer_gate_weight.shape[0]
    wide = hidden // HEAD // 2 * HEAD * 3 + 2 * HEAD
    send, near, reach, keep, give = pl.pallas_call(
        local_body,
        out_shape=(
            jax.ShapeDtypeStruct((blocks, chunk + 8, HEAD), BF16),
            jax.ShapeDtypeStruct((rows, width), F32),
            jax.ShapeDtypeStruct((2, rows, width), BF16),
            jax.ShapeDtypeStruct((slab, wide), BF16),
            jax.ShapeDtypeStruct((slab, wide), BF16),
        ),
        in_specs=[SMEM] + [VMEM] * 8,
        out_specs=(VMEM,) * 5,
        name="local_sweep",
    )(
        (y_at % 2)[None],
        queries,
        forget_logits,
        value_matrix,
        forget_slack[None],
        spike_log_forget.T,
        mixer_gate_weight,
        mixer_up_weight,
        mixer_down_weight.T,
    )
    got = lax.all_to_all(send, SP, 0, 0, tiled=True)
    line = [keep] + [shift(give if d % 2 else keep, "sp_1", d) for d in range(1, y_size)]
    line = jnp.concatenate(line, axis=0)
    line = line.reshape(y_size, slab, wide)
    ups, downs = [shift(line, "sp_0", 1)], [shift(line, "sp_0", z_size - 1)]
    give = pl.pallas_call(
        scan_body,
        out_shape=jax.ShapeDtypeStruct((blocks, chunk, HEAD), BF16),
        in_specs=[SMEM, VMEM],
        out_specs=VMEM,
        compiler_params=pltpu.CompilerParams(vmem_limit_bytes=12 * 1024 * 1024),
        name="block_scan",
    )((sp_at >= blocks // 2).astype(jnp.int32)[None], got)
    enter = lax.all_to_all(give, SP, 0, 0, tiled=True)
    ups.append(shift(ups[0], "sp_0", 1))
    downs.append(shift(downs[0], "sp_0", z_size - 1))
    crossed = [shift(piece, "sp_2", 1) for piece in (line, ups[0], downs[0])]
    crossed, enter = lax.optimization_barrier((crossed, enter))
    enter = enter.reshape(2 * heads, HEAD, HEAD)

    part = rows // n_tp
    parts = pl.pallas_call(
        project_body,
        out_shape=(jax.ShapeDtypeStruct((part, model), BF16),) * n_tp,
        in_specs=[SMEM] + [VMEM] * 6,
        out_specs=(VMEM,) * n_tp,
        scratch_shapes=[pltpu.VMEM((rows, width), BF16)],
        name="norm_project",
    )(tp_at[None], near, reach, enter, output_gate_logits, head_norm_gain[None], output_weight)

    ups.append(shift(ups[1], "sp_0", 1))
    downs.append(shift(downs[1], "sp_0", z_size - 1))
    crossed += [shift(piece, "sp_2", 1) for piece in (ups[1], downs[1])]
    arrived = [parts[0]] + [shift(parts[d], "tp", d) for d in range(1, n_tp)]
    own_resid = lax.dynamic_slice_in_dim(residual, tp_at * part, part, 0)
    hidden_f = own_resid.astype(F32)
    for a in arrived:
        hidden_f = hidden_f + a.astype(F32)
    hidden_state = hidden_f.astype(BF16)
    held = hidden_state.astype(F32)
    normed = (
        held
        * lax.rsqrt(jnp.mean(held * held, axis=-1, keepdims=True) + NORM_EPS)
        * mixer_norm_gain.astype(F32)
    ).astype(BF16)
    swap = [(k, k ^ 1) for k in range(y_size)]
    far = shift(ups[2][: y_size // 2], "sp_0", 1)
    far_back = shift(downs[2][y_size // 2 :], "sp_0", z_size - 1)
    crossed = crossed + [shift(piece, "sp_2", 1) for piece in (ups[2], downs[2])]
    split = model // 2
    left, right = normed[:, :split], normed[:, split:]
    both = jnp.concatenate([right, lax.ppermute(right, "sp_1", swap)], axis=0)
    own = jnp.concatenate([left] + [shift(left, "tp", d) for d in range(1, n_tp)], axis=0)
    lines = [both] + [shift(both, "tp", d) for d in range(1, n_tp)]
    tokens = [own, lax.ppermute(own, "sp_1", swap)] + lines
    crossed = crossed + [shift(piece, "sp_2", 1) for piece in (far, far_back)]
    near_line, u1, d1, u2, d2, u3, d3, f, g = crossed
    pieces = [line] + ups + [far, far_back] + downs[::-1]
    pieces += [near_line, u1, u2, u3, f, g, d3, d2, d1]
    at = jnp.stack([y_at, lax.axis_index("sp_0"), lax.axis_index("sp_2")])
    weights = pl.pallas_call(
        in_order_body,
        out_shape=jax.ShapeDtypeStruct((z_size, y_size, cores, slab, wide), BF16),
        in_specs=[SMEM] + [VMEM] * len(pieces),
        out_specs=VMEM,
        compiler_params=pltpu.CompilerParams(vmem_limit_bytes=28 * 1024 * 1024),
        name="weights_in_order",
    )(at, *pieces)
    weights = weights.reshape(model, wide)
    lowered = pl.pallas_call(
        lambda *refs: mixer_body(*refs, hidden=hidden),
        out_shape=(jax.ShapeDtypeStruct((2 * part, split), F32),)
        + (jax.ShapeDtypeStruct((2 * part, split), BF16),) * (n_tp - 1)
        + (jax.ShapeDtypeStruct((rows, split), F32), jax.ShapeDtypeStruct((rows, split), BF16)),
        in_specs=[SMEM] + [VMEM] * (len(tokens) + 1),
        out_specs=(VMEM,) * (n_tp + 2),
        scratch_shapes=[pltpu.VMEM((2 * rows, model), BF16)],
        compiler_params=pltpu.CompilerParams(vmem_limit_bytes=24 * 1024 * 1024),
        name="channel_mixer",
    )(y_at[None], *tokens, weights)
    crossed = lax.ppermute(lowered[n_tp + 1], "sp_1", swap)
    sums = lowered[0]
    for d in range(1, n_tp):
        sums = sums + shift(lowered[d], "tp", n_tp - d).astype(F32)
    added = lowered[n_tp] + crossed.astype(F32)
    out_right = hidden_state[:, split:].astype(F32) + added[:part]
    for d in range(1, n_tp):
        back = added[d * part : (d + 1) * part].astype(BF16)
        out_right = out_right + shift(back, "tp", n_tp - d).astype(F32)
    theirs = lax.ppermute(sums[part:].astype(BF16), "sp_1", swap)
    out_left = hidden_state[:, :split].astype(F32) + sums[:part] + theirs.astype(F32)
    return jnp.concatenate([out_left, out_right], axis=1).astype(BF16)


def solution(mesh):
    torus = Mesh(mesh.devices.reshape(8, 4, 2, mesh.shape["tp"]), ("sp_0", "sp_1", "sp_2", "tp"))
    return jax.shard_map(
        local,
        mesh=torus,
        in_specs=(
            P(SP, "tp"),
            P(None, SP, "tp"),
            P(SP, "tp"),
            P(SP, "tp"),
            P("tp"),
            P(SP, "tp"),
            P(),
            P("tp", None),
            P(SP, None),
            P(),
            P(SP, "tp"),
            P(SP, "tp"),
            P("tp", SP),
        ),
        out_specs=P(SP_TP, None),
        check_vma=False,
    )
```
